32 devices in a mesh: sp: 16 (over z, y, x), tp: 2 (over core).
Axes of the slice: x: 2, y: 2, z: 4, core: 2. Of those that a mesh axis runs over, the one named last changes fastest.
Arguments:
- tokens: bfloat16 [2048, 4096], P('sp'), may hold values from -6 to 6
- norm_gain: float32 [4096], replicated, may hold values from 0.1 to 1.9
- w_query: bfloat16 [4096, 2048], P('sp', 'tp'), may hold values from -1 to 1
- w_key: bfloat16 [4096, 512], P('sp', 'tp'), may hold values from -1 to 1
- w_value: bfloat16 [4096, 512], P('sp', 'tp'), may hold values from -0.09375 to 0.09375
- w_state_in: bfloat16 [4096, 2048], P('sp', 'tp'), may hold values from -0.09375 to 0.09375
- sink_logit: float32 [32], P('tp'), may hold values from 2 to 6
- decay_rate: float32 [128, 64], P('tp'), may hold values from 0.0002 to 4
- rotation: float32 [128, 64], P('tp'), may hold values from 1 to 60
- log_step: float32 [128], P('tp'), may hold values from -5.3 to -3
- in_re: float32 [128, 64, 16], P('tp'), may hold values from -1.5 to 1.5
- in_im: float32 [128, 64, 16], P('tp'), may hold values from -1.5 to 1.5
- out_re: float32 [128, 16, 64], P('tp'), may hold values from -0.75 to 0.75
- out_im: float32 [128, 16, 64], P('tp'), may hold values from -0.75 to 0.75
- skip_gain: float32 [2048], P('tp'), may hold values from -4 to 4
- w_attn_out: bfloat16 [2048, 4096], P('tp', 'sp'), may hold values from -0.5 to 0.5
- w_state_out: bfloat16 [2048, 4096], P('tp', 'sp'), may hold values from -0.125 to 0.125
- out_gain: float32 [4096], replicated, may hold values from 0.1 to 1.9
Outputs:
- mixed: bfloat16 [2048, 4096], P(('sp', 'tp'))
The draws below stay inside these ranges and needn't reach their ends.
All inputs are finite; a program needn't handle non-finite values.
Results may differ from the reference program's by a relative error of at most 0.015.
The reference program's roundings to bfloat16 on the way count: a program that leaves them out, or rounds other values in their place, can miss the bound.
Values may be sent and summed in bfloat16 or wider, within the bound.
A program may use at most 128 MiB of HBM per device.

```python
import math
import jax
import jax.numpy as jnp
from jax import lax

D = 4096
QH = 32
KVH = 8
HEAD = 64
GSIZE = 16
STATE = 64
WINDOW = 128
TOK_DEV = 128
ATTN = 2048
GROUPS = 128
TOKENS = 2048
N_SP = 16
N_TP = 2


def spiked_columns(key, salt, column_count):
    noise_part = jax.random.normal(jax.random.fold_in(key, salt), (D, column_count), jnp.float32) * D ** (-0.5)
    noise_part = jnp.clip(noise_part, -6.0 * D ** (-0.5), 6.0 * D ** (-0.5))
    return jnp.clip(noise_part, -1.0, 1.0)


def draw_w_query(key, part):
    return spiked_columns(key, 1, QH * HEAD).astype(jnp.bfloat16)


def draw_w_key(key, part):
    return spiked_columns(key, 2, KVH * HEAD).astype(jnp.bfloat16)


def draw_decay_rate(key, part):
    slow_rate = jnp.exp(jax.random.uniform(jax.random.fold_in(key, 11), (GROUPS, STATE), jnp.float32, math.log(0.0002), math.log(0.002)))
    fast_rate = jnp.exp(jax.random.uniform(jax.random.fold_in(key, 12), (GROUPS, STATE), jnp.float32, math.log(2.0), math.log(4.0)))
    picks = jax.random.randint(jax.random.fold_in(key, 13), (GROUPS, 1), 0, 10)
    slow_flag = picks < 5
    return jnp.where(slow_flag, slow_rate, fast_rate)


def levels(key, shape, pieces, smallest, top_value):
    gain = 1.0
    for axis_at, shards_of in pieces:
        heights = jax.random.uniform(jax.random.fold_in(jax.random.fold_in(key, 6), axis_at), (shards_of,), jnp.float32, smallest / len(pieces), top_value / len(pieces))
        gain = gain * jnp.repeat(jnp.exp(heights), shape[axis_at] // shards_of).reshape((-1,) + (1,) * (len(shape) - 1 - axis_at))
    return gain


def noise(key, dims, spread, bound, pieces=(), held_as=jnp.bfloat16):
    values = jax.random.normal(key, dims, jnp.float32) * spread
    if len(pieces) > 0:
        values = levels(key, dims, pieces, -0.22, 0.18) * values
    return jnp.clip(values, min=-bound, max=bound).astype(held_as)


def setup_inputs(seed: int = 0) -> dict:
    key_of = jax.random.split(jax.random.key(seed), 19)
    tokens = noise(key_of[0], (TOKENS, D), 1.0, 6.0, ((0, 16),))
    norm_gain = jnp.clip(1.0 + 0.18 * jax.random.normal(key_of[1], (D,), jnp.float32), 0.1, 1.9)
    w_query = draw_w_query(jax.random.fold_in(key_of[18], 71), 0)
    w_key = draw_w_key(jax.random.fold_in(key_of[18], 71), 0)
    w_value = noise(key_of[4], (D, KVH * HEAD), D ** -0.5, 0.09375, ((0, 16), (1, 2)))
    w_state_in = noise(key_of[5], (D, ATTN), D ** -0.5, 0.09375, ((0, 16), (1, 2)))
    sink_logit = jnp.clip(2.0 + 4.0 * jax.random.uniform(key_of[6], (QH,), jnp.float32) ** levels(key_of[6], (QH,), ((0, 2),), -0.2, 0.2), 2.0, 6.0)
    decay_rate = draw_decay_rate(jax.random.fold_in(key_of[18], 71), 0)
    rotation = jnp.clip(1.0 + 59.0 * jax.random.uniform(key_of[8], (GROUPS, STATE), jnp.float32) ** levels(key_of[8], (GROUPS, STATE), ((0, 2),), -0.2, 0.2), 1.0, 60.0)
    log_step = jnp.clip(-5.3 + 2.3000002 * jax.random.uniform(key_of[9], (GROUPS,), jnp.float32) ** levels(key_of[9], (GROUPS,), ((0, 2),), -0.2, 0.2), -5.3, -3.0)
    in_re = noise(key_of[10], (GROUPS, STATE, GSIZE), GSIZE ** -0.5, 1.5, ((0, 2),), jnp.float32)
    in_im = noise(key_of[11], (GROUPS, STATE, GSIZE), GSIZE ** -0.5, 1.5, ((0, 2),), jnp.float32)
    out_re = noise(key_of[12], (GROUPS, GSIZE, STATE), STATE ** -0.5, 0.75, ((0, 2),), jnp.float32)
    out_im = noise(key_of[13], (GROUPS, GSIZE, STATE), STATE ** -0.5, 0.75, ((0, 2),), jnp.float32)
    skip_gain = noise(key_of[14], (ATTN,), 1.0, 4.0, ((0, 2),), jnp.float32)
    w_attn_out = noise(key_of[15], (ATTN, D), (ATTN // 16) ** -0.5, 0.5, ((0, 2), (1, 16)))
    w_state_out = noise(key_of[16], (ATTN, D), ATTN ** -0.5, 0.125, ((0, 2), (1, 16)))
    out_gain = jnp.clip(1.0 + 0.18 * jax.random.normal(key_of[17], (D,), jnp.float32), 0.1, 1.9)
    return {"tokens": tokens, "norm_gain": norm_gain, "w_query": w_query, "w_key": w_key, "w_value": w_value, "w_state_in": w_state_in, "sink_logit": sink_logit, "decay_rate": decay_rate, "rotation": rotation, "log_step": log_step, "in_re": in_re, "in_im": in_im, "out_re": out_re, "out_im": out_im, "skip_gain": skip_gain, "w_attn_out": w_attn_out, "w_state_out": w_state_out, "out_gain": out_gain}


epsilon = 1e-06
rotary_base = 500000.0

def rotate(heads_block, positions):
    head_width = heads_block.shape[-1]
    half_width = head_width // 2
    frequency = rotary_base ** (-(jnp.arange(half_width, dtype=jnp.float32) * 2.0 / head_width))
    angles = positions.astype(jnp.float32)[:, None] * frequency[None, :]
    cosine = jnp.cos(angles)[:, None, :]
    sine_part = jnp.sin(angles)[:, None, :]
    lower_half = heads_block[..., :half_width]
    upper_half = heads_block[..., half_width:]
    return jnp.concatenate([lower_half * cosine - upper_half * sine_part, upper_half * cosine + lower_half * sine_part], axis=-1)

def shape_heads(query_sum, key_sum, value_sum, positions, head_width):
    row_count = query_sum.shape[0]
    kv_heads = key_sum.shape[1] // head_width
    group_size = query_sum.shape[1] // key_sum.shape[1]
    queries = rotate(query_sum.reshape(row_count, kv_heads * group_size, head_width), positions).astype(jnp.bfloat16)
    queries = queries.reshape(row_count, kv_heads, group_size, head_width)
    key_rows = rotate(key_sum.reshape(row_count, kv_heads, head_width), positions).astype(jnp.bfloat16)
    key_rows = key_rows.reshape(row_count, kv_heads * head_width)
    value_rows = value_sum.astype(jnp.bfloat16)
    return (queries, key_rows, value_rows)

def band_attention(queries, key_rows, value_rows, sink_logit, first_row, window):
    row_count, kv_heads, group_size, head_width = queries.shape
    blocks = row_count // window
    query_blocks = queries.reshape(blocks, window, kv_heads, group_size, head_width).astype(jnp.float32)
    key_blocks = jnp.concatenate([key_rows[:row_count].reshape(blocks, window, kv_heads, head_width), key_rows[window:].reshape(blocks, window, kv_heads, head_width)], axis=1)
    value_blocks = jnp.concatenate([value_rows[:row_count].reshape(blocks, window, kv_heads, head_width), value_rows[window:].reshape(blocks, window, kv_heads, head_width)], axis=1)
    scores = jnp.einsum('bqkgd,bskd->bkgqs', query_blocks, key_blocks.astype(jnp.float32)) / math.sqrt(head_width)
    block_start = jnp.arange(blocks, dtype=jnp.int32)[:, None, None] * window
    query_at = first_row + block_start + jnp.arange(window, dtype=jnp.int32)[None, :, None]
    key_at = first_row - window + block_start + jnp.arange(2 * window, dtype=jnp.int32)[None, None, :]
    offset_gap = query_at - key_at
    visible = (offset_gap >= 0) & (offset_gap < window) & (key_at >= 0)
    scores = jnp.where(visible[:, None, None, :, :], scores, -jnp.inf)
    sink_value = sink_logit.astype(jnp.float32).reshape(1, kv_heads, group_size, 1, 1)
    top_score = jnp.maximum(lax.optimization_barrier(jnp.max(scores, axis=-1, keepdims=True)), sink_value)
    exponent = jnp.exp(scores - top_score)
    totals = lax.optimization_barrier(jnp.sum(exponent, axis=-1, keepdims=True)) + jnp.exp(sink_value - top_score)
    weights = (exponent / totals).astype(jnp.bfloat16)
    attended = jnp.einsum('bkgqs,bskd->bqkgd', weights.astype(jnp.float32), value_blocks.astype(jnp.float32))
    return attended.reshape(row_count, kv_heads * group_size * head_width).astype(jnp.bfloat16)

def discretize(decay_rate, rotation, log_step, in_re, in_im):
    time_step = jnp.exp(log_step)[:, None]
    lambda_re = -decay_rate
    lambda_im = rotation
    modulus = jnp.exp(lambda_re * time_step)
    pole_re = modulus * jnp.cos(lambda_im * time_step)
    pole_im = modulus * jnp.sin(lambda_im * time_step)
    minus_one = pole_re - 1.0
    denominator = lambda_re * lambda_re + lambda_im * lambda_im
    factor_re = ((minus_one * lambda_re + pole_im * lambda_im) / denominator)[..., None]
    factor_im = ((pole_im * lambda_re - minus_one * lambda_im) / denominator)[..., None]
    drive_re = factor_re * in_re - factor_im * in_im
    drive_im = factor_re * in_im + factor_im * in_re
    return (pole_re, pole_im, drive_re, drive_im)

def chain_link(earlier, later):
    early_are, early_aim, early_bre, early_bim = earlier
    late_are, late_aim, late_bre, late_bim = later
    return (late_are * early_are - late_aim * early_aim, late_are * early_aim + late_aim * early_are, late_are * early_bre - late_aim * early_bim + late_bre, late_are * early_bim + late_aim * early_bre + late_bim)

def local_states(inputs, pole_re, pole_im, drive_re, drive_im):
    row_count = inputs.shape[0]
    groups, states, group_width = drive_re.shape
    channel_values = inputs.astype(jnp.float32).reshape(row_count, groups, group_width)
    push_re = jnp.einsum('tgh,gph->tgp', channel_values, drive_re, precision=lax.Precision.HIGHEST).reshape(row_count, groups * states)
    push_im = jnp.einsum('tgh,gph->tgp', channel_values, drive_im, precision=lax.Precision.HIGHEST).reshape(row_count, groups * states)
    decay_re = jnp.broadcast_to(pole_re.reshape(1, groups * states), push_re.shape)
    decay_im = jnp.broadcast_to(pole_im.reshape(1, groups * states), push_im.shape)
    return lax.associative_scan(chain_link, (decay_re, decay_im, push_re, push_im), axis=0)

def apply_carry(running, carry_re, carry_im):
    power_re, power_im, own_re, own_im = running
    return (own_re + power_re * carry_re - power_im * carry_im, own_im + power_re * carry_im + power_im * carry_re)

def read_out(inputs, state_re, state_im, out_re, out_im, skip_gain):
    row_count = inputs.shape[0]
    groups, group_width, states = out_re.shape
    grid_re = state_re.reshape(row_count, groups, states)
    grid_im = state_im.reshape(row_count, groups, states)
    summed = jnp.einsum('tgp,ghp->tgh', grid_re, out_re, precision=lax.Precision.HIGHEST) - jnp.einsum('tgp,ghp->tgh', grid_im, out_im, precision=lax.Precision.HIGHEST)
    summed = summed.reshape(row_count, groups * group_width) + skip_gain * inputs.astype(jnp.float32)
    return jax.nn.gelu(summed).astype(jnp.bfloat16)

def reference(tokens, norm_gain, w_query, w_key, w_value, w_state_in, sink_logit, decay_rate, rotation, log_step, in_re, in_im, out_re, out_im, skip_gain, w_attn_out, w_state_out, out_gain):
    wide_tokens = tokens.astype(jnp.float32)
    normed = (wide_tokens * lax.rsqrt(lax.optimization_barrier(jnp.mean(wide_tokens * wide_tokens, axis=-1, keepdims=True)) + epsilon) * norm_gain).astype(jnp.bfloat16)
    positions = jnp.arange(TOKENS, dtype=jnp.int32)
    query_sum = jnp.dot(normed, w_query, preferred_element_type=jnp.float32)
    key_sum = jnp.dot(normed, w_key, preferred_element_type=jnp.float32)
    value_sum = jnp.dot(normed, w_value, preferred_element_type=jnp.float32)
    queries, key_rows, value_rows = shape_heads(query_sum, key_sum, value_sum, positions, HEAD)
    inputs = jnp.dot(normed, w_state_in, preferred_element_type=jnp.float32).astype(jnp.bfloat16)
    padded_keys = jnp.concatenate([jnp.zeros((WINDOW, KVH * HEAD), jnp.bfloat16), key_rows], axis=0)
    padded_values = jnp.concatenate([jnp.zeros((WINDOW, KVH * HEAD), jnp.bfloat16), value_rows], axis=0)

    def span_attend(span_index):
        first_row = (span_index * TOK_DEV).astype(jnp.int32)
        span_queries = lax.dynamic_slice_in_dim(queries, first_row, TOK_DEV, 0)
        span_keys = lax.dynamic_slice_in_dim(padded_keys, first_row, TOK_DEV + WINDOW, 0).reshape(TOK_DEV + WINDOW, KVH, HEAD)
        span_values = lax.dynamic_slice_in_dim(padded_values, first_row, TOK_DEV + WINDOW, 0).reshape(TOK_DEV + WINDOW, KVH, HEAD)
        return band_attention(span_queries, span_keys, span_values, sink_logit, first_row, WINDOW)
    attended = lax.map(span_attend, jnp.arange(N_SP, dtype=jnp.int32)).reshape(TOKENS, ATTN)
    pole_re, pole_im, drive_re, drive_im = discretize(decay_rate, rotation, log_step, in_re, in_im)
    spans = inputs.reshape(N_SP, TOK_DEV, ATTN)

    def span_step(carried, span_inputs):
        running = local_states(span_inputs, pole_re, pole_im, drive_re, drive_im)
        state_re, state_im = apply_carry(running, carried[0], carried[1])
        out_rows = read_out(span_inputs, state_re, state_im, out_re, out_im, skip_gain)
        return ((state_re[-1], state_im[-1]), out_rows)
    start_state = (jnp.zeros((GROUPS * STATE,), jnp.float32), jnp.zeros((GROUPS * STATE,), jnp.float32))
    final_state, mixed_spans = lax.scan(span_step, start_state, spans)
    mixed_state = mixed_spans.reshape(TOKENS, ATTN)
    block_width = ATTN // N_TP
    projected = jnp.zeros((TOKENS, D), jnp.float32)
    for block_index in range(N_TP):
        low = block_index * block_width
        partial_term = jnp.dot(attended[:, low:low + block_width], w_attn_out[low:low + block_width], preferred_element_type=jnp.float32) + jnp.dot(mixed_state[:, low:low + block_width], w_state_out[low:low + block_width], preferred_element_type=jnp.float32)
        rounded = lax.optimization_barrier(partial_term.astype(jnp.bfloat16))
        projected = projected + rounded.astype(jnp.float32)
    row_scale = lax.rsqrt(lax.optimization_barrier(jnp.mean(projected * projected, axis=-1, keepdims=True)) + epsilon)
    return (projected * row_scale * out_gain).astype(jnp.bfloat16)
```

```python
import math

import jax
import jax.numpy as jnp
import numpy as np
from jax import lax
from jax.experimental import pallas as pl
from jax.experimental.pallas import tpu as pltpu
from jax.sharding import PartitionSpec as P

HEAD = 64
WINDOW = 128
SUB = 8


epsilon = 1e-06
rotary_base = 500000.0


def passed_along(value, axis, by):
    size = lax.axis_size(axis)
    pairs = [(i, i + by) for i in range(size) if 0 <= i + by < size]
    return lax.ppermute(value, axis, pairs)


def rotate(heads_block, positions):
    head_width = heads_block.shape[-1]
    half_width = head_width // 2
    frequency = rotary_base ** (-(jnp.arange(half_width, dtype=jnp.float32) * 2.0 / head_width))
    angles = positions.astype(jnp.float32)[:, None] * frequency[None, :]
    cosine = jnp.cos(angles)[:, None, :]
    sine_part = jnp.sin(angles)[:, None, :]
    lower_half = heads_block[..., :half_width]
    upper_half = heads_block[..., half_width:]
    return jnp.concatenate(
        [
            lower_half * cosine - upper_half * sine_part,
            upper_half * cosine + lower_half * sine_part,
        ],
        axis=-1,
    )


def shape_heads(query_sum, key_sum, value_sum, positions, head_width):
    row_count = query_sum.shape[0]
    kv_heads = key_sum.shape[1] // head_width
    group_size = query_sum.shape[1] // key_sum.shape[1]
    queries = rotate(
        query_sum.reshape(row_count, kv_heads * group_size, head_width), positions
    ).astype(jnp.bfloat16)
    queries = queries.reshape(row_count, kv_heads, group_size, head_width)
    key_rows = rotate(key_sum.reshape(row_count, kv_heads, head_width), positions).astype(
        jnp.bfloat16
    )
    key_rows = key_rows.reshape(row_count, kv_heads * head_width)
    value_rows = value_sum.astype(jnp.bfloat16)
    return (queries, key_rows, value_rows)


def band_attention(queries, key_rows, value_rows, sink_logit, first_row, window):
    row_count, kv_heads, group_size, head_width = queries.shape
    blocks = row_count // window
    query_blocks = queries.reshape(blocks, window, kv_heads, group_size, head_width)
    key_blocks = jnp.concatenate(
        [
            key_rows[:row_count].reshape(blocks, window, kv_heads, head_width),
            key_rows[window:].reshape(blocks, window, kv_heads, head_width),
        ],
        axis=1,
    )
    value_blocks = jnp.concatenate(
        [
            value_rows[:row_count].reshape(blocks, window, kv_heads, head_width),
            value_rows[window:].reshape(blocks, window, kv_heads, head_width),
        ],
        axis=1,
    )
    scores = jnp.einsum(
        "bqkgd,bskd->bkgqs", query_blocks, key_blocks, preferred_element_type=jnp.float32
    ) / math.sqrt(head_width)
    block_start = jnp.arange(blocks, dtype=jnp.int32)[:, None, None] * window
    query_at = first_row + block_start + jnp.arange(window, dtype=jnp.int32)[None, :, None]
    key_at = (
        first_row - window + block_start + jnp.arange(2 * window, dtype=jnp.int32)[None, None, :]
    )
    offset_gap = query_at - key_at
    visible = (offset_gap >= 0) & (offset_gap < window) & (key_at >= 0)
    scores = jnp.where(visible[:, None, None, :, :], scores, -jnp.inf)
    sink_value = sink_logit.reshape(1, kv_heads, group_size, 1, 1)
    top_score = jnp.maximum(jnp.max(scores, axis=-1, keepdims=True), sink_value)
    exponent = jnp.exp(scores - top_score)
    totals = jnp.sum(exponent, axis=-1, keepdims=True) + jnp.exp(sink_value - top_score)
    weights = (exponent / totals).astype(jnp.bfloat16)
    attended = jnp.einsum(
        "bkgqs,bskd->bqkgd", weights, value_blocks, preferred_element_type=jnp.float32
    )
    return attended.reshape(row_count, kv_heads * group_size * head_width).astype(jnp.bfloat16)


def discretize(decay_rate, rotation, log_step, in_re, in_im):
    time_step = jnp.exp(log_step)[:, None]
    lambda_re = -decay_rate
    modulus = jnp.exp(lambda_re * time_step)
    pole_re = modulus * jnp.cos(rotation * time_step)
    pole_im = modulus * jnp.sin(rotation * time_step)
    minus_one = pole_re - 1.0
    denominator = lambda_re * lambda_re + rotation * rotation
    factor_re = ((minus_one * lambda_re + pole_im * rotation) / denominator)[..., None]
    factor_im = ((pole_im * lambda_re - minus_one * rotation) / denominator)[..., None]
    drive_re = factor_re * in_re - factor_im * in_im
    drive_im = factor_re * in_im + factor_im * in_re
    return (pole_re, pole_im, drive_re, drive_im)


def complex_power(decay_rate, rotation, log_step, exponent):
    time_step = jnp.exp(log_step)[:, None]
    modulus = jnp.exp(-decay_rate * time_step * exponent)
    angle = rotation * time_step * exponent
    return (modulus * jnp.cos(angle), modulus * jnp.sin(angle))


def token_shuffle(rows, inverse):
    steps = rows // SUB
    out_row = lax.broadcasted_iota(jnp.int32, (rows, rows), 1 if inverse else 0)
    in_row = lax.broadcasted_iota(jnp.int32, (rows, rows), 0 if inverse else 1)
    token = (out_row % SUB) * steps + out_row // SUB
    return (token == in_row).astype(jnp.bfloat16)


def scan_kernel(
    u_ref, drive_ref, pole_re_ref, pole_im_ref, jump_re_ref, jump_im_ref,
    state_ref, carry_re_ref, carry_im_ref, end_re_ref, end_im_ref,
):
    rows = u_ref.shape[0]
    width = pole_re_ref.shape[-1]
    shuffle = token_shuffle(rows, False)
    shuffled = jnp.dot(shuffle, u_ref[...], preferred_element_type=jnp.float32)
    state_ref[...] = jnp.dot(
        shuffled, drive_ref[0], precision=lax.Precision.HIGHEST,
        preferred_element_type=jnp.float32,
    )
    pole_re = jnp.broadcast_to(pole_re_ref[0], (SUB, width))
    pole_im = jnp.broadcast_to(pole_im_ref[0], (SUB, width))
    now_re = jnp.zeros((SUB, width), jnp.float32)
    now_im = jnp.zeros((SUB, width), jnp.float32)
    for step in range(rows // SUB):
        at = slice(step * SUB, (step + 1) * SUB)
        new_re = pole_re * now_re - pole_im * now_im + state_ref[at, :width]
        new_im = pole_re * now_im + pole_im * now_re + state_ref[at, width:]
        state_ref[at, :width] = new_re
        state_ref[at, width:] = new_im
        now_re, now_im = new_re, new_im
    jump_re, jump_im = (jump_re_ref[0], jump_im_ref[0])
    held_re = jnp.zeros((1, width), jnp.float32)
    held_im = jnp.zeros((1, width), jnp.float32)
    for chunk in range(SUB):
        carry_re_ref[chunk : chunk + 1, :] = held_re
        carry_im_ref[chunk : chunk + 1, :] = held_im
        next_re = jump_re * held_re - jump_im * held_im + now_re[chunk : chunk + 1]
        next_im = jump_re * held_im + jump_im * held_re + now_im[chunk : chunk + 1]
        held_re, held_im = next_re, next_im
    end_re_ref[0] = held_re
    end_im_ref[0] = held_im


def readout_kernel(
    u_ref, state_ref, carry_re_ref, carry_im_ref, prior_re_ref, prior_im_ref,
    chunk_re_ref, chunk_im_ref, pole_re_ref, pole_im_ref, read_ref, skip_ref, out_ref, full_ref,
):
    rows = u_ref.shape[0]
    width = pole_re_ref.shape[-1]
    prior_re, prior_im = (prior_re_ref[0], prior_im_ref[0])
    chunk_re, chunk_im = (chunk_re_ref[...], chunk_im_ref[...])
    add_re = carry_re_ref[...] + chunk_re * prior_re - chunk_im * prior_im
    add_im = carry_im_ref[...] + chunk_re * prior_im + chunk_im * prior_re
    pole_re = jnp.broadcast_to(pole_re_ref[0], (SUB, width))
    pole_im = jnp.broadcast_to(pole_im_ref[0], (SUB, width))
    for step in range(rows // SUB):
        at = slice(step * SUB, (step + 1) * SUB)
        turned_re = pole_re * add_re - pole_im * add_im
        turned_im = pole_re * add_im + pole_im * add_re
        full_ref[at, :width] = state_ref[at, :width] + turned_re
        full_ref[at, width:] = state_ref[at, width:] + turned_im
        add_re, add_im = turned_re, turned_im
    summed = jnp.dot(
        full_ref[...], read_ref[0], precision=lax.Precision.HIGHEST,
        preferred_element_type=jnp.float32,
    )
    shuffled = jnp.dot(
        token_shuffle(rows, False), u_ref[...], preferred_element_type=jnp.float32
    )
    mixed = jax.nn.gelu(summed + skip_ref[...] * shuffled).astype(jnp.bfloat16)
    out_ref[...] = jnp.dot(
        token_shuffle(rows, True), mixed, preferred_element_type=jnp.float32
    ).astype(jnp.bfloat16)


def block_diagonal(parts):
    blocks, per, rows, columns = parts[0].shape
    same = jnp.eye(per, dtype=bool)[None, :, None, :, None]
    spread = [
        jnp.where(same, part[:, :, :, None, :], 0.0).reshape(blocks, per * rows, per * columns)
        for part in parts
    ]
    return jnp.concatenate(spread, axis=2)


def state_tables(rows, decay_rate, rotation, log_step, in_re, in_im, out_re, out_im):
    groups, states = decay_rate.shape
    group_width = in_re.shape[-1]
    per = min(groups, max(1, 128 // group_width))
    blocks, width = (groups // per, per * states)
    pole_re, pole_im, drive_re, drive_im = discretize(decay_rate, rotation, log_step, in_re, in_im)
    steps = rows // SUB

    def by_block(value):
        return value.reshape(blocks, per, *value.shape[1:])

    def flat(value):
        return value.reshape(blocks, 1, width)

    drive = block_diagonal(
        [by_block(jnp.swapaxes(drive_re, 1, 2)), by_block(jnp.swapaxes(drive_im, 1, 2))]
    )
    read = jnp.swapaxes(block_diagonal([by_block(out_re), by_block(-out_im)]), 1, 2)
    jump = complex_power(decay_rate, rotation, log_step, float(steps))
    chunk_powers = [
        complex_power(decay_rate, rotation, log_step, float(steps * c)) for c in range(SUB)
    ]
    chunk_re = jnp.stack([p[0].reshape(groups * states) for p in chunk_powers])
    chunk_im = jnp.stack([p[1].reshape(groups * states) for p in chunk_powers])
    return dict(
        drive=drive, read=read, pole_re=flat(pole_re), pole_im=flat(pole_im),
        jump_re=flat(jump[0]), jump_im=flat(jump[1]), chunk_re=chunk_re, chunk_im=chunk_im,
        blocks=blocks, width=width, channels=per * group_width,
    )


def local_scan(inputs, tables):
    rows = inputs.shape[0]
    blocks, width, channels = (tables["blocks"], tables["width"], tables["channels"])
    row_spec = pl.BlockSpec((1, 1, width), lambda b: (b, 0, 0))
    carry_spec = pl.BlockSpec((SUB, width), lambda b: (0, b))
    return pl.pallas_call(
        scan_kernel,
        grid=(blocks,),
        in_specs=[
            pl.BlockSpec((rows, channels), lambda b: (0, b)),
            pl.BlockSpec((1, channels, 2 * width), lambda b: (b, 0, 0)),
            row_spec, row_spec, row_spec, row_spec,
        ],
        out_specs=[
            pl.BlockSpec((rows, 2 * width), lambda b: (0, b)),
            carry_spec, carry_spec, row_spec, row_spec,
        ],
        out_shape=[
            jax.ShapeDtypeStruct((rows, 2 * width * blocks), jnp.float32),
            jax.ShapeDtypeStruct((SUB, width * blocks), jnp.float32),
            jax.ShapeDtypeStruct((SUB, width * blocks), jnp.float32),
            jax.ShapeDtypeStruct((blocks, 1, width), jnp.float32),
            jax.ShapeDtypeStruct((blocks, 1, width), jnp.float32),
        ],
        cost_estimate=pl.CostEstimate(
            flops=12 * rows * channels * width * blocks, bytes_accessed=10**7, transcendentals=0
        ),
    )(
        inputs, tables["drive"], tables["pole_re"], tables["pole_im"],
        tables["jump_re"], tables["jump_im"],
    )


def read_states(inputs, scanned, prior_re, prior_im, tables, skip_gain):
    rows = inputs.shape[0]
    state, carry_re, carry_im = scanned[:3]
    blocks, width, channels = (tables["blocks"], tables["width"], tables["channels"])
    row_spec = pl.BlockSpec((1, 1, width), lambda b: (b, 0, 0))
    carry_spec = pl.BlockSpec((SUB, width), lambda b: (0, b))
    return pl.pallas_call(
        readout_kernel,
        grid=(blocks,),
        in_specs=[
            pl.BlockSpec((rows, channels), lambda b: (0, b)),
            pl.BlockSpec((rows, 2 * width), lambda b: (0, b)),
            carry_spec, carry_spec, row_spec, row_spec, carry_spec, carry_spec,
            row_spec, row_spec,
            pl.BlockSpec((1, 2 * width, channels), lambda b: (b, 0, 0)),
            pl.BlockSpec((1, channels), lambda b: (0, b)),
        ],
        out_specs=pl.BlockSpec((rows, channels), lambda b: (0, b)),
        out_shape=jax.ShapeDtypeStruct((rows, channels * blocks), jnp.bfloat16),
        scratch_shapes=[pltpu.VMEM((rows, 2 * width), jnp.float32)],
        cost_estimate=pl.CostEstimate(
            flops=12 * rows * channels * width * blocks, bytes_accessed=10**7, transcendentals=0
        ),
    )(
        inputs, state, carry_re, carry_im, prior_re, prior_im,
        tables["chunk_re"], tables["chunk_im"], tables["pole_re"], tables["pole_im"],
        tables["read"], skip_gain.reshape(1, -1),
    )


def carried_state(end_re, end_im, decay_rate, rotation, log_step, rows):
    ends = jnp.stack([end_re, end_im])
    shape = end_re.shape
    size = lax.axis_size("sp")
    reach = 1
    while reach < size:
        power_re, power_im = complex_power(decay_rate, rotation, log_step, float(rows * reach))
        power_re, power_im = (power_re.reshape(shape), power_im.reshape(shape))
        prior = passed_along(ends, "sp", reach)
        ends = ends + jnp.stack(
            [
                power_re * prior[0] - power_im * prior[1],
                power_re * prior[1] + power_im * prior[0],
            ]
        )
        reach *= 2
    before = passed_along(ends, "sp", 1)
    return (before[0], before[1])


def state_branch(inputs, decay_rate, rotation, log_step, in_re, in_im, out_re, out_im, skip_gain):
    rows = inputs.shape[0]
    tables = state_tables(rows, decay_rate, rotation, log_step, in_re, in_im, out_re, out_im)
    scanned = local_scan(inputs, tables)
    prior_re, prior_im = carried_state(
        scanned[3], scanned[4], decay_rate, rotation, log_step, rows
    )
    return read_states(inputs, scanned, prior_re, prior_im, tables, skip_gain)


def earlier_window(key_rows, value_rows):
    joined = jnp.concatenate([key_rows, value_rows], axis=1)
    prior = passed_along(joined, "sp", 1)
    return jnp.concatenate([prior, joined], axis=0)


def make_adder(normed_cols):

    def add_pieces(carried, weight_pieces, row_start):
        updated = []
        for running_total, weight_piece in zip(carried, weight_pieces):
            product = lax.dot_general(
                normed_cols,
                weight_piece,
                (((0,), (0,)), ((), ())),
                preferred_element_type=jnp.float32,
            )
            updated.append(product)
        return tuple(updated)

    return add_pieces


def whole_weights_body(
    tokens,
    norm_gain,
    w_query,
    w_key,
    w_value,
    w_state_in,
    sink_logit,
    decay_rate,
    rotation,
    log_step,
    in_re,
    in_im,
    out_re,
    out_im,
    skip_gain,
    w_attn_out,
    w_state_out,
    out_gain,
):
    row_count = tokens.shape[0]
    window = WINDOW
    head_width = HEAD
    wide_tokens = tokens.astype(jnp.float32)
    normed = (
        wide_tokens
        * lax.rsqrt(jnp.mean(wide_tokens * wide_tokens, axis=-1, keepdims=True) + epsilon)
        * norm_gain
    ).astype(jnp.bfloat16)
    first_row = lax.axis_index("sp") * row_count
    positions = first_row + jnp.arange(row_count, dtype=jnp.int32)
    add_pieces = make_adder(jnp.transpose(normed))

    def empty_like(weight_shard):
        return jnp.zeros((row_count, weight_shard.shape[1]), jnp.float32)

    query_sum, key_sum, value_sum, input_sum = add_pieces(
        (empty_like(w_query), empty_like(w_key), empty_like(w_value), empty_like(w_state_in)),
        (
            lax.all_gather(w_query, "sp", axis=0, tiled=True),
            lax.all_gather(w_key, "sp", axis=0, tiled=True),
            lax.all_gather(w_value, "sp", axis=0, tiled=True),
            lax.all_gather(w_state_in, "sp", axis=0, tiled=True),
        ),
        jnp.int32(0),
    )
    queries, key_rows, value_rows = shape_heads(
        query_sum, key_sum, value_sum, positions, head_width
    )
    joined_rows = earlier_window(key_rows, value_rows)
    inputs = input_sum.astype(jnp.bfloat16)
    mixed_state = state_branch(
        inputs, decay_rate, rotation, log_step, in_re, in_im, out_re, out_im, skip_gain
    )
    kv_width = key_rows.shape[1]
    kv_heads = kv_width // head_width
    all_keys = joined_rows[:, :kv_width].reshape(window + row_count, kv_heads, head_width)
    all_values = joined_rows[:, kv_width:].reshape(window + row_count, kv_heads, head_width)
    attended = band_attention(queries, all_keys, all_values, sink_logit, first_row, window)
    attn_rows, state_rows = (
        lax.all_gather(w_attn_out, "sp", axis=1, tiled=True),
        lax.all_gather(w_state_out, "sp", axis=1, tiled=True),
    )
    projected = lax.psum_scatter(
        (
            jnp.dot(attended, attn_rows, preferred_element_type=jnp.float32)
            + jnp.dot(mixed_state, state_rows, preferred_element_type=jnp.float32)
        ).astype(jnp.bfloat16),
        "tp",
        scatter_dimension=0,
        tiled=True,
    ).astype(jnp.float32)
    row_scale = lax.rsqrt(jnp.mean(projected * projected, axis=-1, keepdims=True) + epsilon)
    return (projected * row_scale * out_gain).astype(jnp.bfloat16)


SIDE = 2
PLANE = SIDE * SIDE
CORES = 2
LANES = 128
MESH = pl.DeviceIdType.MESH


def place():
    me = lax.axis_index("sp")
    return (lax.div(me, PLANE), lax.rem(me, PLANE), lax.axis_index("tp"))


def plane_neighbours(spot):
    beside = spot + 1 - 2 * lax.rem(spot, SIDE)
    above = spot + SIDE - 2 * SIDE * lax.div(spot, SIDE)
    return (beside, above)


def greet(layers, layer, spot, core):
    barrier = pltpu.get_barrier_semaphore()
    beside, above = plane_neighbours(spot)
    for ahead in range(1, layers):
        other = lax.rem(layer + ahead, layers)
        pl.semaphore_signal(
            barrier, inc=1, device_id={"sp": other * PLANE + spot}, device_id_type=MESH
        )
    for other in (beside, above):
        pl.semaphore_signal(
            barrier, inc=1, device_id={"sp": layer * PLANE + other}, device_id_type=MESH
        )
    pl.semaphore_signal(barrier, inc=1, device_id={"tp": 1 - core}, device_id_type=MESH)
    pl.semaphore_wait(barrier, layers + 2)


def remote(source, target, send_sem, recv_sem, device):
    return pltpu.make_async_remote_copy(
        src_ref=source, dst_ref=target, send_sem=send_sem, recv_sem=recv_sem,
        device_id=device, device_id_type=MESH,
    )


def line_first(layers, layer, spot, source, held, send_sems, recv_sems):
    @pl.when(layer < layers - 1)
    def _():
        remote(
            source, held.at[layer], send_sems.at[0, 0], recv_sems.at[0, 0],
            {"sp": (layer + 1) * PLANE + spot},
        ).start()

    @pl.when(layer > 0)
    def _():
        remote(
            source, held.at[layer], send_sems.at[1, 0], recv_sems.at[1, 0],
            {"sp": (layer - 1) * PLANE + spot},
        ).start()


def line_pass(layers, layer, spot, hop, held, send_sems, recv_sems, landed=None):
    @pl.when(layer - hop >= 0)
    def _():
        block = held.at[layer - hop]
        remote(block, block, send_sems.at[0, 0], recv_sems.at[0, hop - 1], {"sp": 0}).wait_recv()

        @pl.when(layer < layers - 1)
        def _():
            if hop < layers - 1:
                remote(
                    block, block, send_sems.at[0, hop], recv_sems.at[0, hop],
                    {"sp": (layer + 1) * PLANE + spot},
                ).start()

        if landed is not None:
            landed(0, hop, block)

    @pl.when(layer + hop <= layers - 1)
    def _():
        block = held.at[layer + hop]
        remote(block, block, send_sems.at[1, 0], recv_sems.at[1, hop - 1], {"sp": 0}).wait_recv()

        @pl.when(layer > 0)
        def _():
            if hop < layers - 1:
                remote(
                    block, block, send_sems.at[1, hop], recv_sems.at[1, hop],
                    {"sp": (layer - 1) * PLANE + spot},
                ).start()

        if landed is not None:
            landed(1, hop, block)


def line_drain(layers, layer, source, held, send_sems, recv_sems):
    for hop in range(layers - 1):

        @pl.when((layer - hop >= 0) & (layer < layers - 1))
        def _():
            remote(
                source, held.at[layer], send_sems.at[0, hop], recv_sems.at[0, 0], {"sp": 0}
            ).wait_send()

        @pl.when((layer + hop <= layers - 1) & (layer > 0))
        def _():
            remote(
                source, held.at[layer], send_sems.at[1, hop], recv_sems.at[1, 0], {"sp": 0}
            ).wait_send()


def plane_first(halves, slots, layer, spot, send_sems, recv_sems):
    beside, above = plane_neighbours(spot)
    copies = []
    for half in (0, 1):
        copies.append(
            remote(
                halves.at[half], slots.at[spot, half], send_sems.at[0, half],
                recv_sems.at[0, half], {"sp": layer * PLANE + beside},
            )
        )
        copies.append(
            remote(
                halves.at[1 - half], slots.at[spot, 1 - half], send_sems.at[1, 1 - half],
                recv_sems.at[1, 1 - half], {"sp": layer * PLANE + above},
            )
        )
    for copy in copies:
        copy.start()


def plane_pass(slots, layer, spot, send_sems, recv_sems):
    beside, above = plane_neighbours(spot)
    block = slots.at[beside, 0]
    remote(block, block, send_sems.at[0, 0], recv_sems.at[0, 0], {"sp": 0}).wait_recv()
    remote(
        block, block, send_sems.at[1, 2], recv_sems.at[1, 2], {"sp": layer * PLANE + above}
    ).start()
    block = slots.at[above, 1]
    remote(block, block, send_sems.at[0, 0], recv_sems.at[1, 1], {"sp": 0}).wait_recv()
    remote(
        block, block, send_sems.at[0, 2], recv_sems.at[0, 2], {"sp": layer * PLANE + beside}
    ).start()


def plane_landed(slots, spot, send_sems, recv_sems):
    for way, half in ((0, 1), (1, 0), (0, 2), (1, 2)):
        block = slots.at[spot, 0]
        remote(block, block, send_sems.at[0, 0], recv_sems.at[way, half], {"sp": 0}).wait_recv()
    for way in (0, 1):
        for half in (0, 1, 2):
            block = slots.at[spot, 0]
            remote(block, block, send_sems.at[way, half], recv_sems.at[0, 0], {"sp": 0}).wait_send()


def project_kernel(
    packed_ref, normed_ref, row_cos_ref, row_sin_ref, block_cos_ref, block_sin_ref,
    query_ref, pair_ref, input_ref,
    weights, held, far_send, far_recv, line_send, line_recv, part_send, part_recv,
    side_send, side_recv, own_sem,
):
    layers = packed_ref.shape[0]
    layer, spot, core = place()
    greet(layers, layer, spot, core)
    for ahead in range(1, layers):
        other = lax.rem(layer + ahead, layers)
        remote(
            packed_ref.at[other], weights.at[layer, spot], far_send.at[ahead], far_recv.at[ahead],
            {"sp": other * PLANE + spot},
        ).start()
    plane_first(
        packed_ref.at[layer], weights.at[layer], layer, spot, side_send.at[0], side_recv.at[0]
    )
    own_weights = pltpu.make_async_copy(
        packed_ref.at[layer], weights.at[layer, spot], own_sem.at[0]
    )
    own_tokens = pltpu.make_async_copy(normed_ref, held.at[layer], own_sem.at[1])
    own_weights.start()
    own_tokens.start()
    mine = held.at[:, core]
    line_first(layers, layer, spot, normed_ref.at[core], mine, line_send, line_recv)

    def to_partner(way, hop, block):
        remote(
            block, block, part_send.at[way, hop - 1], part_recv.at[way, hop - 1], {"tp": 1 - core}
        ).start()

    for ahead in range(layers):
        origin = lax.rem(layer + layers - ahead, layers)
        if ahead > 0:
            block = weights.at[origin, spot]
            remote(block, block, far_send.at[ahead], far_recv.at[ahead], {"sp": 0}).wait_recv()
            plane_first(
                block, weights.at[origin], layer, spot, side_send.at[ahead], side_recv.at[ahead]
            )
        plane_pass(weights.at[origin], layer, spot, side_send.at[ahead], side_recv.at[ahead])
    for hop in range(1, layers):
        line_pass(layers, layer, spot, hop, mine, line_send, line_recv, to_partner)
    own_weights.wait()
    own_tokens.wait()
    for ahead in range(layers):
        origin = lax.rem(layer + layers - ahead, layers)
        plane_landed(weights.at[origin], spot, side_send.at[ahead], side_recv.at[ahead])
    line_drain(layers, layer, normed_ref.at[core], mine, line_send, line_recv)
    for hop in range(1, layers):
        for way, there in ((0, layer - hop >= 0), (1, layer + hop <= layers - 1)):

            @pl.when(there)
            def _():
                block = held.at[layer, 0]
                copy = remote(
                    block, block, part_send.at[way, hop - 1], part_recv.at[way, hop - 1],
                    {"tp": 1 - core},
                )
                copy.wait_send()
                copy.wait_recv()

    for ahead in range(1, layers):
        block = weights.at[layer, spot]
        remote(block, block, far_send.at[ahead], far_recv.at[ahead], {"sp": 0}).wait_send()

    rows = held.shape[1] * held.shape[2]
    depth = weights.shape[2] * weights.shape[3]
    query_width, pair_width = (query_ref.shape[-1], pair_ref.shape[-1])
    half_width = HEAD // 2
    lane = lax.broadcasted_iota(jnp.int32, (rows, LANES), 1)
    low = lax.rem(lane, HEAD) < half_width

    def turn(value, cosine, sine):
        swapped = jnp.where(
            low, -pltpu.roll(value, LANES - half_width, 1), pltpu.roll(value, half_width, 1)
        )
        return value * cosine + swapped * sine

    @pl.loop(0, layers)
    def _(block):
        total = None
        for at in range(layers * PLANE):
            piece = jnp.dot(
                held[block, :, :, at * depth : (at + 1) * depth].reshape(rows, depth),
                weights[at // PLANE, at % PLANE].reshape(depth, weights.shape[-1]),
                preferred_element_type=jnp.float32,
            )
            total = piece if total is None else total + piece
        here = pl.ds(block * PLANE + spot, 1)
        block_cos, block_sin = (block_cos_ref[here, :], block_sin_ref[here, :])
        cosine = row_cos_ref[...] * block_cos - row_sin_ref[...] * block_sin
        sine = row_sin_ref[...] * block_cos + row_cos_ref[...] * block_sin
        turned = [
            turn(total[:, at : at + LANES], cosine, sine) for at in range(0, query_width, LANES)
        ]
        query_ref[block] = jnp.concatenate(turned, axis=1).astype(jnp.bfloat16)
        pairs = []
        for at in range(query_width, query_width + pair_width, LANES):
            value = total[:, at : at + LANES]
            pairs.append(jnp.where(lane < HEAD, turn(value, cosine, sine), value))
        pair_ref[block] = jnp.concatenate(pairs, axis=1).astype(jnp.bfloat16)
        input_ref[block] = total[:, query_width + pair_width :].astype(jnp.bfloat16)


def project(packed, normed, query_width, pair_width):
    layers, _, half_depth, width = packed.shape
    rows, model = normed.shape
    half = HEAD // 2
    frequency = rotary_base ** (-(np.arange(half) * 2.0 / HEAD))
    frequency = np.tile(frequency, LANES // half)[None, :]
    within = np.arange(rows)[:, None] * frequency
    across = (np.arange(layers * PLANE) * rows)[:, None] * frequency
    tables = [np.cos(within), np.sin(within), np.cos(across), np.sin(across)]
    tables = [jnp.asarray(t, jnp.float32) for t in tables]
    anywhere = pl.BlockSpec(memory_space=pl.ANY)
    vmem = pl.BlockSpec(memory_space=pltpu.VMEM)
    input_width = width - query_width - pair_width
    dma = pltpu.SemaphoreType.DMA
    return pl.pallas_call(
        project_kernel,
        out_shape=[
            jax.ShapeDtypeStruct((layers, rows, query_width), jnp.bfloat16),
            jax.ShapeDtypeStruct((layers, rows, pair_width), jnp.bfloat16),
            jax.ShapeDtypeStruct((layers, rows, input_width), jnp.bfloat16),
        ],
        in_specs=[anywhere, anywhere] + [vmem] * 4,
        out_specs=[vmem] * 3,
        scratch_shapes=[
            pltpu.VMEM((layers, PLANE, 2, half_depth, width), jnp.bfloat16),
            pltpu.VMEM((layers, CORES, rows // CORES, model), jnp.bfloat16),
            dma((layers,)), dma((layers,)),
            dma((2, layers)), dma((2, layers)), dma((2, layers)), dma((2, layers)),
            dma((layers, 2, 3)), dma((layers, 2, 3)), dma((2,)),
        ],
        compiler_params=pltpu.CompilerParams(
            collective_id=0, has_side_effects=True, vmem_limit_bytes=48 * 2**20
        ),
    )(packed, normed.reshape(CORES, rows // CORES, model), *tables)


def attend_kernel(query_ref, pair_ref, before_ref, sink_ref, out_ref):
    block = pl.program_id(0)
    layer, spot, core = place()
    rows, query_width = query_ref.shape[1:]
    group = query_width // HEAD
    pair, before = (pair_ref[0], before_ref[0])
    keys = jnp.concatenate([before[:, :HEAD], pair[:, :HEAD]], axis=0)
    values = jnp.concatenate([before[:, HEAD:], pair[:, HEAD:]], axis=0)
    query_at = lax.broadcasted_iota(jnp.int32, (rows, rows + WINDOW), 0)
    key_at = lax.broadcasted_iota(jnp.int32, (rows, rows + WINDOW), 1) - WINDOW
    gap = query_at - key_at
    first = (block * PLANE + spot) * rows
    visible = (gap >= 0) & (gap < WINDOW) & (key_at + first >= 0)
    out = []
    for head in range(group):
        query = query_ref[0, :, head * HEAD : (head + 1) * HEAD]
        scores = lax.dot_general(
            query, keys, (((1,), (1,)), ((), ())), preferred_element_type=jnp.float32
        ) / math.sqrt(HEAD)
        scores = jnp.where(visible, scores, -jnp.inf)
        sink = sink_ref[0:1, head : head + 1]
        top = jnp.maximum(jnp.max(scores, axis=-1, keepdims=True), sink)
        exponent = jnp.exp(scores - top)
        total = jnp.sum(exponent, axis=-1, keepdims=True) + jnp.exp(sink - top)
        weights = (exponent / total).astype(jnp.bfloat16)
        out.append(jnp.dot(weights, values, preferred_element_type=jnp.float32))
    out_ref[0] = jnp.concatenate(out, axis=1).astype(jnp.bfloat16)


def attend(queries, pairs, before, sink):
    layers, rows, query_width = queries.shape
    pair_width = pairs.shape[-1]
    flops = 4 * layers * rows * (rows + WINDOW) * query_width
    return pl.pallas_call(
        attend_kernel,
        grid=(layers,),
        in_specs=[
            pl.BlockSpec((1, rows, query_width), lambda b: (b, 0, 0)),
            pl.BlockSpec((1, rows, pair_width), lambda b: (b, 0, 0)),
            pl.BlockSpec((1, rows, pair_width), lambda b: (b, 0, 0)),
            pl.BlockSpec((1, sink.shape[-1]), lambda b: (0, 0)),
        ],
        out_specs=pl.BlockSpec((1, rows, query_width), lambda b: (b, 0, 0)),
        out_shape=jax.ShapeDtypeStruct((layers, rows, query_width), jnp.bfloat16),
        cost_estimate=pl.CostEstimate(flops=flops, bytes_accessed=10**6, transcendentals=0),
    )(queries, pairs, before, sink)


def output_kernel(
    attended_ref, mixed_ref, attn_out_ref, state_out_ref, gain_ref, out_ref,
    weights, held, partial, arrived, summed, pieces,
    line_send, line_recv, side_send, side_recv, own_sem, half_sem, far_send, far_recv,
):
    layers = held.shape[0]
    layer, spot, core = place()
    greet(layers, layer, spot, core)
    sources = (attended_ref, mixed_ref)
    matrices = (attn_out_ref, state_out_ref)
    for kind in (0, 1):
        line_first(
            layers, layer, spot, sources[kind], held.at[:, kind], line_send.at[kind],
            line_recv.at[kind],
        )
    own = []
    for kind in (0, 1):
        plane_first(
            matrices[kind], weights.at[kind], layer, spot, side_send.at[kind], side_recv.at[kind]
        )
        own.append(
            pltpu.make_async_copy(matrices[kind], weights.at[kind, spot], own_sem.at[kind])
        )
        own.append(
            pltpu.make_async_copy(sources[kind], held.at[layer, kind], own_sem.at[2 + kind])
        )
    for copy in own:
        copy.start()
    for hop in range(1, layers):
        if hop < 3:
            plane_pass(
                weights.at[hop - 1], layer, spot, side_send.at[hop - 1], side_recv.at[hop - 1]
            )
        for kind in (0, 1):
            line_pass(
                layers, layer, spot, hop, held.at[:, kind], line_send.at[kind], line_recv.at[kind]
            )
    for copy in own:
        copy.wait()
    for kind in (0, 1):
        plane_landed(weights.at[kind], spot, side_send.at[kind], side_recv.at[kind])
        line_drain(
            layers, layer, sources[kind], held.at[:, kind], line_send.at[kind], line_recv.at[kind]
        )
    depth = held.shape[-1]
    tokens = held.shape[2] * held.shape[3]
    half_depth, width = weights.shape[3:]
    rows = partial.shape[2]

    @pl.loop(0, PLANE)
    def _(block):
        total = None
        for at in range(layers):
            for kind in (0, 1):
                low = at * depth
                piece = jnp.dot(
                    held[at, kind].reshape(tokens, depth),
                    weights[kind, block, low // half_depth, pl.ds(low % half_depth, depth), :],
                    preferred_element_type=jnp.float32,
                )
                total = piece if total is None else total + piece
        rounded = total.astype(jnp.bfloat16).reshape(layers, CORES, rows, width)
        columns = pl.ds(pl.multiple_of(block * width, width), width)
        for half in range(CORES):
            partial[half, :, :, columns] = rounded[:, half]

    swap = remote(
        partial.at[1 - core], arrived, half_sem.at[0], half_sem.at[1], {"tp": 1 - core}
    )
    swap.start()
    swap.wait()
    for at in range(layers):
        summed[at] = (
            partial[core, at].astype(jnp.float32) + arrived[at].astype(jnp.float32)
        ).astype(jnp.bfloat16)
    copies = []
    for ahead in range(1, layers):
        other = lax.rem(layer + ahead, layers)
        copies.append(
            remote(
                summed.at[other], pieces.at[layer], far_send.at[ahead], far_recv.at[ahead],
                {"sp": other * PLANE + spot},
            )
        )
    for copy in copies:
        copy.start()
    pieces[layer] = summed[layer]
    for copy in copies:
        copy.wait()
    squares = jnp.zeros((rows, 1), jnp.float32)
    span = pieces.shape[-1]
    for at in range(layers):
        value = pieces[at].astype(jnp.float32)
        squares = squares + jnp.sum(value * value, axis=-1, keepdims=True)
    scale = lax.rsqrt(squares / (layers * span) + epsilon)
    for at in range(layers):
        columns = slice(at * span, (at + 1) * span)
        out_ref[:, columns] = (
            pieces[at].astype(jnp.float32) * scale * gain_ref[:, columns]
        ).astype(jnp.bfloat16)


def finish(attended, mixed, attn_out, state_out, out_gain):
    layers, rows, depth = attended.shape
    height, width = attn_out.shape
    half_rows = rows // CORES
    anywhere = pl.BlockSpec(memory_space=pl.ANY)
    vmem = pl.BlockSpec(memory_space=pltpu.VMEM)
    dma = pltpu.SemaphoreType.DMA
    piece = pltpu.VMEM((layers, half_rows, PLANE * width), jnp.bfloat16)
    return pl.pallas_call(
        output_kernel,
        out_shape=jax.ShapeDtypeStruct((half_rows, layers * PLANE * width), jnp.bfloat16),
        in_specs=[anywhere] * 4 + [vmem],
        out_specs=vmem,
        scratch_shapes=[
            pltpu.VMEM((2, PLANE, 2, height // 2, width), jnp.bfloat16),
            pltpu.VMEM((layers, 2, layers, rows, depth), jnp.bfloat16),
            pltpu.VMEM((CORES, layers, half_rows, PLANE * width), jnp.bfloat16),
            piece, piece, piece,
            dma((2, 2, layers)), dma((2, 2, layers)),
            dma((2, 2, 3)), dma((2, 2, 3)), dma((4,)), dma((2,)),
            dma((layers,)), dma((layers,)),
        ],
        compiler_params=pltpu.CompilerParams(
            collective_id=1, has_side_effects=True, vmem_limit_bytes=48 * 2**20
        ),
    )(
        attended, mixed, attn_out.reshape(2, height // 2, width),
        state_out.reshape(2, height // 2, width), out_gain.reshape(1, -1),
    )


def blocks_scan(inputs, tables):
    layers, rows, _ = inputs.shape
    blocks, width, channels = (tables["blocks"], tables["width"], tables["channels"])
    row_spec = pl.BlockSpec((1, 1, width), lambda b, t: (b, 0, 0))
    carry_spec = pl.BlockSpec((SUB, width), lambda b, t: (t, b))
    end_spec = pl.BlockSpec((1, 1, width), lambda b, t: (t, 0, b))
    return pl.pallas_call(
        scan_kernel,
        grid=(blocks, layers),
        in_specs=[
            pl.BlockSpec((rows, channels), lambda b, t: (t, b)),
            pl.BlockSpec((1, channels, 2 * width), lambda b, t: (b, 0, 0)),
            row_spec, row_spec, row_spec, row_spec,
        ],
        out_specs=[
            pl.BlockSpec((rows, 2 * width), lambda b, t: (t, b)),
            carry_spec, carry_spec, end_spec, end_spec,
        ],
        out_shape=[
            jax.ShapeDtypeStruct((layers * rows, 2 * width * blocks), jnp.float32),
            jax.ShapeDtypeStruct((layers * SUB, width * blocks), jnp.float32),
            jax.ShapeDtypeStruct((layers * SUB, width * blocks), jnp.float32),
            jax.ShapeDtypeStruct((layers, 1, width * blocks), jnp.float32),
            jax.ShapeDtypeStruct((layers, 1, width * blocks), jnp.float32),
        ],
        cost_estimate=pl.CostEstimate(
            flops=12 * layers * rows * channels * width * blocks, bytes_accessed=10**7,
            transcendentals=0,
        ),
    )(
        inputs.reshape(layers * rows, -1), tables["drive"], tables["pole_re"], tables["pole_im"],
        tables["jump_re"], tables["jump_im"],
    )


def blocks_read(inputs, scanned, prior_re, prior_im, tables, skip_gain):
    layers, rows, _ = inputs.shape
    state, carry_re, carry_im = scanned[:3]
    blocks, width, channels = (tables["blocks"], tables["width"], tables["channels"])
    row_spec = pl.BlockSpec((1, 1, width), lambda b, t: (b, 0, 0))
    prior_spec = pl.BlockSpec((1, 1, width), lambda b, t: (t, 0, b))
    carry_spec = pl.BlockSpec((SUB, width), lambda b, t: (t, b))
    chunk_spec = pl.BlockSpec((SUB, width), lambda b, t: (0, b))
    return pl.pallas_call(
        readout_kernel,
        grid=(blocks, layers),
        in_specs=[
            pl.BlockSpec((rows, channels), lambda b, t: (t, b)),
            pl.BlockSpec((rows, 2 * width), lambda b, t: (t, b)),
            carry_spec, carry_spec, prior_spec, prior_spec, chunk_spec, chunk_spec,
            row_spec, row_spec,
            pl.BlockSpec((1, 2 * width, channels), lambda b, t: (b, 0, 0)),
            pl.BlockSpec((1, channels), lambda b, t: (0, b)),
        ],
        out_specs=pl.BlockSpec((rows, channels), lambda b, t: (t, b)),
        out_shape=jax.ShapeDtypeStruct((layers * rows, channels * blocks), jnp.bfloat16),
        scratch_shapes=[pltpu.VMEM((rows, 2 * width), jnp.float32)],
        cost_estimate=pl.CostEstimate(
            flops=12 * layers * rows * channels * width * blocks, bytes_accessed=10**7,
            transcendentals=0,
        ),
    )(
        inputs.reshape(layers * rows, -1), state, carry_re, carry_im, prior_re, prior_im,
        tables["chunk_re"], tables["chunk_im"], tables["pole_re"], tables["pole_im"],
        tables["read"], skip_gain.reshape(1, -1),
    ).reshape(inputs.shape)


def prior_states(end_re, end_im, spot, decay_rate, rotation, log_step, rows):
    layers = end_re.shape[0]
    size = lax.axis_size("sp")
    planes = [[at * PLANE + other for other in range(PLANE)] for at in range(size // PLANE)]
    ends = lax.all_gather(jnp.stack([end_re, end_im]), "sp", axis_index_groups=planes)
    power_re, power_im = complex_power(decay_rate, rotation, log_step, float(rows))
    power_re, power_im = (power_re.reshape(1, -1), power_im.reshape(1, -1))
    held_re, held_im = (jnp.zeros_like(end_re[0]), jnp.zeros_like(end_im[0]))
    prior_re, prior_im = ([], [])
    for at in range(layers * PLANE):
        prior_re.append(held_re)
        prior_im.append(held_im)
        end = ends[at % PLANE, :, at // PLANE]
        held_re, held_im = (
            power_re * held_re - power_im * held_im + end[0],
            power_re * held_im + power_im * held_re + end[1],
        )

    def mine(priors):
        stacked = jnp.stack(priors).reshape(layers, PLANE, 1, -1)
        return lax.dynamic_index_in_dim(stacked, spot, axis=1, keepdims=False)

    return (mine(prior_re), mine(prior_im))


def body(
    tokens,
    norm_gain,
    w_query,
    w_key,
    w_value,
    w_state_in,
    sink_logit,
    decay_rate,
    rotation,
    log_step,
    in_re,
    in_im,
    out_re,
    out_im,
    skip_gain,
    w_attn_out,
    w_state_out,
    out_gain,
):
    rows = tokens.shape[0]
    size = lax.axis_size("sp")
    layers = size // PLANE
    layer, spot, core = place()
    wide_tokens = tokens.astype(jnp.float32)
    normed = (
        wide_tokens
        * lax.rsqrt(jnp.mean(wide_tokens * wide_tokens, axis=-1, keepdims=True) + epsilon)
        * norm_gain
    ).astype(jnp.bfloat16)

    def by_layer(matrix):
        return matrix.reshape(matrix.shape[0], layers, -1)

    packed = jnp.concatenate(
        [by_layer(w_query), by_layer(w_key), by_layer(w_value), by_layer(w_state_in)], axis=2
    )
    depth = packed.shape[0]
    packed = jnp.swapaxes(packed, 0, 1).reshape(layers, 2, depth // 2, -1)
    query_width = w_query.shape[1] // layers
    pair_width = 2 * (w_key.shape[1] // layers)
    queries, pairs, inputs = project(packed, normed, query_width, pair_width)

    passed = lax.ppermute(
        pairs, "sp",
        [
            (at * PLANE + other, at * PLANE + (other + 1) % PLANE)
            for at in range(layers)
            for other in range(PLANE)
        ],
    )
    shifted = jnp.concatenate([jnp.zeros_like(passed[:1]), passed[:-1]], axis=0)
    before = jnp.where(spot == 0, shifted, passed)

    def mine(value):
        count = value.shape[0] // layers
        return lax.dynamic_slice_in_dim(value, layer * count, count, 0)

    decay_rate, rotation, log_step = (mine(decay_rate), mine(rotation), mine(log_step))
    tables = state_tables(
        rows, decay_rate, rotation, log_step, mine(in_re), mine(in_im), mine(out_re), mine(out_im)
    )
    scanned = blocks_scan(inputs, tables)
    prior_re, prior_im = prior_states(
        scanned[3], scanned[4], spot, decay_rate, rotation, log_step, rows
    )
    attended = attend(queries, pairs, before, mine(sink_logit).reshape(1, -1))
    mixed = blocks_read(inputs, scanned, prior_re, prior_im, tables, mine(skip_gain))
    return finish(attended, mixed, w_attn_out, w_state_out, out_gain)


def suits(mesh, shapes):
    size, cores = (mesh.shape["sp"], mesh.shape["tp"])
    layers = size // PLANE
    key_width = shapes[3][1] // cores
    state_width = shapes[5][1] // cores
    return (
        size % PLANE == 0
        and layers > 1
        and cores == CORES
        and shapes[0][0] // size == WINDOW
        and key_width == layers * HEAD
        and state_width % (layers * LANES) == 0
        and shapes[2][1] % (cores * layers * LANES) == 0
    )


def solution(mesh):
    def run(*arrays):
        chosen = body if suits(mesh, [array.shape for array in arrays]) else whole_weights_body
        return sharded(mesh, chosen)(*arrays)

    return run


def sharded(mesh, chosen):
    return jax.shard_map(
        chosen,
        mesh=mesh,
        in_specs=(
            P("sp", None),
            P(),
            P("sp", "tp"),
            P("sp", "tp"),
            P("sp", "tp"),
            P("sp", "tp"),
            P("tp"),
            P("tp", None),
            P("tp", None),
            P("tp"),
            P("tp", None, None),
            P("tp", None, None),
            P("tp", None, None),
            P("tp", None, None),
            P("tp"),
            P("tp", "sp"),
            P("tp", "sp"),
            P(),
        ),
        out_specs=P(("sp", "tp"), None),
        check_vma=False,
    )
```

```python
import math

import jax
import jax.numpy as jnp
import numpy as np
from jax import lax
from jax.experimental import pallas as pl
from jax.experimental.pallas import tpu as pltpu
from jax.sharding import PartitionSpec as P

HEAD = 64
WINDOW = 128
SUB = 8


epsilon = 1e-06
rotary_base = 500000.0


def passed_along(value, axis, by):
    size = lax.axis_size(axis)
    pairs = [(i, i + by) for i in range(size) if 0 <= i + by < size]
    return lax.ppermute(value, axis, pairs)


def rotate(heads_block, positions):
    head_width = heads_block.shape[-1]
    half_width = head_width // 2
    frequency = rotary_base ** (-(jnp.arange(half_width, dtype=jnp.float32) * 2.0 / head_width))
    angles = positions.astype(jnp.float32)[:, None] * frequency[None, :]
    cosine = jnp.cos(angles)[:, None, :]
    sine_part = jnp.sin(angles)[:, None, :]
    lower_half = heads_block[..., :half_width]
    upper_half = heads_block[..., half_width:]
    return jnp.concatenate(
        [
            lower_half * cosine - upper_half * sine_part,
            upper_half * cosine + lower_half * sine_part,
        ],
        axis=-1,
    )


def shape_heads(query_sum, key_sum, value_sum, positions, head_width):
    row_count = query_sum.shape[0]
    kv_heads = key_sum.shape[1] // head_width
    group_size = query_sum.shape[1] // key_sum.shape[1]
    queries = rotate(
        query_sum.reshape(row_count, kv_heads * group_size, head_width), positions
    ).astype(jnp.bfloat16)
    queries = queries.reshape(row_count, kv_heads, group_size, head_width)
    key_rows = rotate(key_sum.reshape(row_count, kv_heads, head_width), positions).astype(
        jnp.bfloat16
    )
    key_rows = key_rows.reshape(row_count, kv_heads * head_width)
    value_rows = value_sum.astype(jnp.bfloat16)
    return (queries, key_rows, value_rows)


def band_attention(queries, key_rows, value_rows, sink_logit, first_row, window):
    row_count, kv_heads, group_size, head_width = queries.shape
    blocks = row_count // window
    query_blocks = queries.reshape(blocks, window, kv_heads, group_size, head_width)
    key_blocks = jnp.concatenate(
        [
            key_rows[:row_count].reshape(blocks, window, kv_heads, head_width),
            key_rows[window:].reshape(blocks, window, kv_heads, head_width),
        ],
        axis=1,
    )
    value_blocks = jnp.concatenate(
        [
            value_rows[:row_count].reshape(blocks, window, kv_heads, head_width),
            value_rows[window:].reshape(blocks, window, kv_heads, head_width),
        ],
        axis=1,
    )
    scores = jnp.einsum(
        "bqkgd,bskd->bkgqs", query_blocks, key_blocks, preferred_element_type=jnp.float32
    ) / math.sqrt(head_width)
    block_start = jnp.arange(blocks, dtype=jnp.int32)[:, None, None] * window
    query_at = first_row + block_start + jnp.arange(window, dtype=jnp.int32)[None, :, None]
    key_at = (
        first_row - window + block_start + jnp.arange(2 * window, dtype=jnp.int32)[None, None, :]
    )
    offset_gap = query_at - key_at
    visible = (offset_gap >= 0) & (offset_gap < window) & (key_at >= 0)
    scores = jnp.where(visible[:, None, None, :, :], scores, -jnp.inf)
    sink_value = sink_logit.reshape(1, kv_heads, group_size, 1, 1)
    top_score = jnp.maximum(jnp.max(scores, axis=-1, keepdims=True), sink_value)
    exponent = jnp.exp(scores - top_score)
    totals = jnp.sum(exponent, axis=-1, keepdims=True) + jnp.exp(sink_value - top_score)
    weights = (exponent / totals).astype(jnp.bfloat16)
    attended = jnp.einsum(
        "bkgqs,bskd->bqkgd", weights, value_blocks, preferred_element_type=jnp.float32
    )
    return attended.reshape(row_count, kv_heads * group_size * head_width).astype(jnp.bfloat16)


def discretize(decay_rate, rotation, log_step, in_re, in_im):
    time_step = jnp.exp(log_step)[:, None]
    lambda_re = -decay_rate
    modulus = jnp.exp(lambda_re * time_step)
    pole_re = modulus * jnp.cos(rotation * time_step)
    pole_im = modulus * jnp.sin(rotation * time_step)
    minus_one = pole_re - 1.0
    denominator = lambda_re * lambda_re + rotation * rotation
    factor_re = ((minus_one * lambda_re + pole_im * rotation) / denominator)[..., None]
    factor_im = ((pole_im * lambda_re - minus_one * rotation) / denominator)[..., None]
    drive_re = factor_re * in_re - factor_im * in_im
    drive_im = factor_re * in_im + factor_im * in_re
    return (pole_re, pole_im, drive_re, drive_im)


def complex_power(decay_rate, rotation, log_step, exponent):
    time_step = jnp.exp(log_step)[:, None]
    modulus = jnp.exp(-decay_rate * time_step * exponent)
    angle = rotation * time_step * exponent
    return (modulus * jnp.cos(angle), modulus * jnp.sin(angle))


def token_shuffle(rows, inverse):
    steps = rows // SUB
    out_row = lax.broadcasted_iota(jnp.int32, (rows, rows), 1 if inverse else 0)
    in_row = lax.broadcasted_iota(jnp.int32, (rows, rows), 0 if inverse else 1)
    token = (out_row % SUB) * steps + out_row // SUB
    return (token == in_row).astype(jnp.bfloat16)


def scan_kernel(
    u_ref, drive_ref, pole_re_ref, pole_im_ref, jump_re_ref, jump_im_ref,
    state_ref, carry_re_ref, carry_im_ref, end_re_ref, end_im_ref,
):
    rows = u_ref.shape[0]
    width = pole_re_ref.shape[-1]
    shuffle = token_shuffle(rows, False)
    shuffled = jnp.dot(shuffle, u_ref[...], preferred_element_type=jnp.float32)
    state_ref[...] = jnp.dot(
        shuffled, drive_ref[0], precision=lax.Precision.HIGHEST,
        preferred_element_type=jnp.float32,
    )
    pole_re = jnp.broadcast_to(pole_re_ref[0], (SUB, width))
    pole_im = jnp.broadcast_to(pole_im_ref[0], (SUB, width))
    now_re = jnp.zeros((SUB, width), jnp.float32)
    now_im = jnp.zeros((SUB, width), jnp.float32)
    for step in range(rows // SUB):
        at = slice(step * SUB, (step + 1) * SUB)
        new_re = pole_re * now_re - pole_im * now_im + state_ref[at, :width]
        new_im = pole_re * now_im + pole_im * now_re + state_ref[at, width:]
        state_ref[at, :width] = new_re
        state_ref[at, width:] = new_im
        now_re, now_im = new_re, new_im
    jump_re, jump_im = (jump_re_ref[0], jump_im_ref[0])
    held_re = jnp.zeros((1, width), jnp.float32)
    held_im = jnp.zeros((1, width), jnp.float32)
    for chunk in range(SUB):
        carry_re_ref[chunk : chunk + 1, :] = held_re
        carry_im_ref[chunk : chunk + 1, :] = held_im
        next_re = jump_re * held_re - jump_im * held_im + now_re[chunk : chunk + 1]
        next_im = jump_re * held_im + jump_im * held_re + now_im[chunk : chunk + 1]
        held_re, held_im = next_re, next_im
    end_re_ref[0] = held_re
    end_im_ref[0] = held_im


def readout_kernel(
    u_ref, state_ref, carry_re_ref, carry_im_ref, prior_re_ref, prior_im_ref,
    chunk_re_ref, chunk_im_ref, pole_re_ref, pole_im_ref, read_ref, skip_ref, out_ref, full_ref,
):
    rows = u_ref.shape[0]
    width = pole_re_ref.shape[-1]
    prior_re, prior_im = (prior_re_ref[0], prior_im_ref[0])
    chunk_re, chunk_im = (chunk_re_ref[...], chunk_im_ref[...])
    add_re = carry_re_ref[...] + chunk_re * prior_re - chunk_im * prior_im
    add_im = carry_im_ref[...] + chunk_re * prior_im + chunk_im * prior_re
    pole_re = jnp.broadcast_to(pole_re_ref[0], (SUB, width))
    pole_im = jnp.broadcast_to(pole_im_ref[0], (SUB, width))
    for step in range(rows // SUB):
        at = slice(step * SUB, (step + 1) * SUB)
        turned_re = pole_re * add_re - pole_im * add_im
        turned_im = pole_re * add_im + pole_im * add_re
        full_ref[at, :width] = state_ref[at, :width] + turned_re
        full_ref[at, width:] = state_ref[at, width:] + turned_im
        add_re, add_im = turned_re, turned_im
    summed = jnp.dot(
        full_ref[...], read_ref[0], precision=lax.Precision.HIGHEST,
        preferred_element_type=jnp.float32,
    )
    shuffled = jnp.dot(
        token_shuffle(rows, False), u_ref[...], preferred_element_type=jnp.float32
    )
    mixed = jax.nn.gelu(summed + skip_ref[...] * shuffled).astype(jnp.bfloat16)
    out_ref[...] = jnp.dot(
        token_shuffle(rows, True), mixed, preferred_element_type=jnp.float32
    ).astype(jnp.bfloat16)


def block_diagonal(parts):
    blocks, per, rows, columns = parts[0].shape
    same = jnp.eye(per, dtype=bool)[None, :, None, :, None]
    spread = [
        jnp.where(same, part[:, :, :, None, :], 0.0).reshape(blocks, per * rows, per * columns)
        for part in parts
    ]
    return jnp.concatenate(spread, axis=2)


def state_tables(rows, decay_rate, rotation, log_step, in_re, in_im, out_re, out_im):
    groups, states = decay_rate.shape
    group_width = in_re.shape[-1]
    per = min(groups, max(1, 128 // group_width))
    blocks, width = (groups // per, per * states)
    pole_re, pole_im, drive_re, drive_im = discretize(decay_rate, rotation, log_step, in_re, in_im)
    steps = rows // SUB

    def by_block(value):
        return value.reshape(blocks, per, *value.shape[1:])

    def flat(value):
        return value.reshape(blocks, 1, width)

    drive = block_diagonal(
        [by_block(jnp.swapaxes(drive_re, 1, 2)), by_block(jnp.swapaxes(drive_im, 1, 2))]
    )
    read = jnp.swapaxes(block_diagonal([by_block(out_re), by_block(-out_im)]), 1, 2)
    jump = complex_power(decay_rate, rotation, log_step, float(steps))
    chunk_powers = [
        complex_power(decay_rate, rotation, log_step, float(steps * c)) for c in range(SUB)
    ]
    chunk_re = jnp.stack([p[0].reshape(groups * states) for p in chunk_powers])
    chunk_im = jnp.stack([p[1].reshape(groups * states) for p in chunk_powers])
    return dict(
        drive=drive, read=read, pole_re=flat(pole_re), pole_im=flat(pole_im),
        jump_re=flat(jump[0]), jump_im=flat(jump[1]), chunk_re=chunk_re, chunk_im=chunk_im,
        blocks=blocks, width=width, channels=per * group_width,
    )


def local_scan(inputs, tables):
    rows = inputs.shape[0]
    blocks, width, channels = (tables["blocks"], tables["width"], tables["channels"])
    row_spec = pl.BlockSpec((1, 1, width), lambda b: (b, 0, 0))
    carry_spec = pl.BlockSpec((SUB, width), lambda b: (0, b))
    return pl.pallas_call(
        scan_kernel,
        grid=(blocks,),
        in_specs=[
            pl.BlockSpec((rows, channels), lambda b: (0, b)),
            pl.BlockSpec((1, channels, 2 * width), lambda b: (b, 0, 0)),
            row_spec, row_spec, row_spec, row_spec,
        ],
        out_specs=[
            pl.BlockSpec((rows, 2 * width), lambda b: (0, b)),
            carry_spec, carry_spec, row_spec, row_spec,
        ],
        out_shape=[
            jax.ShapeDtypeStruct((rows, 2 * width * blocks), jnp.float32),
            jax.ShapeDtypeStruct((SUB, width * blocks), jnp.float32),
            jax.ShapeDtypeStruct((SUB, width * blocks), jnp.float32),
            jax.ShapeDtypeStruct((blocks, 1, width), jnp.float32),
            jax.ShapeDtypeStruct((blocks, 1, width), jnp.float32),
        ],
        cost_estimate=pl.CostEstimate(
            flops=12 * rows * channels * width * blocks, bytes_accessed=10**7, transcendentals=0
        ),
    )(
        inputs, tables["drive"], tables["pole_re"], tables["pole_im"],
        tables["jump_re"], tables["jump_im"],
    )


def read_states(inputs, scanned, prior_re, prior_im, tables, skip_gain):
    rows = inputs.shape[0]
    state, carry_re, carry_im = scanned[:3]
    blocks, width, channels = (tables["blocks"], tables["width"], tables["channels"])
    row_spec = pl.BlockSpec((1, 1, width), lambda b: (b, 0, 0))
    carry_spec = pl.BlockSpec((SUB, width), lambda b: (0, b))
    return pl.pallas_call(
        readout_kernel,
        grid=(blocks,),
        in_specs=[
            pl.BlockSpec((rows, channels), lambda b: (0, b)),
            pl.BlockSpec((rows, 2 * width), lambda b: (0, b)),
            carry_spec, carry_spec, row_spec, row_spec, carry_spec, carry_spec,
            row_spec, row_spec,
            pl.BlockSpec((1, 2 * width, channels), lambda b: (b, 0, 0)),
            pl.BlockSpec((1, channels), lambda b: (0, b)),
        ],
        out_specs=pl.BlockSpec((rows, channels), lambda b: (0, b)),
        out_shape=jax.ShapeDtypeStruct((rows, channels * blocks), jnp.bfloat16),
        scratch_shapes=[pltpu.VMEM((rows, 2 * width), jnp.float32)],
        cost_estimate=pl.CostEstimate(
            flops=12 * rows * channels * width * blocks, bytes_accessed=10**7, transcendentals=0
        ),
    )(
        inputs, state, carry_re, carry_im, prior_re, prior_im,
        tables["chunk_re"], tables["chunk_im"], tables["pole_re"], tables["pole_im"],
        tables["read"], skip_gain.reshape(1, -1),
    )


def carried_state(end_re, end_im, decay_rate, rotation, log_step, rows):
    ends = jnp.stack([end_re, end_im])
    shape = end_re.shape
    size = lax.axis_size("sp")
    reach = 1
    while reach < size:
        power_re, power_im = complex_power(decay_rate, rotation, log_step, float(rows * reach))
        power_re, power_im = (power_re.reshape(shape), power_im.reshape(shape))
        prior = passed_along(ends, "sp", reach)
        ends = ends + jnp.stack(
            [
                power_re * prior[0] - power_im * prior[1],
                power_re * prior[1] + power_im * prior[0],
            ]
        )
        reach *= 2
    before = passed_along(ends, "sp", 1)
    return (before[0], before[1])


def state_branch(inputs, decay_rate, rotation, log_step, in_re, in_im, out_re, out_im, skip_gain):
    rows = inputs.shape[0]
    tables = state_tables(rows, decay_rate, rotation, log_step, in_re, in_im, out_re, out_im)
    scanned = local_scan(inputs, tables)
    prior_re, prior_im = carried_state(
        scanned[3], scanned[4], decay_rate, rotation, log_step, rows
    )
    return read_states(inputs, scanned, prior_re, prior_im, tables, skip_gain)


def earlier_window(key_rows, value_rows):
    joined = jnp.concatenate([key_rows, value_rows], axis=1)
    prior = passed_along(joined, "sp", 1)
    return jnp.concatenate([prior, joined], axis=0)


def make_adder(normed_cols):

    def add_pieces(carried, weight_pieces, row_start):
        updated = []
        for running_total, weight_piece in zip(carried, weight_pieces):
            product = lax.dot_general(
                normed_cols,
                weight_piece,
                (((0,), (0,)), ((), ())),
                preferred_element_type=jnp.float32,
            )
            updated.append(product)
        return tuple(updated)

    return add_pieces


def whole_weights_body(
    tokens,
    norm_gain,
    w_query,
    w_key,
    w_value,
    w_state_in,
    sink_logit,
    decay_rate,
    rotation,
    log_step,
    in_re,
    in_im,
    out_re,
    out_im,
    skip_gain,
    w_attn_out,
    w_state_out,
    out_gain,
):
    row_count = tokens.shape[0]
    window = WINDOW
    head_width = HEAD
    wide_tokens = tokens.astype(jnp.float32)
    normed = (
        wide_tokens
        * lax.rsqrt(jnp.mean(wide_tokens * wide_tokens, axis=-1, keepdims=True) + epsilon)
        * norm_gain
    ).astype(jnp.bfloat16)
    first_row = lax.axis_index("sp") * row_count
    positions = first_row + jnp.arange(row_count, dtype=jnp.int32)
    add_pieces = make_adder(jnp.transpose(normed))

    def empty_like(weight_shard):
        return jnp.zeros((row_count, weight_shard.shape[1]), jnp.float32)

    query_sum, key_sum, value_sum, input_sum = add_pieces(
        (empty_like(w_query), empty_like(w_key), empty_like(w_value), empty_like(w_state_in)),
        (
            lax.all_gather(w_query, "sp", axis=0, tiled=True),
            lax.all_gather(w_key, "sp", axis=0, tiled=True),
            lax.all_gather(w_value, "sp", axis=0, tiled=True),
            lax.all_gather(w_state_in, "sp", axis=0, tiled=True),
        ),
        jnp.int32(0),
    )
    queries, key_rows, value_rows = shape_heads(
        query_sum, key_sum, value_sum, positions, head_width
    )
    joined_rows = earlier_window(key_rows, value_rows)
    inputs = input_sum.astype(jnp.bfloat16)
    mixed_state = state_branch(
        inputs, decay_rate, rotation, log_step, in_re, in_im, out_re, out_im, skip_gain
    )
    kv_width = key_rows.shape[1]
    kv_heads = kv_width // head_width
    all_keys = joined_rows[:, :kv_width].reshape(window + row_count, kv_heads, head_width)
    all_values = joined_rows[:, kv_width:].reshape(window + row_count, kv_heads, head_width)
    attended = band_attention(queries, all_keys, all_values, sink_logit, first_row, window)
    attn_rows, state_rows = (
        lax.all_gather(w_attn_out, "sp", axis=1, tiled=True),
        lax.all_gather(w_state_out, "sp", axis=1, tiled=True),
    )
    projected = lax.psum_scatter(
        (
            jnp.dot(attended, attn_rows, preferred_element_type=jnp.float32)
            + jnp.dot(mixed_state, state_rows, preferred_element_type=jnp.float32)
        ).astype(jnp.bfloat16),
        "tp",
        scatter_dimension=0,
        tiled=True,
    ).astype(jnp.float32)
    row_scale = lax.rsqrt(jnp.mean(projected * projected, axis=-1, keepdims=True) + epsilon)
    return (projected * row_scale * out_gain).astype(jnp.bfloat16)


SIDE = 2
PLANE = SIDE * SIDE
CORES = 2
LANES = 128
MESH = pl.DeviceIdType.MESH


def place():
    me = lax.axis_index("sp")
    return (lax.div(me, PLANE), lax.rem(me, PLANE), lax.axis_index("tp"))


def plane_neighbours(spot):
    beside = spot + 1 - 2 * lax.rem(spot, SIDE)
    above = spot + SIDE - 2 * SIDE * lax.div(spot, SIDE)
    return (beside, above)


def greet(layers, layer, spot, core):
    barrier = pltpu.get_barrier_semaphore()
    beside, above = plane_neighbours(spot)
    for ahead in range(1, layers):
        other = lax.rem(layer + ahead, layers)
        pl.semaphore_signal(
            barrier, inc=1, device_id={"sp": other * PLANE + spot}, device_id_type=MESH
        )
    for other in (beside, above, PLANE - 1 - spot):
        pl.semaphore_signal(
            barrier, inc=1, device_id={"sp": layer * PLANE + other}, device_id_type=MESH
        )
    pl.semaphore_signal(barrier, inc=1, device_id={"tp": 1 - core}, device_id_type=MESH)
    pl.semaphore_wait(barrier, layers + 3)


def remote(source, target, send_sem, recv_sem, device):
    return pltpu.make_async_remote_copy(
        src_ref=source, dst_ref=target, send_sem=send_sem, recv_sem=recv_sem,
        device_id=device, device_id_type=MESH,
    )


def line_first(layers, layer, spot, source, held, send_sems, recv_sems):
    @pl.when(layer < layers - 1)
    def _():
        remote(
            source, held.at[layer], send_sems.at[0, 0], recv_sems.at[0, 0],
            {"sp": (layer + 1) * PLANE + spot},
        ).start()

    @pl.when(layer > 0)
    def _():
        remote(
            source, held.at[layer], send_sems.at[1, 0], recv_sems.at[1, 0],
            {"sp": (layer - 1) * PLANE + spot},
        ).start()


def line_pass(layers, layer, spot, hop, held, send_sems, recv_sems, landed=None):
    @pl.when(layer - hop >= 0)
    def _():
        block = held.at[layer - hop]
        remote(block, block, send_sems.at[0, 0], recv_sems.at[0, hop - 1], {"sp": 0}).wait_recv()

        @pl.when(layer < layers - 1)
        def _():
            if hop < layers - 1:
                remote(
                    block, block, send_sems.at[0, hop], recv_sems.at[0, hop],
                    {"sp": (layer + 1) * PLANE + spot},
                ).start()

        if landed is not None:
            landed(0, hop, block)

    @pl.when(layer + hop <= layers - 1)
    def _():
        block = held.at[layer + hop]
        remote(block, block, send_sems.at[1, 0], recv_sems.at[1, hop - 1], {"sp": 0}).wait_recv()

        @pl.when(layer > 0)
        def _():
            if hop < layers - 1:
                remote(
                    block, block, send_sems.at[1, hop], recv_sems.at[1, hop],
                    {"sp": (layer - 1) * PLANE + spot},
                ).start()

        if landed is not None:
            landed(1, hop, block)


def line_drain(layers, layer, source, held, send_sems, recv_sems):
    for hop in range(layers - 1):

        @pl.when((layer - hop >= 0) & (layer < layers - 1))
        def _():
            remote(
                source, held.at[layer], send_sems.at[0, hop], recv_sems.at[0, 0], {"sp": 0}
            ).wait_send()

        @pl.when((layer + hop <= layers - 1) & (layer > 0))
        def _():
            remote(
                source, held.at[layer], send_sems.at[1, hop], recv_sems.at[1, 0], {"sp": 0}
            ).wait_send()


def plane_first(halves, slots, layer, spot, send_sems, recv_sems):
    beside, above = plane_neighbours(spot)
    copies = []
    for half in (0, 1):
        copies.append(
            remote(
                halves.at[half], slots.at[spot, half], send_sems.at[0, half],
                recv_sems.at[0, half], {"sp": layer * PLANE + beside},
            )
        )
        copies.append(
            remote(
                halves.at[1 - half], slots.at[spot, 1 - half], send_sems.at[1, 1 - half],
                recv_sems.at[1, 1 - half], {"sp": layer * PLANE + above},
            )
        )
    for copy in copies:
        copy.start()


def plane_pass(slots, layer, spot, send_sems, recv_sems):
    beside, above = plane_neighbours(spot)
    block = slots.at[beside, 0]
    remote(block, block, send_sems.at[0, 0], recv_sems.at[0, 0], {"sp": 0}).wait_recv()
    remote(
        block, block, send_sems.at[1, 2], recv_sems.at[1, 2], {"sp": layer * PLANE + above}
    ).start()
    block = slots.at[above, 1]
    remote(block, block, send_sems.at[0, 0], recv_sems.at[1, 1], {"sp": 0}).wait_recv()
    remote(
        block, block, send_sems.at[0, 2], recv_sems.at[0, 2], {"sp": layer * PLANE + beside}
    ).start()


def plane_landed(slots, spot, send_sems, recv_sems):
    for way, half in ((0, 1), (1, 0), (0, 2), (1, 2)):
        block = slots.at[spot, 0]
        remote(block, block, send_sems.at[0, 0], recv_sems.at[way, half], {"sp": 0}).wait_recv()
    for way in (0, 1):
        for half in (0, 1, 2):
            block = slots.at[spot, 0]
            remote(block, block, send_sems.at[way, half], recv_sems.at[0, 0], {"sp": 0}).wait_send()


def lanes_of(rows):
    return jnp.concatenate([rows[at : at + 1] for at in range(rows.shape[0])], axis=1)


def split_pair(value):
    high = value.astype(jnp.bfloat16)
    return (high, (value - high.astype(jnp.float32)).astype(jnp.bfloat16))


def make_tables(
    layer, rows, decay_ref, rotation_ref, step_ref, in_re_ref, in_im_ref, out_re_ref, out_im_ref,
    drive, read, powers,
):
    groups, states, group_width = in_re_ref.shape
    kinds, _, width2 = drive.shape
    per = groups // kinds
    width = per * states
    channels = per * group_width
    base = layer * groups
    decay = lanes_of(decay_ref[pl.ds(base, groups), :])
    rotation = lanes_of(rotation_ref[pl.ds(base, groups), :])
    step = jnp.exp(
        jnp.concatenate(
            [jnp.full((1, states), step_ref[base + at], jnp.float32) for at in range(groups)],
            axis=1,
        )
    )
    row = lax.broadcasted_iota(jnp.int32, (SUB, groups * states), 0)
    steps = rows // SUB
    shares = (row * steps, jnp.where(row == 0, 1, jnp.where(row == 1, steps, rows)))
    for at, share in enumerate(shares):
        share = share.astype(jnp.float32)
        modulus = jnp.exp(-decay * step * share)
        angle = rotation * step * share
        powers[2 * at] = modulus * jnp.cos(angle)
        powers[2 * at + 1] = modulus * jnp.sin(angle)
    pole_re, pole_im = (powers[2, 0:1, :], powers[3, 0:1, :])
    minus_one = pole_re - 1.0
    denominator = decay * decay + rotation * rotation
    factor_re = (pole_im * rotation - minus_one * decay) / denominator
    factor_im = (-pole_im * decay - minus_one * rotation) / denominator
    same = (
        lax.broadcasted_iota(jnp.int32, (channels, width), 0) // group_width
        == lax.broadcasted_iota(jnp.int32, (channels, width), 1) // states
    )

    def spread(pieces):
        beside = jnp.concatenate(pieces, axis=1)
        return jnp.concatenate([beside] * per, axis=0)

    for kind in range(kinds):
        lanes = slice(kind * width, (kind + 1) * width)
        f_re, f_im = (factor_re[:, lanes], factor_im[:, lanes])
        own = range(kind * per, (kind + 1) * per)
        m_re = spread([jnp.transpose(in_re_ref[at]) for at in own])
        m_im = spread([jnp.transpose(in_im_ref[at]) for at in own])
        for part, value in ((0, f_re * m_re - f_im * m_im), (1, f_re * m_im + f_im * m_re)):
            high, low = split_pair(jnp.where(same, value, 0.0))
            columns = slice(part * width, (part + 1) * width)
            drive[kind, :channels, columns] = high
            drive[kind, channels:, columns] = low
        r_re = spread([out_re_ref[at] for at in own])
        r_im = spread([-out_im_ref[at] for at in own])
        for part, value in ((0, r_re), (1, r_im)):
            high, low = split_pair(jnp.where(same, value, 0.0))
            columns = slice(part * width, (part + 1) * width)
            read[kind, :channels, columns] = high
            read[kind, channels:, columns] = low


def normalise(block, held, gain_ref, normed):
    _, parts, part_rows, model = held.shape
    tall = 16
    per = part_rows // tall

    @pl.loop(0, parts * per)
    def _(at):
        value = held[
            block, at // per, pl.ds(pl.multiple_of((at % per) * tall, tall), tall), :
        ].astype(jnp.float32)
        scale = lax.rsqrt(jnp.sum(value * value, axis=-1, keepdims=True) / model + epsilon)
        normed[pl.ds(pl.multiple_of(at * tall, tall), tall), :] = (
            value * scale * gain_ref[...]
        ).astype(jnp.bfloat16)


def project_block(block, spot, normed, weights, tables, queries, pairs, inputs):
    rows, model = normed.shape
    layers = weights.shape[0]
    depth = weights.shape[2] * weights.shape[3]
    query_width, pair_width = (queries.shape[-1], pairs.shape[-1])
    half_width = HEAD // 2
    row_cos_ref, row_sin_ref, block_cos_ref, block_sin_ref = tables
    lane = lax.broadcasted_iota(jnp.int32, (rows, LANES), 1)
    low = lax.rem(lane, HEAD) < half_width

    def turn(value, cosine, sine):
        swapped = jnp.where(
            low, -pltpu.roll(value, LANES - half_width, 1), pltpu.roll(value, half_width, 1)
        )
        return value * cosine + swapped * sine

    total = None
    for at in range(layers * PLANE):
        piece = jnp.dot(
            normed[:, at * depth : (at + 1) * depth],
            weights[at // PLANE, at % PLANE].reshape(depth, weights.shape[-1]),
            preferred_element_type=jnp.float32,
        )
        total = piece if total is None else total + piece
    here = pl.ds(block * PLANE + spot, 1)
    block_cos, block_sin = (block_cos_ref[here, :], block_sin_ref[here, :])
    cosine = row_cos_ref[...] * block_cos - row_sin_ref[...] * block_sin
    sine = row_sin_ref[...] * block_cos + row_cos_ref[...] * block_sin
    turned = [turn(total[:, at : at + LANES], cosine, sine) for at in range(0, query_width, LANES)]
    queries[block] = jnp.concatenate(turned, axis=1).astype(jnp.bfloat16)
    value = total[:, query_width : query_width + pair_width]
    pairs[block] = jnp.where(lane < HEAD, turn(value, cosine, sine), value).astype(jnp.bfloat16)
    inputs[block] = jnp.dot(
        token_shuffle(rows, False), total[:, query_width + pair_width :].astype(jnp.bfloat16),
        preferred_element_type=jnp.float32,
    ).astype(jnp.bfloat16)


def scan_block(block, spot, inputs, drive, powers, states, carries, ends):
    kinds, _, width2 = drive.shape
    width = width2 // 2
    channels = inputs.shape[-1] // kinds
    rows = inputs.shape[1]
    for kind in range(kinds):
        lanes = slice(kind * width, (kind + 1) * width)
        own = inputs[block, :, kind * channels : (kind + 1) * channels]
        states[block, kind] = jnp.dot(
            jnp.concatenate([own, own], axis=1), drive[kind], preferred_element_type=jnp.float32
        )
        pole_re = jnp.broadcast_to(powers[2, 0:1, lanes], (SUB, width))
        pole_im = jnp.broadcast_to(powers[3, 0:1, lanes], (SUB, width))
        now_re = jnp.zeros((SUB, width), jnp.float32)
        now_im = jnp.zeros((SUB, width), jnp.float32)
        for step in range(rows // SUB):
            at = slice(step * SUB, (step + 1) * SUB)
            new_re = pole_re * now_re - pole_im * now_im + states[block, kind, at, :width]
            new_im = pole_re * now_im + pole_im * now_re + states[block, kind, at, width:]
            states[block, kind, at, :width] = new_re
            states[block, kind, at, width:] = new_im
            now_re, now_im = new_re, new_im
        jump_re, jump_im = (powers[2, 1:2, lanes], powers[3, 1:2, lanes])
        held_re = jnp.zeros((1, width), jnp.float32)
        held_im = jnp.zeros((1, width), jnp.float32)
        re, im = ([], [])
        for chunk in range(SUB):
            re.append(held_re)
            im.append(held_im)
            next_re = jump_re * held_re - jump_im * held_im + now_re[chunk : chunk + 1]
            next_im = jump_re * held_im + jump_im * held_re + now_im[chunk : chunk + 1]
            held_re, held_im = next_re, next_im
        carries[block, kind, :, :width] = jnp.concatenate(re, axis=0)
        carries[block, kind, :, width:] = jnp.concatenate(im, axis=0)
        ends[spot, block, kind, :, :width] = held_re
        ends[spot, block, kind, :, width:] = held_im


def attend_block(block, layer, spot, queries, pairs, before, sink_ref, out):
    rows, query_width = queries.shape[1:]
    group = query_width // HEAD
    pair, prior = (pairs[block], before[block])
    keys = jnp.concatenate([prior[:, :HEAD], pair[:, :HEAD]], axis=0)
    values = jnp.concatenate([prior[:, HEAD:], pair[:, HEAD:]], axis=0)
    query_at = lax.broadcasted_iota(jnp.int32, (rows, rows + WINDOW), 0)
    key_at = lax.broadcasted_iota(jnp.int32, (rows, rows + WINDOW), 1) - WINDOW
    gap = query_at - key_at
    first = (block * PLANE + spot) * rows
    visible = (gap >= 0) & (gap < WINDOW) & (key_at + first >= 0)
    pieces = []
    for head in range(group):
        query = queries[block, :, head * HEAD : (head + 1) * HEAD]
        scores = lax.dot_general(
            query, keys, (((1,), (1,)), ((), ())), preferred_element_type=jnp.float32
        ) / math.sqrt(HEAD)
        scores = jnp.where(visible, scores, -jnp.inf)
        sink = jnp.full((1, 1), sink_ref[layer * group + head], jnp.float32)
        top = jnp.maximum(jnp.max(scores, axis=-1, keepdims=True), sink)
        exponent = jnp.exp(scores - top)
        total = jnp.sum(exponent, axis=-1, keepdims=True) + jnp.exp(sink - top)
        weights = (exponent / total).astype(jnp.bfloat16)
        pieces.append(jnp.dot(weights, values, preferred_element_type=jnp.float32))
    out[...] = jnp.concatenate(pieces, axis=1).astype(jnp.bfloat16)


def find_priors(ends, powers, priors):
    plane, layers, kinds = ends.shape[:3]
    width = ends.shape[-1] // 2
    for kind in range(kinds):
        lanes = slice(kind * width, (kind + 1) * width)
        power_re, power_im = (powers[2, 2:3, lanes], powers[3, 2:3, lanes])
        held_re = jnp.zeros((1, width), jnp.float32)
        held_im = jnp.zeros((1, width), jnp.float32)
        for at in range(layers * plane):
            priors[at, kind, :, :width] = held_re
            priors[at, kind, :, width:] = held_im
            end_re = ends[at % plane, at // plane, kind, :, :width]
            end_im = ends[at % plane, at // plane, kind, :, width:]
            held_re, held_im = (
                power_re * held_re - power_im * held_im + end_re,
                power_re * held_im + power_im * held_re + end_im,
            )


def read_block(block, layer, spot, inputs, states, carries, priors, powers, read, skip_ref, out):
    kinds, channels2, width2 = read.shape
    width, channels = (width2 // 2, channels2 // 2)
    rows = inputs.shape[1]
    contract = (((1,), (1,)), ((), ()))
    pieces = []
    for kind in range(kinds):
        lanes = slice(kind * width, (kind + 1) * width)
        prior_re = priors[block * PLANE + spot, kind, :, :width]
        prior_im = priors[block * PLANE + spot, kind, :, width:]
        chunk_re, chunk_im = (powers[0, :, lanes], powers[1, :, lanes])
        add_re = carries[block, kind, :, :width] + chunk_re * prior_re - chunk_im * prior_im
        add_im = carries[block, kind, :, width:] + chunk_re * prior_im + chunk_im * prior_re
        pole_re = jnp.broadcast_to(powers[2, 0:1, lanes], (SUB, width))
        pole_im = jnp.broadcast_to(powers[3, 0:1, lanes], (SUB, width))
        for step in range(rows // SUB):
            at = slice(step * SUB, (step + 1) * SUB)
            turned_re = pole_re * add_re - pole_im * add_im
            turned_im = pole_re * add_im + pole_im * add_re
            states[block, kind, at, :width] += turned_re
            states[block, kind, at, width:] += turned_im
            add_re, add_im = turned_re, turned_im
        high, low = split_pair(states[block, kind])
        both = lax.dot_general(high, read[kind], contract, preferred_element_type=jnp.float32)
        rest = lax.dot_general(
            low, read[kind, :channels], contract, preferred_element_type=jnp.float32
        )
        summed = both[:, :channels] + both[:, channels:] + rest
        at = pl.multiple_of(layer * (kinds * channels) + kind * channels, channels)
        skip = skip_ref[:, pl.ds(at, channels)]
        own = inputs[block, :, kind * channels : (kind + 1) * channels].astype(jnp.float32)
        pieces.append(jax.nn.gelu(summed + skip * own).astype(jnp.bfloat16))
    out[...] = jnp.dot(
        token_shuffle(rows, True), jnp.concatenate(pieces, axis=1),
        preferred_element_type=jnp.float32,
    ).astype(jnp.bfloat16)


def whole_kernel(
    tokens_ref, query_ref, key_ref, value_ref, state_ref,
    in_re_ref, in_im_ref, out_re_ref, out_im_ref, attn_out_ref, state_out_ref,
    norm_gain_ref, out_gain_ref, decay_ref, rotation_ref, skip_ref,
    row_cos_ref, row_sin_ref, block_cos_ref, block_sin_ref, step_ref, sink_ref,
    out_ref,
    key_value, packed, weights, held, normed, in_re, in_im, out_re, out_im, drive, read, powers,
    queries, pairs, before, inputs, states, carries, ends, priors,
    mixers, matrices, partial, arrived, summed, pieces,
    load_sem, far_send, far_recv, line_send, line_recv, part_send, part_recv,
    side_send, side_recv, halo_send, halo_recv, end_send, end_recv,
    mixer_send, mixer_recv, matrix_send, matrix_recv, half_sem, piece_send, piece_recv,
):
    layers = held.shape[0]
    rows = pairs.shape[1]
    layer, spot, core = place()
    query_width, pair_width = (queries.shape[-1], pairs.shape[-1])
    state_width = inputs.shape[-1]
    groups = in_re.shape[0]
    mine = pl.ds(layer * groups, groups)
    loads = [
        pltpu.make_async_copy(key_ref, key_value.at[0], load_sem.at[0]),
        pltpu.make_async_copy(value_ref, key_value.at[1], load_sem.at[1]),
    ]
    spans = (
        (query_ref, query_width, 0, 0),
        (state_ref, state_width, query_width + pair_width, 2),
    )
    own_weights = [
        pltpu.make_async_copy(
            source.at[:, :, pl.ds(pl.multiple_of(layer * wide, wide), wide)],
            weights.at[layer, spot, :, :, pl.ds(to, wide)], load_sem.at[2 + at],
        )
        for source, wide, to, at in spans
    ]
    own_tokens = pltpu.make_async_copy(tokens_ref, held.at[layer], load_sem.at[3])
    table_loads = [
        pltpu.make_async_copy(source.at[mine], target, load_sem.at[5 + at])
        for at, (source, target) in enumerate(
            ((in_re_ref, in_re), (in_im_ref, in_im), (out_re_ref, out_re), (out_im_ref, out_im))
        )
    ]
    matrix_loads = [
        pltpu.make_async_copy(source, matrices.at[kind, spot], load_sem.at[9 + kind])
        for kind, source in enumerate((attn_out_ref, state_out_ref))
    ]
    for copy in loads + own_weights + [own_tokens] + table_loads + matrix_loads:
        copy.start()
    greet(layers, layer, spot, core)
    far = []
    for ahead in range(1, layers):
        other = lax.rem(layer + ahead, layers)
        for source, wide, to, at in spans:
            far.append(
                remote(
                    source.at[:, :, pl.ds(pl.multiple_of(other * wide, wide), wide)],
                    weights.at[layer, spot, :, :, pl.ds(to, wide)],
                    far_send.at[ahead, at], far_recv.at[ahead, at], {"sp": other * PLANE + spot},
                )
            )
            far[-1].start()
    for copy in loads:
        copy.wait()
    for at in range(layers):
        head = slice(at * HEAD, (at + 1) * HEAD)
        packed[at] = jnp.concatenate([key_value[0, :, :, head], key_value[1, :, :, head]], axis=-1)
    middle = pl.ds(query_width, pair_width)
    for ahead in range(1, layers):
        other = lax.rem(layer + ahead, layers)
        far.append(
            remote(
                packed.at[other], weights.at[layer, spot, :, :, middle],
                far_send.at[ahead, 1], far_recv.at[ahead, 1], {"sp": other * PLANE + spot},
            )
        )
        far[-1].start()
    weights[layer, spot, :, :, query_width : query_width + pair_width] = packed[layer]
    half_held = held.at[:, core]
    line_first(layers, layer, spot, tokens_ref.at[core], half_held, line_send, line_recv)
    for copy in own_weights:
        copy.wait()
    plane_first(
        weights.at[layer, spot], weights.at[layer], layer, spot, side_send.at[0], side_recv.at[0]
    )
    for copy in table_loads:
        copy.wait()
    make_tables(
        layer, rows, decay_ref, rotation_ref, step_ref, in_re, in_im, out_re, out_im,
        drive, read, powers,
    )
    before[0] = jnp.zeros(before.shape[1:], before.dtype)

    def to_partner(way, hop, block):
        remote(
            block, block, part_send.at[way, hop - 1], part_recv.at[way, hop - 1], {"tp": 1 - core}
        ).start()

    for ahead in range(layers):
        origin = lax.rem(layer + layers - ahead, layers)
        if ahead > 0:
            for at, (to, wide) in enumerate(
                ((0, query_width), (query_width, pair_width),
                 (query_width + pair_width, state_width))
            ):
                block = weights.at[origin, spot, :, :, pl.ds(to, wide)]
                remote(
                    block, block, far_send.at[ahead, at], far_recv.at[ahead, at], {"sp": 0}
                ).wait_recv()
            plane_first(
                weights.at[origin, spot], weights.at[origin], layer, spot,
                side_send.at[ahead], side_recv.at[ahead],
            )
        plane_pass(weights.at[origin], layer, spot, side_send.at[ahead], side_recv.at[ahead])
    for copy in matrix_loads:
        copy.wait()
    plane_first(
        matrices.at[0, spot], matrices.at[0], layer, spot, matrix_send.at[0], matrix_recv.at[0]
    )
    line_pass(layers, layer, spot, 1, half_held, line_send, line_recv, to_partner)
    own_tokens.wait()
    for ahead in range(layers):
        origin = lax.rem(layer + layers - ahead, layers)
        plane_landed(weights.at[origin], spot, side_send.at[ahead], side_recv.at[ahead])
    for copy in far:
        copy.wait_send()

    below, above = (layer, layers - 1 - layer)
    least = jnp.minimum(below, above)
    behind = layer * PLANE + lax.rem(spot + 1, PLANE)
    late = lax.div(spot, PLANE - 1)

    def hand_on(block):
        return remote(
            pairs.at[block], before.at[block + late], halo_send.at[block],
            halo_recv.at[block + late], {"sp": behind},
        )

    def arrive(block):
        remote(
            pairs.at[0], before.at[block], halo_send.at[0], halo_recv.at[block], {"sp": behind}
        ).wait_recv()

    def tell(block, at):
        other = lax.rem(spot + 1 + at, PLANE)
        return remote(
            ends.at[spot, block], ends.at[spot, block], end_send.at[at, block],
            end_recv.at[at, block], {"sp": layer * PLANE + other},
        )

    @pl.loop(0, layers)
    def _(at):
        paired = at <= 2 * least
        hop = jnp.where(paired, lax.div(at + 1, 2), at - least)
        way = jnp.where(paired, lax.rem(at + 1, 2), jnp.where(below > above, 1, 0))
        way = 1 - way
        block = jnp.where(at == 0, layer, jnp.where(way == 0, layer - hop, layer + hop))

        @pl.when(at > 0)
        def _():
            half = half_held.at[block]

            @pl.when(hop > 1)
            def _():
                remote(
                    half, half, line_send.at[way, 0], line_recv.at[way, hop - 1], {"sp": 0}
                ).wait_recv()
                onward = jnp.where(way == 0, layer < layers - 1, layer > 0)

                @pl.when(onward & (hop < layers - 1))
                def _():
                    remote(
                        half, half, line_send.at[way, hop], line_recv.at[way, hop],
                        {"sp": (layer + 1 - 2 * way) * PLANE + spot},
                    ).start()

                remote(
                    half, half, part_send.at[way, hop - 1], part_recv.at[way, hop - 1],
                    {"tp": 1 - core},
                ).start()

            other_half = held.at[block, 1 - core]
            remote(
                other_half, other_half, part_send.at[way, hop - 1], part_recv.at[way, hop - 1],
                {"tp": 1 - core},
            ).wait_recv()

        normalise(block, held, norm_gain_ref, normed)
        project_block(
            block, spot, normed, weights,
            (row_cos_ref, row_sin_ref, block_cos_ref, block_sin_ref), queries, pairs, inputs,
        )
        hand_on(block).start()
        scan_block(block, spot, inputs, drive, powers, states, carries, ends)
        for peer in range(PLANE - 1):
            tell(block, peer).start()

        @pl.when((spot > 0) | (block == 0) | ((at > 0) & (way == 1)))
        def _():
            @pl.when((spot > 0) | (block > 0))
            def _():
                arrive(block)

            attend_block(
                block, layer, spot, queries, pairs, before, sink_ref, mixers.at[layer, 0, block]
            )

        @pl.when((spot == 0) & (at > 0) & (way == 0))
        def _():
            arrive(block + 1)
            attend_block(
                block + 1, layer, spot, queries, pairs, before, sink_ref,
                mixers.at[layer, 0, block + 1],
            )

    @pl.when(spot == 0)
    def _():
        arrive(layers)

    for kind in (0, 1):
        if kind == 1:
            for block in range(layers):
                for peer in range(PLANE - 1):
                    tell(block, peer).wait()
            find_priors(ends, powers, priors)

            @pl.loop(0, layers)
            def _(block):
                read_block(
                    block, layer, spot, inputs, states, carries, priors, powers, read, skip_ref,
                    mixers.at[layer, 1, block],
                )

        line_first(
            layers, layer, spot, mixers.at[layer, kind], mixers.at[:, kind],
            mixer_send.at[kind], mixer_recv.at[kind],
        )
    plane_pass(matrices.at[0], layer, spot, matrix_send.at[0], matrix_recv.at[0])
    plane_first(
        matrices.at[1, spot], matrices.at[1], layer, spot, matrix_send.at[1], matrix_recv.at[1]
    )
    for hop in range(1, layers):
        for kind in (0, 1):
            line_pass(
                layers, layer, spot, hop, mixers.at[:, kind], mixer_send.at[kind],
                mixer_recv.at[kind],
            )
        if hop == 1:
            plane_pass(matrices.at[1], layer, spot, matrix_send.at[1], matrix_recv.at[1])
    for kind in (0, 1):
        plane_landed(matrices.at[kind], spot, matrix_send.at[kind], matrix_recv.at[kind])
        line_drain(
            layers, layer, mixers.at[layer, kind], mixers.at[:, kind], mixer_send.at[kind],
            mixer_recv.at[kind],
        )
    line_drain(layers, layer, tokens_ref.at[core], half_held, line_send, line_recv)
    for hop in range(1, layers):
        for way, there in ((0, layer - hop >= 0), (1, layer + hop <= layers - 1)):

            @pl.when(there)
            def _():
                block = held.at[layer, 0]
                remote(
                    block, block, part_send.at[way, hop - 1], part_recv.at[way, hop - 1],
                    {"tp": 1 - core},
                ).wait_send()

    for block in range(layers):
        hand_on(block).wait_send()

    depth = mixers.shape[-1]
    tokens = layers * rows
    half_depth, width = matrices.shape[3:]
    half_rows = rows // CORES

    @pl.loop(0, PLANE)
    def _(block):
        total = None
        for at in range(layers):
            for kind in (0, 1):
                low = at * depth
                piece = jnp.dot(
                    mixers[at, kind].reshape(tokens, depth),
                    matrices[kind, block, low // half_depth, pl.ds(low % half_depth, depth), :],
                    preferred_element_type=jnp.float32,
                )
                total = piece if total is None else total + piece
        rounded = total.astype(jnp.bfloat16).reshape(layers, CORES, half_rows, width)
        columns = pl.ds(pl.multiple_of(block * width, width), width)
        for half in range(CORES):
            partial[half, :, :, columns] = rounded[:, half]

    swap = remote(
        partial.at[1 - core], arrived, half_sem.at[0], half_sem.at[1], {"tp": 1 - core}
    )
    swap.start()
    swap.wait()
    for at in range(layers):
        summed[at] = (
            partial[core, at].astype(jnp.float32) + arrived[at].astype(jnp.float32)
        ).astype(jnp.bfloat16)
    copies = []
    for ahead in range(1, layers):
        other = lax.rem(layer + ahead, layers)
        copies.append(
            remote(
                summed.at[other], pieces.at[layer], piece_send.at[ahead], piece_recv.at[ahead],
                {"sp": other * PLANE + spot},
            )
        )
    for copy in copies:
        copy.start()
    pieces[layer] = summed[layer]
    for copy in copies:
        copy.wait()
    squares = jnp.zeros((half_rows, 1), jnp.float32)
    span = pieces.shape[-1]
    for at in range(layers):
        value = pieces[at].astype(jnp.float32)
        squares = squares + jnp.sum(value * value, axis=-1, keepdims=True)
    scale = lax.rsqrt(squares / (layers * span) + epsilon)
    for at in range(layers):
        columns = slice(at * span, (at + 1) * span)
        out_ref[:, columns] = (
            pieces[at].astype(jnp.float32) * scale * out_gain_ref[:, columns]
        ).astype(jnp.bfloat16)


def body(
    tokens,
    norm_gain,
    w_query,
    w_key,
    w_value,
    w_state_in,
    sink_logit,
    decay_rate,
    rotation,
    log_step,
    in_re,
    in_im,
    out_re,
    out_im,
    skip_gain,
    w_attn_out,
    w_state_out,
    out_gain,
):
    rows, model = tokens.shape
    layers = lax.axis_size("sp") // PLANE
    half_rows = rows // CORES
    depth = w_query.shape[0]
    query_width = w_query.shape[1] // layers
    pair_width = 2 * (w_key.shape[1] // layers)
    state_width = w_state_in.shape[1] // layers
    width = query_width + pair_width + state_width
    groups, states, group_width = (in_re.shape[0] // layers, in_re.shape[1], in_re.shape[2])
    kinds = state_width // LANES
    lanes = groups // kinds * states
    height, out_width = w_attn_out.shape
    half = HEAD // 2
    frequency = rotary_base ** (-(np.arange(half) * 2.0 / HEAD))
    frequency = np.tile(frequency, LANES // half)[None, :]
    within = np.arange(rows)[:, None] * frequency
    across = (np.arange(layers * PLANE) * rows)[:, None] * frequency
    tables = [np.cos(within), np.sin(within), np.cos(across), np.sin(across)]
    tables = [jnp.asarray(t, jnp.float32) for t in tables]
    anywhere = pl.BlockSpec(memory_space=pl.ANY)
    vmem = pl.BlockSpec(memory_space=pltpu.VMEM)
    smem = pl.BlockSpec(memory_space=pltpu.SMEM)
    dma = pltpu.SemaphoreType.DMA
    low, full = (jnp.bfloat16, jnp.float32)
    piece = pltpu.VMEM((layers, half_rows, PLANE * out_width), low)

    def halved(matrix):
        return matrix.reshape(2, matrix.shape[0] // 2, matrix.shape[1])

    return pl.pallas_call(
        whole_kernel,
        out_shape=jax.ShapeDtypeStruct((half_rows, model), low),
        in_specs=[anywhere] * 11 + [vmem] * 9 + [smem] * 2,
        out_specs=vmem,
        scratch_shapes=[
            pltpu.VMEM((2, 2, depth // 2, w_key.shape[1]), low),
            pltpu.VMEM((layers, 2, depth // 2, pair_width), low),
            pltpu.VMEM((layers, PLANE, 2, depth // 2, width), low),
            pltpu.VMEM((layers, CORES, half_rows, model), low),
            pltpu.VMEM((rows, model), low),
            pltpu.VMEM((groups, states, group_width), full),
            pltpu.VMEM((groups, states, group_width), full),
            pltpu.VMEM((groups, group_width, states), full),
            pltpu.VMEM((groups, group_width, states), full),
            pltpu.VMEM((kinds, 2 * LANES, 2 * lanes), low),
            pltpu.VMEM((kinds, 2 * LANES, 2 * lanes), low),
            pltpu.VMEM((4, SUB, groups * states), full),
            pltpu.VMEM((layers, rows, query_width), low),
            pltpu.VMEM((layers, rows, pair_width), low),
            pltpu.VMEM((layers + 1, rows, pair_width), low),
            pltpu.VMEM((layers, rows, state_width), low),
            pltpu.VMEM((layers, kinds, rows, 2 * lanes), full),
            pltpu.VMEM((layers, kinds, SUB, 2 * lanes), full),
            pltpu.VMEM((PLANE, layers, kinds, 1, 2 * lanes), full),
            pltpu.VMEM((layers * PLANE, kinds, 1, 2 * lanes), full),
            pltpu.VMEM((layers, 2, layers, rows, query_width), low),
            pltpu.VMEM((2, PLANE, 2, height // 2, out_width), low),
            pltpu.VMEM((CORES, layers, half_rows, PLANE * out_width), low),
            piece, piece, piece,
            dma((11,)), dma((layers, 3)), dma((layers, 3)),
            dma((2, layers)), dma((2, layers)), dma((2, layers)), dma((2, layers)),
            dma((layers, 2, 3)), dma((layers, 2, 3)), dma((layers,)), dma((layers + 1,)),
            dma((PLANE - 1, layers)), dma((PLANE - 1, layers)),
            dma((2, 2, layers)), dma((2, 2, layers)), dma((2, 2, 3)), dma((2, 2, 3)),
            dma((2,)), dma((layers,)), dma((layers,)),
        ],
        compiler_params=pltpu.CompilerParams(
            collective_id=0, has_side_effects=True, vmem_limit_bytes=60 * 2**20
        ),
    )(
        tokens.reshape(CORES, half_rows, model), halved(w_query), halved(w_key), halved(w_value),
        halved(w_state_in), in_re, in_im, out_re, out_im, halved(w_attn_out),
        halved(w_state_out), norm_gain.reshape(1, -1), out_gain.reshape(1, -1), decay_rate,
        rotation, skip_gain.reshape(1, -1), *tables, log_step, sink_logit,
    )


def suits(mesh, shapes):
    size, cores = (mesh.shape["sp"], mesh.shape["tp"])
    layers = size // PLANE
    query_width, key_width, state_width = (shapes[at][1] // cores for at in (2, 3, 5))
    return (
        size % PLANE == 0
        and layers > 1
        and layers % 2 == 0
        and cores == CORES
        and shapes[0][0] // size == WINDOW
        and key_width == layers * HEAD
        and state_width == query_width
        and query_width % (layers * LANES) == 0
    )


def solution(mesh):
    def run(*arrays):
        chosen = body if suits(mesh, [array.shape for array in arrays]) else whole_weights_body
        return sharded(mesh, chosen)(*arrays)

    return run


def sharded(mesh, chosen):
    return jax.shard_map(
        chosen,
        mesh=mesh,
        in_specs=(
            P("sp", None),
            P(),
            P("sp", "tp"),
            P("sp", "tp"),
            P("sp", "tp"),
            P("sp", "tp"),
            P("tp"),
            P("tp", None),
            P("tp", None),
            P("tp"),
            P("tp", None, None),
            P("tp", None, None),
            P("tp", None, None),
            P("tp", None, None),
            P("tp"),
            P("tp", "sp"),
            P("tp", "sp"),
            P(),
        ),
        out_specs=P(("sp", "tp"), None),
        check_vma=False,
    )
```

```python
import math

import jax
import jax.numpy as jnp
import numpy as np
from jax import lax
from jax.experimental import pallas as pl
from jax.experimental.pallas import tpu as pltpu
from jax.sharding import PartitionSpec as P

HEAD = 64
WINDOW = 128
SUB = 8


epsilon = 1e-06
rotary_base = 500000.0


def passed_along(value, axis, by):
    size = lax.axis_size(axis)
    pairs = [(i, i + by) for i in range(size) if 0 <= i + by < size]
    return lax.ppermute(value, axis, pairs)


def rotate(heads_block, positions):
    head_width = heads_block.shape[-1]
    half_width = head_width // 2
    frequency = rotary_base ** (-(jnp.arange(half_width, dtype=jnp.float32) * 2.0 / head_width))
    angles = positions.astype(jnp.float32)[:, None] * frequency[None, :]
    cosine = jnp.cos(angles)[:, None, :]
    sine_part = jnp.sin(angles)[:, None, :]
    lower_half = heads_block[..., :half_width]
    upper_half = heads_block[..., half_width:]
    return jnp.concatenate(
        [
            lower_half * cosine - upper_half * sine_part,
            upper_half * cosine + lower_half * sine_part,
        ],
        axis=-1,
    )


def shape_heads(query_sum, key_sum, value_sum, positions, head_width):
    row_count = query_sum.shape[0]
    kv_heads = key_sum.shape[1] // head_width
    group_size = query_sum.shape[1] // key_sum.shape[1]
    queries = rotate(
        query_sum.reshape(row_count, kv_heads * group_size, head_width), positions
    ).astype(jnp.bfloat16)
    queries = queries.reshape(row_count, kv_heads, group_size, head_width)
    key_rows = rotate(key_sum.reshape(row_count, kv_heads, head_width), positions).astype(
        jnp.bfloat16
    )
    key_rows = key_rows.reshape(row_count, kv_heads * head_width)
    value_rows = value_sum.astype(jnp.bfloat16)
    return (queries, key_rows, value_rows)


def band_attention(queries, key_rows, value_rows, sink_logit, first_row, window):
    row_count, kv_heads, group_size, head_width = queries.shape
    blocks = row_count // window
    query_blocks = queries.reshape(blocks, window, kv_heads, group_size, head_width)
    key_blocks = jnp.concatenate(
        [
            key_rows[:row_count].reshape(blocks, window, kv_heads, head_width),
            key_rows[window:].reshape(blocks, window, kv_heads, head_width),
        ],
        axis=1,
    )
    value_blocks = jnp.concatenate(
        [
            value_rows[:row_count].reshape(blocks, window, kv_heads, head_width),
            value_rows[window:].reshape(blocks, window, kv_heads, head_width),
        ],
        axis=1,
    )
    scores = jnp.einsum(
        "bqkgd,bskd->bkgqs", query_blocks, key_blocks, preferred_element_type=jnp.float32
    ) / math.sqrt(head_width)
    block_start = jnp.arange(blocks, dtype=jnp.int32)[:, None, None] * window
    query_at = first_row + block_start + jnp.arange(window, dtype=jnp.int32)[None, :, None]
    key_at = (
        first_row - window + block_start + jnp.arange(2 * window, dtype=jnp.int32)[None, None, :]
    )
    offset_gap = query_at - key_at
    visible = (offset_gap >= 0) & (offset_gap < window) & (key_at >= 0)
    scores = jnp.where(visible[:, None, None, :, :], scores, -jnp.inf)
    sink_value = sink_logit.reshape(1, kv_heads, group_size, 1, 1)
    top_score = jnp.maximum(jnp.max(scores, axis=-1, keepdims=True), sink_value)
    exponent = jnp.exp(scores - top_score)
    totals = jnp.sum(exponent, axis=-1, keepdims=True) + jnp.exp(sink_value - top_score)
    weights = (exponent / totals).astype(jnp.bfloat16)
    attended = jnp.einsum(
        "bkgqs,bskd->bqkgd", weights, value_blocks, preferred_element_type=jnp.float32
    )
    return attended.reshape(row_count, kv_heads * group_size * head_width).astype(jnp.bfloat16)


def discretize(decay_rate, rotation, log_step, in_re, in_im):
    time_step = jnp.exp(log_step)[:, None]
    lambda_re = -decay_rate
    modulus = jnp.exp(lambda_re * time_step)
    pole_re = modulus * jnp.cos(rotation * time_step)
    pole_im = modulus * jnp.sin(rotation * time_step)
    minus_one = pole_re - 1.0
    denominator = lambda_re * lambda_re + rotation * rotation
    factor_re = ((minus_one * lambda_re + pole_im * rotation) / denominator)[..., None]
    factor_im = ((pole_im * lambda_re - minus_one * rotation) / denominator)[..., None]
    drive_re = factor_re * in_re - factor_im * in_im
    drive_im = factor_re * in_im + factor_im * in_re
    return (pole_re, pole_im, drive_re, drive_im)


def complex_power(decay_rate, rotation, log_step, exponent):
    time_step = jnp.exp(log_step)[:, None]
    modulus = jnp.exp(-decay_rate * time_step * exponent)
    angle = rotation * time_step * exponent
    return (modulus * jnp.cos(angle), modulus * jnp.sin(angle))


def token_shuffle(rows, inverse):
    steps = rows // SUB
    out_row = lax.broadcasted_iota(jnp.int32, (rows, rows), 1 if inverse else 0)
    in_row = lax.broadcasted_iota(jnp.int32, (rows, rows), 0 if inverse else 1)
    token = (out_row % SUB) * steps + out_row // SUB
    return (token == in_row).astype(jnp.bfloat16)


def scan_kernel(
    u_ref, drive_ref, pole_re_ref, pole_im_ref, jump_re_ref, jump_im_ref,
    state_ref, carry_re_ref, carry_im_ref, end_re_ref, end_im_ref,
):
    rows = u_ref.shape[0]
    width = pole_re_ref.shape[-1]
    shuffle = token_shuffle(rows, False)
    shuffled = jnp.dot(shuffle, u_ref[...], preferred_element_type=jnp.float32)
    state_ref[...] = jnp.dot(
        shuffled, drive_ref[0], precision=lax.Precision.HIGHEST,
        preferred_element_type=jnp.float32,
    )
    pole_re = jnp.broadcast_to(pole_re_ref[0], (SUB, width))
    pole_im = jnp.broadcast_to(pole_im_ref[0], (SUB, width))
    now_re = jnp.zeros((SUB, width), jnp.float32)
    now_im = jnp.zeros((SUB, width), jnp.float32)
    for step in range(rows // SUB):
        at = slice(step * SUB, (step + 1) * SUB)
        new_re = pole_re * now_re - pole_im * now_im + state_ref[at, :width]
        new_im = pole_re * now_im + pole_im * now_re + state_ref[at, width:]
        state_ref[at, :width] = new_re
        state_ref[at, width:] = new_im
        now_re, now_im = new_re, new_im
    jump_re, jump_im = (jump_re_ref[0], jump_im_ref[0])
    held_re = jnp.zeros((1, width), jnp.float32)
    held_im = jnp.zeros((1, width), jnp.float32)
    for chunk in range(SUB):
        carry_re_ref[chunk : chunk + 1, :] = held_re
        carry_im_ref[chunk : chunk + 1, :] = held_im
        next_re = jump_re * held_re - jump_im * held_im + now_re[chunk : chunk + 1]
        next_im = jump_re * held_im + jump_im * held_re + now_im[chunk : chunk + 1]
        held_re, held_im = next_re, next_im
    end_re_ref[0] = held_re
    end_im_ref[0] = held_im


def readout_kernel(
    u_ref, state_ref, carry_re_ref, carry_im_ref, prior_re_ref, prior_im_ref,
    chunk_re_ref, chunk_im_ref, pole_re_ref, pole_im_ref, read_ref, skip_ref, out_ref, full_ref,
):
    rows = u_ref.shape[0]
    width = pole_re_ref.shape[-1]
    prior_re, prior_im = (prior_re_ref[0], prior_im_ref[0])
    chunk_re, chunk_im = (chunk_re_ref[...], chunk_im_ref[...])
    add_re = carry_re_ref[...] + chunk_re * prior_re - chunk_im * prior_im
    add_im = carry_im_ref[...] + chunk_re * prior_im + chunk_im * prior_re
    pole_re = jnp.broadcast_to(pole_re_ref[0], (SUB, width))
    pole_im = jnp.broadcast_to(pole_im_ref[0], (SUB, width))
    for step in range(rows // SUB):
        at = slice(step * SUB, (step + 1) * SUB)
        turned_re = pole_re * add_re - pole_im * add_im
        turned_im = pole_re * add_im + pole_im * add_re
        full_ref[at, :width] = state_ref[at, :width] + turned_re
        full_ref[at, width:] = state_ref[at, width:] + turned_im
        add_re, add_im = turned_re, turned_im
    summed = jnp.dot(
        full_ref[...], read_ref[0], precision=lax.Precision.HIGHEST,
        preferred_element_type=jnp.float32,
    )
    shuffled = jnp.dot(
        token_shuffle(rows, False), u_ref[...], preferred_element_type=jnp.float32
    )
    mixed = jax.nn.gelu(summed + skip_ref[...] * shuffled).astype(jnp.bfloat16)
    out_ref[...] = jnp.dot(
        token_shuffle(rows, True), mixed, preferred_element_type=jnp.float32
    ).astype(jnp.bfloat16)


def block_diagonal(parts):
    blocks, per, rows, columns = parts[0].shape
    same = jnp.eye(per, dtype=bool)[None, :, None, :, None]
    spread = [
        jnp.where(same, part[:, :, :, None, :], 0.0).reshape(blocks, per * rows, per * columns)
        for part in parts
    ]
    return jnp.concatenate(spread, axis=2)


def state_tables(rows, decay_rate, rotation, log_step, in_re, in_im, out_re, out_im):
    groups, states = decay_rate.shape
    group_width = in_re.shape[-1]
    per = min(groups, max(1, 128 // group_width))
    blocks, width = (groups // per, per * states)
    pole_re, pole_im, drive_re, drive_im = discretize(decay_rate, rotation, log_step, in_re, in_im)
    steps = rows // SUB

    def by_block(value):
        return value.reshape(blocks, per, *value.shape[1:])

    def flat(value):
        return value.reshape(blocks, 1, width)

    drive = block_diagonal(
        [by_block(jnp.swapaxes(drive_re, 1, 2)), by_block(jnp.swapaxes(drive_im, 1, 2))]
    )
    read = jnp.swapaxes(block_diagonal([by_block(out_re), by_block(-out_im)]), 1, 2)
    jump = complex_power(decay_rate, rotation, log_step, float(steps))
    chunk_powers = [
        complex_power(decay_rate, rotation, log_step, float(steps * c)) for c in range(SUB)
    ]
    chunk_re = jnp.stack([p[0].reshape(groups * states) for p in chunk_powers])
    chunk_im = jnp.stack([p[1].reshape(groups * states) for p in chunk_powers])
    return dict(
        drive=drive, read=read, pole_re=flat(pole_re), pole_im=flat(pole_im),
        jump_re=flat(jump[0]), jump_im=flat(jump[1]), chunk_re=chunk_re, chunk_im=chunk_im,
        blocks=blocks, width=width, channels=per * group_width,
    )


def local_scan(inputs, tables):
    rows = inputs.shape[0]
    blocks, width, channels = (tables["blocks"], tables["width"], tables["channels"])
    row_spec = pl.BlockSpec((1, 1, width), lambda b: (b, 0, 0))
    carry_spec = pl.BlockSpec((SUB, width), lambda b: (0, b))
    return pl.pallas_call(
        scan_kernel,
        grid=(blocks,),
        in_specs=[
            pl.BlockSpec((rows, channels), lambda b: (0, b)),
            pl.BlockSpec((1, channels, 2 * width), lambda b: (b, 0, 0)),
            row_spec, row_spec, row_spec, row_spec,
        ],
        out_specs=[
            pl.BlockSpec((rows, 2 * width), lambda b: (0, b)),
            carry_spec, carry_spec, row_spec, row_spec,
        ],
        out_shape=[
            jax.ShapeDtypeStruct((rows, 2 * width * blocks), jnp.float32),
            jax.ShapeDtypeStruct((SUB, width * blocks), jnp.float32),
            jax.ShapeDtypeStruct((SUB, width * blocks), jnp.float32),
            jax.ShapeDtypeStruct((blocks, 1, width), jnp.float32),
            jax.ShapeDtypeStruct((blocks, 1, width), jnp.float32),
        ],
        cost_estimate=pl.CostEstimate(
            flops=12 * rows * channels * width * blocks, bytes_accessed=10**7, transcendentals=0
        ),
    )(
        inputs, tables["drive"], tables["pole_re"], tables["pole_im"],
        tables["jump_re"], tables["jump_im"],
    )


def read_states(inputs, scanned, prior_re, prior_im, tables, skip_gain):
    rows = inputs.shape[0]
    state, carry_re, carry_im = scanned[:3]
    blocks, width, channels = (tables["blocks"], tables["width"], tables["channels"])
    row_spec = pl.BlockSpec((1, 1, width), lambda b: (b, 0, 0))
    carry_spec = pl.BlockSpec((SUB, width), lambda b: (0, b))
    return pl.pallas_call(
        readout_kernel,
        grid=(blocks,),
        in_specs=[
            pl.BlockSpec((rows, channels), lambda b: (0, b)),
            pl.BlockSpec((rows, 2 * width), lambda b: (0, b)),
            carry_spec, carry_spec, row_spec, row_spec, carry_spec, carry_spec,
            row_spec, row_spec,
            pl.BlockSpec((1, 2 * width, channels), lambda b: (b, 0, 0)),
            pl.BlockSpec((1, channels), lambda b: (0, b)),
        ],
        out_specs=pl.BlockSpec((rows, channels), lambda b: (0, b)),
        out_shape=jax.ShapeDtypeStruct((rows, channels * blocks), jnp.bfloat16),
        scratch_shapes=[pltpu.VMEM((rows, 2 * width), jnp.float32)],
        cost_estimate=pl.CostEstimate(
            flops=12 * rows * channels * width * blocks, bytes_accessed=10**7, transcendentals=0
        ),
    )(
        inputs, state, carry_re, carry_im, prior_re, prior_im,
        tables["chunk_re"], tables["chunk_im"], tables["pole_re"], tables["pole_im"],
        tables["read"], skip_gain.reshape(1, -1),
    )


def carried_state(end_re, end_im, decay_rate, rotation, log_step, rows):
    ends = jnp.stack([end_re, end_im])
    shape = end_re.shape
    size = lax.axis_size("sp")
    reach = 1
    while reach < size:
        power_re, power_im = complex_power(decay_rate, rotation, log_step, float(rows * reach))
        power_re, power_im = (power_re.reshape(shape), power_im.reshape(shape))
        prior = passed_along(ends, "sp", reach)
        ends = ends + jnp.stack(
            [
                power_re * prior[0] - power_im * prior[1],
                power_re * prior[1] + power_im * prior[0],
            ]
        )
        reach *= 2
    before = passed_along(ends, "sp", 1)
    return (before[0], before[1])


def state_branch(inputs, decay_rate, rotation, log_step, in_re, in_im, out_re, out_im, skip_gain):
    rows = inputs.shape[0]
    tables = state_tables(rows, decay_rate, rotation, log_step, in_re, in_im, out_re, out_im)
    scanned = local_scan(inputs, tables)
    prior_re, prior_im = carried_state(
        scanned[3], scanned[4], decay_rate, rotation, log_step, rows
    )
    return read_states(inputs, scanned, prior_re, prior_im, tables, skip_gain)


def earlier_window(key_rows, value_rows):
    joined = jnp.concatenate([key_rows, value_rows], axis=1)
    prior = passed_along(joined, "sp", 1)
    return jnp.concatenate([prior, joined], axis=0)


def make_adder(normed_cols):

    def add_pieces(carried, weight_pieces, row_start):
        updated = []
        for running_total, weight_piece in zip(carried, weight_pieces):
            product = lax.dot_general(
                normed_cols,
                weight_piece,
                (((0,), (0,)), ((), ())),
                preferred_element_type=jnp.float32,
            )
            updated.append(product)
        return tuple(updated)

    return add_pieces


def whole_weights_body(
    tokens,
    norm_gain,
    w_query,
    w_key,
    w_value,
    w_state_in,
    sink_logit,
    decay_rate,
    rotation,
    log_step,
    in_re,
    in_im,
    out_re,
    out_im,
    skip_gain,
    w_attn_out,
    w_state_out,
    out_gain,
):
    row_count = tokens.shape[0]
    window = WINDOW
    head_width = HEAD
    wide_tokens = tokens.astype(jnp.float32)
    normed = (
        wide_tokens
        * lax.rsqrt(jnp.mean(wide_tokens * wide_tokens, axis=-1, keepdims=True) + epsilon)
        * norm_gain
    ).astype(jnp.bfloat16)
    first_row = lax.axis_index("sp") * row_count
    positions = first_row + jnp.arange(row_count, dtype=jnp.int32)
    add_pieces = make_adder(jnp.transpose(normed))

    def empty_like(weight_shard):
        return jnp.zeros((row_count, weight_shard.shape[1]), jnp.float32)

    query_sum, key_sum, value_sum, input_sum = add_pieces(
        (empty_like(w_query), empty_like(w_key), empty_like(w_value), empty_like(w_state_in)),
        (
            lax.all_gather(w_query, "sp", axis=0, tiled=True),
            lax.all_gather(w_key, "sp", axis=0, tiled=True),
            lax.all_gather(w_value, "sp", axis=0, tiled=True),
            lax.all_gather(w_state_in, "sp", axis=0, tiled=True),
        ),
        jnp.int32(0),
    )
    queries, key_rows, value_rows = shape_heads(
        query_sum, key_sum, value_sum, positions, head_width
    )
    joined_rows = earlier_window(key_rows, value_rows)
    inputs = input_sum.astype(jnp.bfloat16)
    mixed_state = state_branch(
        inputs, decay_rate, rotation, log_step, in_re, in_im, out_re, out_im, skip_gain
    )
    kv_width = key_rows.shape[1]
    kv_heads = kv_width // head_width
    all_keys = joined_rows[:, :kv_width].reshape(window + row_count, kv_heads, head_width)
    all_values = joined_rows[:, kv_width:].reshape(window + row_count, kv_heads, head_width)
    attended = band_attention(queries, all_keys, all_values, sink_logit, first_row, window)
    attn_rows, state_rows = (
        lax.all_gather(w_attn_out, "sp", axis=1, tiled=True),
        lax.all_gather(w_state_out, "sp", axis=1, tiled=True),
    )
    projected = lax.psum_scatter(
        (
            jnp.dot(attended, attn_rows, preferred_element_type=jnp.float32)
            + jnp.dot(mixed_state, state_rows, preferred_element_type=jnp.float32)
        ).astype(jnp.bfloat16),
        "tp",
        scatter_dimension=0,
        tiled=True,
    ).astype(jnp.float32)
    row_scale = lax.rsqrt(jnp.mean(projected * projected, axis=-1, keepdims=True) + epsilon)
    return (projected * row_scale * out_gain).astype(jnp.bfloat16)


SIDE = 2
PLANE = SIDE * SIDE
CORES = 2
LANES = 128
MESH = pl.DeviceIdType.MESH


def place():
    me = lax.axis_index("sp")
    return (lax.div(me, PLANE), lax.rem(me, PLANE), lax.axis_index("tp"))


def plane_neighbours(spot):
    beside = spot + 1 - 2 * lax.rem(spot, SIDE)
    above = spot + SIDE - 2 * SIDE * lax.div(spot, SIDE)
    return (beside, above)


def greet(layers, layer, spot, core):
    barrier = pltpu.get_barrier_semaphore()
    beside, above = plane_neighbours(spot)
    for ahead in range(1, layers):
        other = lax.rem(layer + ahead, layers)
        pl.semaphore_signal(
            barrier, inc=1, device_id={"sp": other * PLANE + spot}, device_id_type=MESH
        )
    for other in (beside, above, PLANE - 1 - spot):
        pl.semaphore_signal(
            barrier, inc=1, device_id={"sp": layer * PLANE + other}, device_id_type=MESH
        )
    pl.semaphore_signal(barrier, inc=1, device_id={"tp": 1 - core}, device_id_type=MESH)
    pl.semaphore_wait(barrier, layers + 3)


def remote(source, target, send_sem, recv_sem, device):
    return pltpu.make_async_remote_copy(
        src_ref=source, dst_ref=target, send_sem=send_sem, recv_sem=recv_sem,
        device_id=device, device_id_type=MESH,
    )


def line_first(layers, layer, spot, source, held, send_sems, recv_sems):
    @pl.when(layer < layers - 1)
    def _():
        remote(
            source, held.at[layer], send_sems.at[0, 0], recv_sems.at[0, 0],
            {"sp": (layer + 1) * PLANE + spot},
        ).start()

    @pl.when(layer > 0)
    def _():
        remote(
            source, held.at[layer], send_sems.at[1, 0], recv_sems.at[1, 0],
            {"sp": (layer - 1) * PLANE + spot},
        ).start()


def line_pass(layers, layer, spot, hop, held, send_sems, recv_sems, landed=None):
    @pl.when(layer - hop >= 0)
    def _():
        block = held.at[layer - hop]
        remote(block, block, send_sems.at[0, 0], recv_sems.at[0, hop - 1], {"sp": 0}).wait_recv()

        @pl.when(layer < layers - 1)
        def _():
            if hop < layers - 1:
                remote(
                    block, block, send_sems.at[0, hop], recv_sems.at[0, hop],
                    {"sp": (layer + 1) * PLANE + spot},
                ).start()

        if landed is not None:
            landed(0, hop, block)

    @pl.when(layer + hop <= layers - 1)
    def _():
        block = held.at[layer + hop]
        remote(block, block, send_sems.at[1, 0], recv_sems.at[1, hop - 1], {"sp": 0}).wait_recv()

        @pl.when(layer > 0)
        def _():
            if hop < layers - 1:
                remote(
                    block, block, send_sems.at[1, hop], recv_sems.at[1, hop],
                    {"sp": (layer - 1) * PLANE + spot},
                ).start()

        if landed is not None:
            landed(1, hop, block)


def line_drain(layers, layer, source, held, send_sems, recv_sems):
    for hop in range(layers - 1):

        @pl.when((layer - hop >= 0) & (layer < layers - 1))
        def _():
            remote(
                source, held.at[layer], send_sems.at[0, hop], recv_sems.at[0, 0], {"sp": 0}
            ).wait_send()

        @pl.when((layer + hop <= layers - 1) & (layer > 0))
        def _():
            remote(
                source, held.at[layer], send_sems.at[1, hop], recv_sems.at[1, 0], {"sp": 0}
            ).wait_send()


def plane_halves(halves, slots, layer, spot, send_sems, recv_sems, half):
    beside, above = plane_neighbours(spot)
    return [
        remote(
            halves.at[half], slots.at[spot, half], send_sems.at[0, half],
            recv_sems.at[0, half], {"sp": layer * PLANE + beside},
        ),
        remote(
            halves.at[1 - half], slots.at[spot, 1 - half], send_sems.at[1, 1 - half],
            recv_sems.at[1, 1 - half], {"sp": layer * PLANE + above},
        ),
    ]


def plane_first(halves, slots, layer, spot, send_sems, recv_sems):
    for half in (0, 1):
        for copy in plane_halves(halves, slots, layer, spot, send_sems, recv_sems, half):
            copy.start()


def plane_pass(slots, layer, spot, send_sems, recv_sems):
    beside, above = plane_neighbours(spot)
    block = slots.at[beside, 0]
    remote(block, block, send_sems.at[0, 0], recv_sems.at[0, 0], {"sp": 0}).wait_recv()
    remote(
        block, block, send_sems.at[1, 2], recv_sems.at[1, 2], {"sp": layer * PLANE + above}
    ).start()
    block = slots.at[above, 1]
    remote(block, block, send_sems.at[0, 0], recv_sems.at[1, 1], {"sp": 0}).wait_recv()
    remote(
        block, block, send_sems.at[0, 2], recv_sems.at[0, 2], {"sp": layer * PLANE + beside}
    ).start()


def plane_landed(slots, spot, send_sems, recv_sems):
    for way, half in ((0, 1), (1, 0), (0, 2), (1, 2)):
        block = slots.at[spot, 0]
        remote(block, block, send_sems.at[0, 0], recv_sems.at[way, half], {"sp": 0}).wait_recv()
    for way in (0, 1):
        for half in (0, 1, 2):
            block = slots.at[spot, 0]
            remote(block, block, send_sems.at[way, half], recv_sems.at[0, 0], {"sp": 0}).wait_send()


def lanes_of(rows):
    return jnp.concatenate([rows[at : at + 1] for at in range(rows.shape[0])], axis=1)


def split_pair(value):
    high = value.astype(jnp.bfloat16)
    return (high, (value - high.astype(jnp.float32)).astype(jnp.bfloat16))


def make_tables(
    layer, rows, decay_ref, rotation_ref, step_ref, in_re_ref, in_im_ref, out_re_ref, out_im_ref,
    drive, read, powers,
):
    groups, group_width, states = in_re_ref.shape
    kinds, _, width2 = drive.shape
    per = groups // kinds
    width = per * states
    channels = per * group_width
    base = layer * groups
    decay = lanes_of(decay_ref[pl.ds(base, groups), :])
    rotation = lanes_of(rotation_ref[pl.ds(base, groups), :])
    step = jnp.exp(
        jnp.concatenate(
            [jnp.full((1, states), step_ref[base + at], jnp.float32) for at in range(groups)],
            axis=1,
        )
    )
    row = lax.broadcasted_iota(jnp.int32, (SUB, groups * states), 0)
    steps = rows // SUB
    shares = (row * steps, jnp.where(row == 0, 1, jnp.where(row == 1, steps, rows)))
    for at, share in enumerate(shares):
        share = share.astype(jnp.float32)
        modulus = jnp.exp(-decay * step * share)
        angle = rotation * step * share
        powers[2 * at] = modulus * jnp.cos(angle)
        powers[2 * at + 1] = modulus * jnp.sin(angle)
    pole_re, pole_im = (powers[2, 0:1, :], powers[3, 0:1, :])
    minus_one = pole_re - 1.0
    denominator = decay * decay + rotation * rotation
    factor_re = (pole_im * rotation - minus_one * decay) / denominator
    factor_im = (-pole_im * decay - minus_one * rotation) / denominator
    same = (
        lax.broadcasted_iota(jnp.int32, (channels, width), 0) // group_width
        == lax.broadcasted_iota(jnp.int32, (channels, width), 1) // states
    )

    def spread(pieces):
        beside = jnp.concatenate(pieces, axis=1)
        return jnp.concatenate([beside] * per, axis=0)

    for kind in range(kinds):
        lanes = slice(kind * width, (kind + 1) * width)
        f_re, f_im = (factor_re[:, lanes], factor_im[:, lanes])
        own = range(kind * per, (kind + 1) * per)
        m_re = spread([in_re_ref[at] for at in own])
        m_im = spread([in_im_ref[at] for at in own])
        for part, value in ((0, f_re * m_re - f_im * m_im), (1, f_re * m_im + f_im * m_re)):
            high, low = split_pair(jnp.where(same, value, 0.0))
            columns = slice(part * width, (part + 1) * width)
            drive[kind, :channels, columns] = high
            drive[kind, channels:, columns] = low
        r_re = spread([out_re_ref[at] for at in own])
        r_im = spread([-out_im_ref[at] for at in own])
        for part, value in ((0, r_re), (1, r_im)):
            high, low = split_pair(jnp.where(same, value, 0.0))
            columns = slice(part * width, (part + 1) * width)
            read[kind, :channels, columns] = high
            read[kind, channels:, columns] = low


def normalise(block, held, gain_ref, normed):
    _, parts, part_rows, model = held.shape
    tall = 16
    per = part_rows // tall

    @pl.loop(0, parts * per)
    def _(at):
        value = held[
            block, at // per, pl.ds(pl.multiple_of((at % per) * tall, tall), tall), :
        ].astype(jnp.float32)
        scale = lax.rsqrt(jnp.sum(value * value, axis=-1, keepdims=True) / model + epsilon)
        normed[pl.ds(pl.multiple_of(at * tall, tall), tall), :] = (
            value * scale * gain_ref[...]
        ).astype(jnp.bfloat16)


def project_block(block, spot, normed, weights, tables, queries, pairs, inputs):
    rows, model = normed.shape
    layers = weights.shape[0]
    depth = weights.shape[2] * weights.shape[3]
    query_width, pair_width = (queries.shape[-1], pairs.shape[-1])
    half_width = HEAD // 2
    row_cos_ref, row_sin_ref, block_cos_ref, block_sin_ref = tables
    lane = lax.broadcasted_iota(jnp.int32, (rows, LANES), 1)
    low = lax.rem(lane, HEAD) < half_width

    def turn(value, cosine, sine):
        swapped = jnp.where(
            low, -pltpu.roll(value, LANES - half_width, 1), pltpu.roll(value, half_width, 1)
        )
        return value * cosine + swapped * sine

    total = None
    for at in range(layers * PLANE):
        piece = jnp.dot(
            normed[:, at * depth : (at + 1) * depth],
            weights[at // PLANE, at % PLANE].reshape(depth, weights.shape[-1]),
            preferred_element_type=jnp.float32,
        )
        total = piece if total is None else total + piece
    here = pl.ds(block * PLANE + spot, 1)
    block_cos, block_sin = (block_cos_ref[here, :], block_sin_ref[here, :])
    cosine = row_cos_ref[...] * block_cos - row_sin_ref[...] * block_sin
    sine = row_sin_ref[...] * block_cos + row_cos_ref[...] * block_sin
    turned = [turn(total[:, at : at + LANES], cosine, sine) for at in range(0, query_width, LANES)]
    queries[block] = jnp.concatenate(turned, axis=1).astype(jnp.bfloat16)
    value = total[:, query_width : query_width + pair_width]
    pairs[block] = jnp.where(lane < HEAD, turn(value, cosine, sine), value).astype(jnp.bfloat16)
    inputs[block] = jnp.dot(
        token_shuffle(rows, False), total[:, query_width + pair_width :].astype(jnp.bfloat16),
        preferred_element_type=jnp.float32,
    ).astype(jnp.bfloat16)


def scan_block(block, spot, inputs, drive, powers, states, carries, ends):
    kinds, _, width2 = drive.shape
    width = width2 // 2
    channels = inputs.shape[-1] // kinds
    rows = inputs.shape[1]
    for kind in range(kinds):
        lanes = slice(kind * width, (kind + 1) * width)
        own = inputs[block, :, kind * channels : (kind + 1) * channels]
        states[block, kind] = jnp.dot(
            jnp.concatenate([own, own], axis=1), drive[kind], preferred_element_type=jnp.float32
        )
        pole_re = jnp.broadcast_to(powers[2, 0:1, lanes], (SUB, width))
        pole_im = jnp.broadcast_to(powers[3, 0:1, lanes], (SUB, width))
        now_re = jnp.zeros((SUB, width), jnp.float32)
        now_im = jnp.zeros((SUB, width), jnp.float32)
        for step in range(rows // SUB):
            at = slice(step * SUB, (step + 1) * SUB)
            new_re = pole_re * now_re - pole_im * now_im + states[block, kind, at, :width]
            new_im = pole_re * now_im + pole_im * now_re + states[block, kind, at, width:]
            states[block, kind, at, :width] = new_re
            states[block, kind, at, width:] = new_im
            now_re, now_im = new_re, new_im
        jump_re, jump_im = (powers[2, 1:2, lanes], powers[3, 1:2, lanes])
        held_re = jnp.zeros((1, width), jnp.float32)
        held_im = jnp.zeros((1, width), jnp.float32)
        re, im = ([], [])
        for chunk in range(SUB):
            re.append(held_re)
            im.append(held_im)
            next_re = jump_re * held_re - jump_im * held_im + now_re[chunk : chunk + 1]
            next_im = jump_re * held_im + jump_im * held_re + now_im[chunk : chunk + 1]
            held_re, held_im = next_re, next_im
        carries[block, kind, :, :width] = jnp.concatenate(re, axis=0)
        carries[block, kind, :, width:] = jnp.concatenate(im, axis=0)
        ends[spot, block, kind, :, :width] = held_re
        ends[spot, block, kind, :, width:] = held_im


def attend_block(block, layer, spot, queries, pairs, before, sink_ref, out):
    rows, query_width = queries.shape[1:]
    group = query_width // HEAD
    pair, prior = (pairs[block], before[block])
    keys = jnp.concatenate([prior[:, :HEAD], pair[:, :HEAD]], axis=0)
    values = jnp.concatenate([prior[:, HEAD:], pair[:, HEAD:]], axis=0)
    query_at = lax.broadcasted_iota(jnp.int32, (rows, rows + WINDOW), 0)
    key_at = lax.broadcasted_iota(jnp.int32, (rows, rows + WINDOW), 1) - WINDOW
    gap = query_at - key_at
    first = (block * PLANE + spot) * rows
    visible = (gap >= 0) & (gap < WINDOW) & (key_at + first >= 0)
    pieces = []
    for head in range(group):
        query = queries[block, :, head * HEAD : (head + 1) * HEAD]
        scores = lax.dot_general(
            query, keys, (((1,), (1,)), ((), ())), preferred_element_type=jnp.float32
        ) / math.sqrt(HEAD)
        scores = jnp.where(visible, scores, -jnp.inf)
        sink = jnp.full((1, 1), sink_ref[layer * group + head], jnp.float32)
        top = jnp.maximum(jnp.max(scores, axis=-1, keepdims=True), sink)
        exponent = jnp.exp(scores - top)
        total = jnp.sum(exponent, axis=-1, keepdims=True) + jnp.exp(sink - top)
        weights = (exponent / total).astype(jnp.bfloat16)
        pieces.append(jnp.dot(weights, values, preferred_element_type=jnp.float32))
    out[...] = jnp.concatenate(pieces, axis=1).astype(jnp.bfloat16)


def find_priors(ends, powers, priors):
    plane, layers, kinds = ends.shape[:3]
    width = ends.shape[-1] // 2
    for kind in range(kinds):
        lanes = slice(kind * width, (kind + 1) * width)
        power_re, power_im = (powers[2, 2:3, lanes], powers[3, 2:3, lanes])
        held_re = jnp.zeros((1, width), jnp.float32)
        held_im = jnp.zeros((1, width), jnp.float32)
        for at in range(layers * plane):
            priors[at, kind, :, :width] = held_re
            priors[at, kind, :, width:] = held_im
            end_re = ends[at % plane, at // plane, kind, :, :width]
            end_im = ends[at % plane, at // plane, kind, :, width:]
            held_re, held_im = (
                power_re * held_re - power_im * held_im + end_re,
                power_re * held_im + power_im * held_re + end_im,
            )


def read_block(block, layer, spot, inputs, states, carries, priors, powers, read, skip_ref, out):
    kinds, channels2, width2 = read.shape
    width, channels = (width2 // 2, channels2 // 2)
    rows = inputs.shape[1]
    contract = (((1,), (1,)), ((), ()))
    pieces = []
    for kind in range(kinds):
        lanes = slice(kind * width, (kind + 1) * width)
        prior_re = priors[block * PLANE + spot, kind, :, :width]
        prior_im = priors[block * PLANE + spot, kind, :, width:]
        chunk_re, chunk_im = (powers[0, :, lanes], powers[1, :, lanes])
        add_re = carries[block, kind, :, :width] + chunk_re * prior_re - chunk_im * prior_im
        add_im = carries[block, kind, :, width:] + chunk_re * prior_im + chunk_im * prior_re
        pole_re = jnp.broadcast_to(powers[2, 0:1, lanes], (SUB, width))
        pole_im = jnp.broadcast_to(powers[3, 0:1, lanes], (SUB, width))
        for step in range(rows // SUB):
            at = slice(step * SUB, (step + 1) * SUB)
            turned_re = pole_re * add_re - pole_im * add_im
            turned_im = pole_re * add_im + pole_im * add_re
            states[block, kind, at, :width] += turned_re
            states[block, kind, at, width:] += turned_im
            add_re, add_im = turned_re, turned_im
        high, low = split_pair(states[block, kind])
        both = lax.dot_general(high, read[kind], contract, preferred_element_type=jnp.float32)
        rest = lax.dot_general(
            low, read[kind, :channels], contract, preferred_element_type=jnp.float32
        )
        summed = both[:, :channels] + both[:, channels:] + rest
        at = pl.multiple_of(layer * (kinds * channels) + kind * channels, channels)
        skip = skip_ref[:, pl.ds(at, channels)]
        own = inputs[block, :, kind * channels : (kind + 1) * channels].astype(jnp.float32)
        pieces.append(jax.nn.gelu(summed + skip * own).astype(jnp.bfloat16))
    out[...] = jnp.dot(
        token_shuffle(rows, True), jnp.concatenate(pieces, axis=1),
        preferred_element_type=jnp.float32,
    ).astype(jnp.bfloat16)


def whole_kernel(
    tokens_ref, query_ref, key_ref, value_ref, state_ref,
    in_re_ref, in_im_ref, out_re_ref, out_im_ref, attn_out_ref, state_out_ref,
    norm_gain_ref, out_gain_ref, decay_ref, rotation_ref, skip_ref,
    row_cos_ref, row_sin_ref, block_cos_ref, block_sin_ref, step_ref, sink_ref,
    out_ref,
    key_value, packed, weights, held, normed, in_re, in_im, out_re, out_im, drive, read, powers,
    queries, pairs, before, inputs, states, carries, ends, priors,
    mixers, matrices, total, partial, arrived, summed, pieces,
    load_sem, far_send, far_recv, line_send, line_recv, part_send, part_recv,
    side_send, side_recv, halo_send, halo_recv, end_send, end_recv,
    mixer_send, mixer_recv, matrix_send, matrix_recv, half_send, half_recv,
    piece_send, piece_recv,
):
    layers = held.shape[0]
    rows = pairs.shape[1]
    layer, spot, core = place()
    query_width, pair_width = (queries.shape[-1], pairs.shape[-1])
    state_width = inputs.shape[-1]
    groups = in_re.shape[0]
    mine = pl.ds(layer * groups, groups)
    loads = [
        pltpu.make_async_copy(key_ref, key_value.at[0], load_sem.at[0]),
        pltpu.make_async_copy(value_ref, key_value.at[1], load_sem.at[1]),
    ]
    spans = (
        (query_ref, query_width, 0, 0),
        (state_ref, state_width, query_width + pair_width, 2),
    )
    own_weights = [
        pltpu.make_async_copy(
            source.at[:, :, pl.ds(pl.multiple_of(layer * wide, wide), wide)],
            weights.at[layer, spot, :, :, pl.ds(to, wide)], load_sem.at[2 + at],
        )
        for source, wide, to, at in spans
    ]
    own_tokens = pltpu.make_async_copy(tokens_ref, held.at[layer], load_sem.at[3])
    table_loads = [
        pltpu.make_async_copy(source.at[mine], target, load_sem.at[5 + at])
        for at, (source, target) in enumerate(
            ((in_re_ref, in_re), (in_im_ref, in_im), (out_re_ref, out_re), (out_im_ref, out_im))
        )
    ]
    matrix_loads = [
        pltpu.make_async_copy(source, matrices.at[kind, spot], load_sem.at[9 + kind])
        for kind, source in enumerate((attn_out_ref, state_out_ref))
    ]
    for copy in loads + own_weights + [own_tokens] + table_loads + matrix_loads:
        copy.start()
    for copy in loads:
        copy.wait()
    for at in range(layers):
        head = slice(at * HEAD, (at + 1) * HEAD)
        packed[at] = jnp.concatenate([key_value[0, :, :, head], key_value[1, :, :, head]], axis=-1)
    middle = pl.ds(query_width, pair_width)
    weights[layer, spot, :, :, query_width : query_width + pair_width] = packed[layer]
    greet(layers, layer, spot, core)

    def far_copies(way, hop):
        other = layer + hop if way == 0 else layer - hop
        device = {"sp": other * PLANE + spot}
        sources = [
            (source.at[:, :, pl.ds(pl.multiple_of(other * wide, wide), wide)], pl.ds(to, wide))
            for source, wide, to, _ in spans
        ] + [(packed.at[other], middle)]
        return [
            remote(
                source, weights.at[layer, spot, :, :, columns],
                far_send.at[way, hop, at], far_recv.at[way, hop, at], device,
            )
            for at, (source, columns) in enumerate(sources)
        ]

    def each_far(action):
        for hop in range(1, layers):
            for way, there in ((0, layer + hop <= layers - 1), (1, layer - hop >= 0)):

                @pl.when(there)
                def _():
                    for copy in far_copies(way, hop):
                        action(copy)

    each_far(lambda copy: copy.start())
    half_held = held.at[:, core]
    line_first(layers, layer, spot, tokens_ref.at[core], half_held, line_send, line_recv)
    for copy in own_weights:
        copy.wait()

    below, above = (layer, layers - 1 - layer)
    least = jnp.minimum(below, above)

    def arrival(at):
        paired = at <= 2 * least
        hop = jnp.where(paired, lax.div(at + 1, 2), at - least)
        way = jnp.where(paired, lax.rem(at, 2), jnp.where(below > above, 0, 1))
        return (jnp.where(way == 0, layer - hop, layer + hop), hop, way)

    plane_first(
        weights.at[layer, spot], weights.at[layer], layer, spot, side_send.at[0], side_recv.at[0]
    )
    for copy in table_loads:
        copy.wait()
    make_tables(
        layer, rows, decay_ref, rotation_ref, step_ref, in_re, in_im, out_re, out_im,
        drive, read, powers,
    )
    before[0] = jnp.zeros(before.shape[1:], before.dtype)
    plane_pass(weights.at[layer], layer, spot, side_send.at[0], side_recv.at[0])

    def to_partner(way, hop, block):
        remote(
            block, block, part_send.at[way, hop - 1], part_recv.at[way, hop - 1], {"tp": 1 - core}
        ).start()

    for at in range(1, layers):
        origin, hop, way = arrival(jnp.int32(at))
        for part, (to, wide) in enumerate(
            ((0, query_width), (query_width + pair_width, state_width), (query_width, pair_width))
        ):
            block = weights.at[origin, spot, :, :, pl.ds(to, wide)]
            remote(
                block, block, far_send.at[0, 0, 0], far_recv.at[way, hop, part], {"sp": 0}
            ).wait_recv()
        plane_first(
            weights.at[origin, spot], weights.at[origin], layer, spot,
            side_send.at[at], side_recv.at[at],
        )
        plane_pass(weights.at[origin], layer, spot, side_send.at[at], side_recv.at[at])
    line_pass(layers, layer, spot, 1, half_held, line_send, line_recv, to_partner)
    own_tokens.wait()
    for copy in matrix_loads:
        copy.wait()
    for at in range(layers):
        origin = layer if at == 0 else arrival(jnp.int32(at))[0]
        plane_landed(weights.at[origin], spot, side_send.at[at], side_recv.at[at])
    each_far(lambda copy: copy.wait_send())

    behind = layer * PLANE + lax.rem(spot + 1, PLANE)
    late = lax.div(spot, PLANE - 1)

    def hand_on(block):
        return remote(
            pairs.at[block], before.at[block + late], halo_send.at[block],
            halo_recv.at[block + late], {"sp": behind},
        )

    def arrive(block):
        remote(
            pairs.at[0], before.at[block], halo_send.at[0], halo_recv.at[block], {"sp": behind}
        ).wait_recv()

    def tell(block, at):
        other = lax.rem(spot + 1 + at, PLANE)
        return remote(
            ends.at[spot, block], ends.at[spot, block], end_send.at[at, block],
            end_recv.at[at, block], {"sp": layer * PLANE + other},
        )

    @pl.loop(0, layers)
    def _(at):
        block, hop, way = arrival(at)

        @pl.when(at > 0)
        def _():
            half = half_held.at[block]

            @pl.when(hop > 1)
            def _():
                remote(
                    half, half, line_send.at[way, 0], line_recv.at[way, hop - 1], {"sp": 0}
                ).wait_recv()
                onward = jnp.where(way == 0, layer < layers - 1, layer > 0)

                @pl.when(onward & (hop < layers - 1))
                def _():
                    remote(
                        half, half, line_send.at[way, hop], line_recv.at[way, hop],
                        {"sp": (layer + 1 - 2 * way) * PLANE + spot},
                    ).start()

                remote(
                    half, half, part_send.at[way, hop - 1], part_recv.at[way, hop - 1],
                    {"tp": 1 - core},
                ).start()

            other_half = held.at[block, 1 - core]
            remote(
                other_half, other_half, part_send.at[way, hop - 1], part_recv.at[way, hop - 1],
                {"tp": 1 - core},
            ).wait_recv()

        normalise(block, held, norm_gain_ref, normed)
        project_block(
            block, spot, normed, weights,
            (row_cos_ref, row_sin_ref, block_cos_ref, block_sin_ref), queries, pairs, inputs,
        )
        hand_on(block).start()
        scan_block(block, spot, inputs, drive, powers, states, carries, ends)
        for peer in range(PLANE - 1):
            tell(block, peer).start()

        kind, half = (lax.div(at, 2), lax.rem(at, 2))

        @pl.when(kind < 2)
        def _():
            for copy in plane_halves(
                matrices.at[kind, spot], matrices.at[kind], layer, spot, matrix_send.at[kind],
                matrix_recv.at[kind], half,
            ):
                copy.start()

        @pl.when((spot > 0) | (block == 0) | ((at > 0) & (way == 1)))
        def _():
            @pl.when((spot > 0) | (block > 0))
            def _():
                arrive(block)

            attend_block(
                block, layer, spot, queries, pairs, before, sink_ref, mixers.at[layer, 0, block]
            )

        @pl.when((spot == 0) & (at > 0) & (way == 0))
        def _():
            arrive(block + 1)
            attend_block(
                block + 1, layer, spot, queries, pairs, before, sink_ref,
                mixers.at[layer, 0, block + 1],
            )

    @pl.when(spot == 0)
    def _():
        arrive(layers)

    def mixers_first(kind):
        line_first(
            layers, layer, spot, mixers.at[layer, kind], mixers.at[:, kind],
            mixer_send.at[kind], mixer_recv.at[kind],
        )

    mixers_first(0)
    plane_pass(matrices.at[0], layer, spot, matrix_send.at[0], matrix_recv.at[0])
    for block in range(layers):
        for peer in range(PLANE - 1):
            tell(block, peer).wait()
    find_priors(ends, powers, priors)

    @pl.loop(0, layers)
    def _(block):
        read_block(
            block, layer, spot, inputs, states, carries, priors, powers, read, skip_ref,
            mixers.at[layer, 1, block],
        )

    mixers_first(1)
    plane_pass(matrices.at[1], layer, spot, matrix_send.at[1], matrix_recv.at[1])
    for kind in (0, 1):
        line_pass(
            layers, layer, spot, 1, mixers.at[:, kind], mixer_send.at[kind], mixer_recv.at[kind]
        )
    for kind in (0, 1):
        plane_landed(matrices.at[kind], spot, matrix_send.at[kind], matrix_recv.at[kind])

    depth = mixers.shape[-1]
    tokens = layers * rows
    half_depth, width = matrices.shape[3:]
    half_rows = rows // CORES
    per = half_depth // depth

    def take(at):
        block, hop, way = arrival(at)

        @pl.when(hop > 1)
        def _():
            for kind in (0, 1):
                columns = mixers.at[block, kind]
                remote(
                    columns, columns, mixer_send.at[kind, 0, 0],
                    mixer_recv.at[kind, way, hop - 1], {"sp": 0},
                ).wait_recv()
                onward = jnp.where(way == 0, layer < layers - 1, layer > 0)

                @pl.when(onward & (hop < layers - 1))
                def _():
                    remote(
                        columns, columns, mixer_send.at[kind, way, hop],
                        mixer_recv.at[kind, way, hop],
                        {"sp": (layer + 1 - 2 * way) * PLANE + spot},
                    ).start()

        return block

    def product(block, column):
        low = pl.ds(pl.multiple_of(lax.rem(block, per) * depth, depth), depth)
        return sum(
            jnp.dot(
                mixers[block, kind].reshape(tokens, depth),
                matrices[kind, column, lax.div(block, per), low, :],
                preferred_element_type=jnp.float32,
            )
            for kind in (0, 1)
        )

    @pl.loop(0, layers - 1)
    def _(at):
        block = take(at)
        for column in range(PLANE):
            value = product(block, column)

            @pl.when(at == 0)
            def _():
                total[column] = value

            @pl.when(at > 0)
            def _():
                total[column] += value

    last = take(jnp.int32(layers - 1))

    def swap(column):
        return remote(
            partial.at[column, 1 - core], arrived.at[column], half_send.at[column],
            half_recv.at[column], {"tp": 1 - core},
        )

    def each_piece(column, action):
        for hop in range(layers - 1, 0, -1):
            for way, there in ((0, layer + hop <= layers - 1), (1, layer - hop >= 0)):

                @pl.when(there)
                def _():
                    other = layer + hop if way == 0 else layer - hop
                    action(
                        remote(
                            summed.at[column, other], pieces.at[column, layer],
                            piece_send.at[column, way, hop], piece_recv.at[column, way, hop],
                            {"sp": other * PLANE + spot},
                        )
                    )

    def each_landing(column):
        for hop in range(1, layers):
            for way, there in ((0, layer - hop >= 0), (1, layer + hop <= layers - 1)):

                @pl.when(there)
                def _():
                    other = layer - hop if way == 0 else layer + hop
                    piece = pieces.at[column, other]
                    remote(
                        piece, piece, piece_send.at[0, 0, 0], piece_recv.at[column, way, hop],
                        {"sp": 0},
                    ).wait_recv()

    def send_column(column):
        swap(column).wait_recv()
        for at in range(layers):
            summed[column, at] = (
                partial[column, core, at].astype(jnp.float32)
                + arrived[column, at].astype(jnp.float32)
            ).astype(jnp.bfloat16)
        each_piece(column, lambda copy: copy.start())
        pieces[column, layer] = summed[column, layer]

    for column in range(PLANE):
        value = total[column] + product(last, column)
        value = value.astype(jnp.bfloat16).reshape(layers, CORES, half_rows, width)
        for half in range(CORES):
            partial[column, half] = value[:, half]
        swap(column).start()
        if column > 0:
            send_column(column - 1)
    send_column(PLANE - 1)
    for kind in (0, 1):
        line_drain(
            layers, layer, mixers.at[layer, kind], mixers.at[:, kind], mixer_send.at[kind],
            mixer_recv.at[kind],
        )
    line_drain(layers, layer, tokens_ref.at[core], half_held, line_send, line_recv)
    for hop in range(1, layers):
        for way, there in ((0, layer - hop >= 0), (1, layer + hop <= layers - 1)):

            @pl.when(there)
            def _():
                block = held.at[layer, 0]
                remote(
                    block, block, part_send.at[way, hop - 1], part_recv.at[way, hop - 1],
                    {"tp": 1 - core},
                ).wait_send()

    for block in range(layers):
        hand_on(block).wait_send()
    for column in range(PLANE):
        each_landing(column)
    for column in range(PLANE):
        swap(column).wait_send()
        each_piece(column, lambda copy: copy.wait_send())
    squares = jnp.zeros((half_rows, 1), jnp.float32)
    for column in range(PLANE):
        for at in range(layers):
            value = pieces[column, at].astype(jnp.float32)
            squares = squares + jnp.sum(value * value, axis=-1, keepdims=True)
    scale = lax.rsqrt(squares / (layers * PLANE * width) + epsilon)
    for at in range(layers):
        for column in range(PLANE):
            low = (at * PLANE + column) * width
            columns = slice(low, low + width)
            out_ref[:, columns] = (
                pieces[column, at].astype(jnp.float32) * scale * out_gain_ref[:, columns]
            ).astype(jnp.bfloat16)


def body(
    tokens,
    norm_gain,
    w_query,
    w_key,
    w_value,
    w_state_in,
    sink_logit,
    decay_rate,
    rotation,
    log_step,
    in_re,
    in_im,
    out_re,
    out_im,
    skip_gain,
    w_attn_out,
    w_state_out,
    out_gain,
):
    rows, model = tokens.shape
    layers = lax.axis_size("sp") // PLANE
    half_rows = rows // CORES
    depth = w_query.shape[0]
    query_width = w_query.shape[1] // layers
    pair_width = 2 * (w_key.shape[1] // layers)
    state_width = w_state_in.shape[1] // layers
    width = query_width + pair_width + state_width
    groups, states, group_width = (in_re.shape[0] // layers, in_re.shape[1], in_re.shape[2])
    kinds = state_width // LANES
    lanes = groups // kinds * states
    height, out_width = w_attn_out.shape
    half = HEAD // 2
    frequency = rotary_base ** (-(np.arange(half) * 2.0 / HEAD))
    frequency = np.tile(frequency, LANES // half)[None, :]
    within = np.arange(rows)[:, None] * frequency
    across = (np.arange(layers * PLANE) * rows)[:, None] * frequency
    tables = [np.cos(within), np.sin(within), np.cos(across), np.sin(across)]
    tables = [jnp.asarray(t, jnp.float32) for t in tables]
    anywhere = pl.BlockSpec(memory_space=pl.ANY)
    vmem = pl.BlockSpec(memory_space=pltpu.VMEM)
    smem = pl.BlockSpec(memory_space=pltpu.SMEM)
    dma = pltpu.SemaphoreType.DMA
    low, full = (jnp.bfloat16, jnp.float32)
    piece = pltpu.VMEM((PLANE, layers, half_rows, out_width), low)

    def halved(matrix):
        return matrix.reshape(2, matrix.shape[0] // 2, matrix.shape[1])

    return pl.pallas_call(
        whole_kernel,
        out_shape=jax.ShapeDtypeStruct((half_rows, model), low),
        in_specs=[anywhere] * 11 + [vmem] * 9 + [smem] * 2,
        out_specs=vmem,
        scratch_shapes=[
            pltpu.VMEM((2, 2, depth // 2, w_key.shape[1]), low),
            pltpu.VMEM((layers, 2, depth // 2, pair_width), low),
            pltpu.VMEM((layers, PLANE, 2, depth // 2, width), low),
            pltpu.VMEM((layers, CORES, half_rows, model), low),
            pltpu.VMEM((rows, model), low),
            pltpu.VMEM((groups, group_width, states), full),
            pltpu.VMEM((groups, group_width, states), full),
            pltpu.VMEM((groups, group_width, states), full),
            pltpu.VMEM((groups, group_width, states), full),
            pltpu.VMEM((kinds, 2 * LANES, 2 * lanes), low),
            pltpu.VMEM((kinds, 2 * LANES, 2 * lanes), low),
            pltpu.VMEM((4, SUB, groups * states), full),
            pltpu.VMEM((layers, rows, query_width), low),
            pltpu.VMEM((layers, rows, pair_width), low),
            pltpu.VMEM((layers + 1, rows, pair_width), low),
            pltpu.VMEM((layers, rows, state_width), low),
            pltpu.VMEM((layers, kinds, rows, 2 * lanes), full),
            pltpu.VMEM((layers, kinds, SUB, 2 * lanes), full),
            pltpu.VMEM((PLANE, layers, kinds, 1, 2 * lanes), full),
            pltpu.VMEM((layers * PLANE, kinds, 1, 2 * lanes), full),
            pltpu.VMEM((layers, 2, layers, rows, query_width), low),
            pltpu.VMEM((2, PLANE, 2, height // 2, out_width), low),
            pltpu.VMEM((PLANE, layers * rows, out_width), full),
            pltpu.VMEM((PLANE, CORES, layers, half_rows, out_width), low),
            piece, piece, piece,
            dma((11,)), dma((2, layers, 3)), dma((2, layers, 3)),
            dma((2, layers)), dma((2, layers)), dma((2, layers)), dma((2, layers)),
            dma((layers, 2, 3)), dma((layers, 2, 3)), dma((layers,)), dma((layers + 1,)),
            dma((PLANE - 1, layers)), dma((PLANE - 1, layers)),
            dma((2, 2, layers)), dma((2, 2, layers)), dma((2, 2, 3)), dma((2, 2, 3)),
            dma((PLANE,)), dma((PLANE,)), dma((PLANE, 2, layers)), dma((PLANE, 2, layers)),
        ],
        compiler_params=pltpu.CompilerParams(
            collective_id=0, has_side_effects=True, vmem_limit_bytes=60 * 2**20
        ),
    )(
        tokens.reshape(CORES, half_rows, model), halved(w_query), halved(w_key), halved(w_value),
        halved(w_state_in), jnp.swapaxes(in_re, 1, 2), jnp.swapaxes(in_im, 1, 2), out_re, out_im, halved(w_attn_out),
        halved(w_state_out), norm_gain.reshape(1, -1), out_gain.reshape(1, -1), decay_rate,
        rotation, skip_gain.reshape(1, -1), *tables, log_step, sink_logit,
    )


def suits(mesh, shapes):
    size, cores = (mesh.shape["sp"], mesh.shape["tp"])
    layers = size // PLANE
    query_width, key_width, state_width = (shapes[at][1] // cores for at in (2, 3, 5))
    return (
        size % PLANE == 0
        and layers % 4 == 0
        and cores == CORES
        and shapes[0][0] // size == WINDOW
        and key_width == layers * HEAD
        and state_width == query_width
        and query_width % (layers * LANES) == 0
    )


def solution(mesh):
    def run(*arrays):
        chosen = body if suits(mesh, [array.shape for array in arrays]) else whole_weights_body
        return sharded(mesh, chosen)(*arrays)

    return run


def sharded(mesh, chosen):
    return jax.shard_map(
        chosen,
        mesh=mesh,
        in_specs=(
            P("sp", None),
            P(),
            P("sp", "tp"),
            P("sp", "tp"),
            P("sp", "tp"),
            P("sp", "tp"),
            P("tp"),
            P("tp", None),
            P("tp", None),
            P("tp"),
            P("tp", None, None),
            P("tp", None, None),
            P("tp", None, None),
            P("tp", None, None),
            P("tp"),
            P("tp", "sp"),
            P("tp", "sp"),
            P(),
        ),
        out_specs=P(("sp", "tp"), None),
        check_vma=False,
    )
```

```python
import math

import jax
import jax.numpy as jnp
import numpy as np
from jax import lax
from jax.experimental import pallas as pl
from jax.experimental.pallas import tpu as pltpu
from jax.sharding import PartitionSpec as P

HEAD = 64
WINDOW = 128
SUB = 8


epsilon = 1e-06
rotary_base = 500000.0


def passed_along(value, axis, by):
    size = lax.axis_size(axis)
    pairs = [(i, i + by) for i in range(size) if 0 <= i + by < size]
    return lax.ppermute(value, axis, pairs)


def rotate(heads_block, positions):
    head_width = heads_block.shape[-1]
    half_width = head_width // 2
    frequency = rotary_base ** (-(jnp.arange(half_width, dtype=jnp.float32) * 2.0 / head_width))
    angles = positions.astype(jnp.float32)[:, None] * frequency[None, :]
    cosine = jnp.cos(angles)[:, None, :]
    sine_part = jnp.sin(angles)[:, None, :]
    lower_half = heads_block[..., :half_width]
    upper_half = heads_block[..., half_width:]
    return jnp.concatenate(
        [
            lower_half * cosine - upper_half * sine_part,
            upper_half * cosine + lower_half * sine_part,
        ],
        axis=-1,
    )


def shape_heads(query_sum, key_sum, value_sum, positions, head_width):
    row_count = query_sum.shape[0]
    kv_heads = key_sum.shape[1] // head_width
    group_size = query_sum.shape[1] // key_sum.shape[1]
    queries = rotate(
        query_sum.reshape(row_count, kv_heads * group_size, head_width), positions
    ).astype(jnp.bfloat16)
    queries = queries.reshape(row_count, kv_heads, group_size, head_width)
    key_rows = rotate(key_sum.reshape(row_count, kv_heads, head_width), positions).astype(
        jnp.bfloat16
    )
    key_rows = key_rows.reshape(row_count, kv_heads * head_width)
    value_rows = value_sum.astype(jnp.bfloat16)
    return (queries, key_rows, value_rows)


def band_attention(queries, key_rows, value_rows, sink_logit, first_row, window):
    row_count, kv_heads, group_size, head_width = queries.shape
    blocks = row_count // window
    query_blocks = queries.reshape(blocks, window, kv_heads, group_size, head_width)
    key_blocks = jnp.concatenate(
        [
            key_rows[:row_count].reshape(blocks, window, kv_heads, head_width),
            key_rows[window:].reshape(blocks, window, kv_heads, head_width),
        ],
        axis=1,
    )
    value_blocks = jnp.concatenate(
        [
            value_rows[:row_count].reshape(blocks, window, kv_heads, head_width),
            value_rows[window:].reshape(blocks, window, kv_heads, head_width),
        ],
        axis=1,
    )
    scores = jnp.einsum(
        "bqkgd,bskd->bkgqs", query_blocks, key_blocks, preferred_element_type=jnp.float32
    ) / math.sqrt(head_width)
    block_start = jnp.arange(blocks, dtype=jnp.int32)[:, None, None] * window
    query_at = first_row + block_start + jnp.arange(window, dtype=jnp.int32)[None, :, None]
    key_at = (
        first_row - window + block_start + jnp.arange(2 * window, dtype=jnp.int32)[None, None, :]
    )
    offset_gap = query_at - key_at
    visible = (offset_gap >= 0) & (offset_gap < window) & (key_at >= 0)
    scores = jnp.where(visible[:, None, None, :, :], scores, -jnp.inf)
    sink_value = sink_logit.reshape(1, kv_heads, group_size, 1, 1)
    top_score = jnp.maximum(jnp.max(scores, axis=-1, keepdims=True), sink_value)
    exponent = jnp.exp(scores - top_score)
    totals = jnp.sum(exponent, axis=-1, keepdims=True) + jnp.exp(sink_value - top_score)
    weights = (exponent / totals).astype(jnp.bfloat16)
    attended = jnp.einsum(
        "bkgqs,bskd->bqkgd", weights, value_blocks, preferred_element_type=jnp.float32
    )
    return attended.reshape(row_count, kv_heads * group_size * head_width).astype(jnp.bfloat16)


def discretize(decay_rate, rotation, log_step, in_re, in_im):
    time_step = jnp.exp(log_step)[:, None]
    lambda_re = -decay_rate
    modulus = jnp.exp(lambda_re * time_step)
    pole_re = modulus * jnp.cos(rotation * time_step)
    pole_im = modulus * jnp.sin(rotation * time_step)
    minus_one = pole_re - 1.0
    denominator = lambda_re * lambda_re + rotation * rotation
    factor_re = ((minus_one * lambda_re + pole_im * rotation) / denominator)[..., None]
    factor_im = ((pole_im * lambda_re - minus_one * rotation) / denominator)[..., None]
    drive_re = factor_re * in_re - factor_im * in_im
    drive_im = factor_re * in_im + factor_im * in_re
    return (pole_re, pole_im, drive_re, drive_im)


def complex_power(decay_rate, rotation, log_step, exponent):
    time_step = jnp.exp(log_step)[:, None]
    modulus = jnp.exp(-decay_rate * time_step * exponent)
    angle = rotation * time_step * exponent
    return (modulus * jnp.cos(angle), modulus * jnp.sin(angle))


def token_shuffle(rows, inverse):
    steps = rows // SUB
    out_row = lax.broadcasted_iota(jnp.int32, (rows, rows), 1 if inverse else 0)
    in_row = lax.broadcasted_iota(jnp.int32, (rows, rows), 0 if inverse else 1)
    token = (out_row % SUB) * steps + out_row // SUB
    return (token == in_row).astype(jnp.bfloat16)


def scan_kernel(
    u_ref, drive_ref, pole_re_ref, pole_im_ref, jump_re_ref, jump_im_ref,
    state_ref, carry_re_ref, carry_im_ref, end_re_ref, end_im_ref,
):
    rows = u_ref.shape[0]
    width = pole_re_ref.shape[-1]
    shuffle = token_shuffle(rows, False)
    shuffled = jnp.dot(shuffle, u_ref[...], preferred_element_type=jnp.float32)
    state_ref[...] = jnp.dot(
        shuffled, drive_ref[0], precision=lax.Precision.HIGHEST,
        preferred_element_type=jnp.float32,
    )
    pole_re = jnp.broadcast_to(pole_re_ref[0], (SUB, width))
    pole_im = jnp.broadcast_to(pole_im_ref[0], (SUB, width))
    now_re = jnp.zeros((SUB, width), jnp.float32)
    now_im = jnp.zeros((SUB, width), jnp.float32)
    for step in range(rows // SUB):
        at = slice(step * SUB, (step + 1) * SUB)
        new_re = pole_re * now_re - pole_im * now_im + state_ref[at, :width]
        new_im = pole_re * now_im + pole_im * now_re + state_ref[at, width:]
        state_ref[at, :width] = new_re
        state_ref[at, width:] = new_im
        now_re, now_im = new_re, new_im
    jump_re, jump_im = (jump_re_ref[0], jump_im_ref[0])
    held_re = jnp.zeros((1, width), jnp.float32)
    held_im = jnp.zeros((1, width), jnp.float32)
    for chunk in range(SUB):
        carry_re_ref[chunk : chunk + 1, :] = held_re
        carry_im_ref[chunk : chunk + 1, :] = held_im
        next_re = jump_re * held_re - jump_im * held_im + now_re[chunk : chunk + 1]
        next_im = jump_re * held_im + jump_im * held_re + now_im[chunk : chunk + 1]
        held_re, held_im = next_re, next_im
    end_re_ref[0] = held_re
    end_im_ref[0] = held_im


def readout_kernel(
    u_ref, state_ref, carry_re_ref, carry_im_ref, prior_re_ref, prior_im_ref,
    chunk_re_ref, chunk_im_ref, pole_re_ref, pole_im_ref, read_ref, skip_ref, out_ref, full_ref,
):
    rows = u_ref.shape[0]
    width = pole_re_ref.shape[-1]
    prior_re, prior_im = (prior_re_ref[0], prior_im_ref[0])
    chunk_re, chunk_im = (chunk_re_ref[...], chunk_im_ref[...])
    add_re = carry_re_ref[...] + chunk_re * prior_re - chunk_im * prior_im
    add_im = carry_im_ref[...] + chunk_re * prior_im + chunk_im * prior_re
    pole_re = jnp.broadcast_to(pole_re_ref[0], (SUB, width))
    pole_im = jnp.broadcast_to(pole_im_ref[0], (SUB, width))
    for step in range(rows // SUB):
        at = slice(step * SUB, (step + 1) * SUB)
        turned_re = pole_re * add_re - pole_im * add_im
        turned_im = pole_re * add_im + pole_im * add_re
        full_ref[at, :width] = state_ref[at, :width] + turned_re
        full_ref[at, width:] = state_ref[at, width:] + turned_im
        add_re, add_im = turned_re, turned_im
    summed = jnp.dot(
        full_ref[...], read_ref[0], precision=lax.Precision.HIGHEST,
        preferred_element_type=jnp.float32,
    )
    shuffled = jnp.dot(
        token_shuffle(rows, False), u_ref[...], preferred_element_type=jnp.float32
    )
    mixed = jax.nn.gelu(summed + skip_ref[...] * shuffled).astype(jnp.bfloat16)
    out_ref[...] = jnp.dot(
        token_shuffle(rows, True), mixed, preferred_element_type=jnp.float32
    ).astype(jnp.bfloat16)


def block_diagonal(parts):
    blocks, per, rows, columns = parts[0].shape
    same = jnp.eye(per, dtype=bool)[None, :, None, :, None]
    spread = [
        jnp.where(same, part[:, :, :, None, :], 0.0).reshape(blocks, per * rows, per * columns)
        for part in parts
    ]
    return jnp.concatenate(spread, axis=2)


def state_tables(rows, decay_rate, rotation, log_step, in_re, in_im, out_re, out_im):
    groups, states = decay_rate.shape
    group_width = in_re.shape[-1]
    per = min(groups, max(1, 128 // group_width))
    blocks, width = (groups // per, per * states)
    pole_re, pole_im, drive_re, drive_im = discretize(decay_rate, rotation, log_step, in_re, in_im)
    steps = rows // SUB

    def by_block(value):
        return value.reshape(blocks, per, *value.shape[1:])

    def flat(value):
        return value.reshape(blocks, 1, width)

    drive = block_diagonal(
        [by_block(jnp.swapaxes(drive_re, 1, 2)), by_block(jnp.swapaxes(drive_im, 1, 2))]
    )
    read = jnp.swapaxes(block_diagonal([by_block(out_re), by_block(-out_im)]), 1, 2)
    jump = complex_power(decay_rate, rotation, log_step, float(steps))
    chunk_powers = [
        complex_power(decay_rate, rotation, log_step, float(steps * c)) for c in range(SUB)
    ]
    chunk_re = jnp.stack([p[0].reshape(groups * states) for p in chunk_powers])
    chunk_im = jnp.stack([p[1].reshape(groups * states) for p in chunk_powers])
    return dict(
        drive=drive, read=read, pole_re=flat(pole_re), pole_im=flat(pole_im),
        jump_re=flat(jump[0]), jump_im=flat(jump[1]), chunk_re=chunk_re, chunk_im=chunk_im,
        blocks=blocks, width=width, channels=per * group_width,
    )


def local_scan(inputs, tables):
    rows = inputs.shape[0]
    blocks, width, channels = (tables["blocks"], tables["width"], tables["channels"])
    row_spec = pl.BlockSpec((1, 1, width), lambda b: (b, 0, 0))
    carry_spec = pl.BlockSpec((SUB, width), lambda b: (0, b))
    return pl.pallas_call(
        scan_kernel,
        grid=(blocks,),
        in_specs=[
            pl.BlockSpec((rows, channels), lambda b: (0, b)),
            pl.BlockSpec((1, channels, 2 * width), lambda b: (b, 0, 0)),
            row_spec, row_spec, row_spec, row_spec,
        ],
        out_specs=[
            pl.BlockSpec((rows, 2 * width), lambda b: (0, b)),
            carry_spec, carry_spec, row_spec, row_spec,
        ],
        out_shape=[
            jax.ShapeDtypeStruct((rows, 2 * width * blocks), jnp.float32),
            jax.ShapeDtypeStruct((SUB, width * blocks), jnp.float32),
            jax.ShapeDtypeStruct((SUB, width * blocks), jnp.float32),
            jax.ShapeDtypeStruct((blocks, 1, width), jnp.float32),
            jax.ShapeDtypeStruct((blocks, 1, width), jnp.float32),
        ],
        cost_estimate=pl.CostEstimate(
            flops=12 * rows * channels * width * blocks, bytes_accessed=10**7, transcendentals=0
        ),
    )(
        inputs, tables["drive"], tables["pole_re"], tables["pole_im"],
        tables["jump_re"], tables["jump_im"],
    )


def read_states(inputs, scanned, prior_re, prior_im, tables, skip_gain):
    rows = inputs.shape[0]
    state, carry_re, carry_im = scanned[:3]
    blocks, width, channels = (tables["blocks"], tables["width"], tables["channels"])
    row_spec = pl.BlockSpec((1, 1, width), lambda b: (b, 0, 0))
    carry_spec = pl.BlockSpec((SUB, width), lambda b: (0, b))
    return pl.pallas_call(
        readout_kernel,
        grid=(blocks,),
        in_specs=[
            pl.BlockSpec((rows, channels), lambda b: (0, b)),
            pl.BlockSpec((rows, 2 * width), lambda b: (0, b)),
            carry_spec, carry_spec, row_spec, row_spec, carry_spec, carry_spec,
            row_spec, row_spec,
            pl.BlockSpec((1, 2 * width, channels), lambda b: (b, 0, 0)),
            pl.BlockSpec((1, channels), lambda b: (0, b)),
        ],
        out_specs=pl.BlockSpec((rows, channels), lambda b: (0, b)),
        out_shape=jax.ShapeDtypeStruct((rows, channels * blocks), jnp.bfloat16),
        scratch_shapes=[pltpu.VMEM((rows, 2 * width), jnp.float32)],
        cost_estimate=pl.CostEstimate(
            flops=12 * rows * channels * width * blocks, bytes_accessed=10**7, transcendentals=0
        ),
    )(
        inputs, state, carry_re, carry_im, prior_re, prior_im,
        tables["chunk_re"], tables["chunk_im"], tables["pole_re"], tables["pole_im"],
        tables["read"], skip_gain.reshape(1, -1),
    )


def carried_state(end_re, end_im, decay_rate, rotation, log_step, rows):
    ends = jnp.stack([end_re, end_im])
    shape = end_re.shape
    size = lax.axis_size("sp")
    reach = 1
    while reach < size:
        power_re, power_im = complex_power(decay_rate, rotation, log_step, float(rows * reach))
        power_re, power_im = (power_re.reshape(shape), power_im.reshape(shape))
        prior = passed_along(ends, "sp", reach)
        ends = ends + jnp.stack(
            [
                power_re * prior[0] - power_im * prior[1],
                power_re * prior[1] + power_im * prior[0],
            ]
        )
        reach *= 2
    before = passed_along(ends, "sp", 1)
    return (before[0], before[1])


def state_branch(inputs, decay_rate, rotation, log_step, in_re, in_im, out_re, out_im, skip_gain):
    rows = inputs.shape[0]
    tables = state_tables(rows, decay_rate, rotation, log_step, in_re, in_im, out_re, out_im)
    scanned = local_scan(inputs, tables)
    prior_re, prior_im = carried_state(
        scanned[3], scanned[4], decay_rate, rotation, log_step, rows
    )
    return read_states(inputs, scanned, prior_re, prior_im, tables, skip_gain)


def earlier_window(key_rows, value_rows):
    joined = jnp.concatenate([key_rows, value_rows], axis=1)
    prior = passed_along(joined, "sp", 1)
    return jnp.concatenate([prior, joined], axis=0)


def make_adder(normed_cols):

    def add_pieces(carried, weight_pieces, row_start):
        updated = []
        for running_total, weight_piece in zip(carried, weight_pieces):
            product = lax.dot_general(
                normed_cols,
                weight_piece,
                (((0,), (0,)), ((), ())),
                preferred_element_type=jnp.float32,
            )
            updated.append(product)
        return tuple(updated)

    return add_pieces


def whole_weights_body(
    tokens,
    norm_gain,
    w_query,
    w_key,
    w_value,
    w_state_in,
    sink_logit,
    decay_rate,
    rotation,
    log_step,
    in_re,
    in_im,
    out_re,
    out_im,
    skip_gain,
    w_attn_out,
    w_state_out,
    out_gain,
):
    row_count = tokens.shape[0]
    window = WINDOW
    head_width = HEAD
    wide_tokens = tokens.astype(jnp.float32)
    normed = (
        wide_tokens
        * lax.rsqrt(jnp.mean(wide_tokens * wide_tokens, axis=-1, keepdims=True) + epsilon)
        * norm_gain
    ).astype(jnp.bfloat16)
    first_row = lax.axis_index("sp") * row_count
    positions = first_row + jnp.arange(row_count, dtype=jnp.int32)
    add_pieces = make_adder(jnp.transpose(normed))

    def empty_like(weight_shard):
        return jnp.zeros((row_count, weight_shard.shape[1]), jnp.float32)

    query_sum, key_sum, value_sum, input_sum = add_pieces(
        (empty_like(w_query), empty_like(w_key), empty_like(w_value), empty_like(w_state_in)),
        (
            lax.all_gather(w_query, "sp", axis=0, tiled=True),
            lax.all_gather(w_key, "sp", axis=0, tiled=True),
            lax.all_gather(w_value, "sp", axis=0, tiled=True),
            lax.all_gather(w_state_in, "sp", axis=0, tiled=True),
        ),
        jnp.int32(0),
    )
    queries, key_rows, value_rows = shape_heads(
        query_sum, key_sum, value_sum, positions, head_width
    )
    joined_rows = earlier_window(key_rows, value_rows)
    inputs = input_sum.astype(jnp.bfloat16)
    mixed_state = state_branch(
        inputs, decay_rate, rotation, log_step, in_re, in_im, out_re, out_im, skip_gain
    )
    kv_width = key_rows.shape[1]
    kv_heads = kv_width // head_width
    all_keys = joined_rows[:, :kv_width].reshape(window + row_count, kv_heads, head_width)
    all_values = joined_rows[:, kv_width:].reshape(window + row_count, kv_heads, head_width)
    attended = band_attention(queries, all_keys, all_values, sink_logit, first_row, window)
    attn_rows, state_rows = (
        lax.all_gather(w_attn_out, "sp", axis=1, tiled=True),
        lax.all_gather(w_state_out, "sp", axis=1, tiled=True),
    )
    projected = lax.psum_scatter(
        (
            jnp.dot(attended, attn_rows, preferred_element_type=jnp.float32)
            + jnp.dot(mixed_state, state_rows, preferred_element_type=jnp.float32)
        ).astype(jnp.bfloat16),
        "tp",
        scatter_dimension=0,
        tiled=True,
    ).astype(jnp.float32)
    row_scale = lax.rsqrt(jnp.mean(projected * projected, axis=-1, keepdims=True) + epsilon)
    return (projected * row_scale * out_gain).astype(jnp.bfloat16)


SIDE = 2
PLANE = SIDE * SIDE
CORES = 2
CHUNKS = 2
LANES = 128
MESH = pl.DeviceIdType.MESH


def place():
    me = lax.axis_index("sp")
    return (lax.div(me, PLANE), lax.rem(me, PLANE), lax.axis_index("tp"))


def plane_neighbours(spot):
    beside = spot + 1 - 2 * lax.rem(spot, SIDE)
    above = spot + SIDE - 2 * SIDE * lax.div(spot, SIDE)
    return (beside, above)


def greet(layers, layer, spot, core):
    barrier = pltpu.get_barrier_semaphore()
    beside, above = plane_neighbours(spot)
    for ahead in range(1, layers):
        other = lax.rem(layer + ahead, layers)
        pl.semaphore_signal(
            barrier, inc=1, device_id={"sp": other * PLANE + spot}, device_id_type=MESH
        )
    for other in (beside, above, PLANE - 1 - spot):
        pl.semaphore_signal(
            barrier, inc=1, device_id={"sp": layer * PLANE + other}, device_id_type=MESH
        )
    pl.semaphore_signal(barrier, inc=1, device_id={"tp": 1 - core}, device_id_type=MESH)
    pl.semaphore_wait(barrier, layers + 3)


def remote(source, target, send_sem, recv_sem, device):
    return pltpu.make_async_remote_copy(
        src_ref=source, dst_ref=target, send_sem=send_sem, recv_sem=recv_sem,
        device_id=device, device_id_type=MESH,
    )


def line_first(layers, layer, spot, source, held, send_sems, recv_sems):
    @pl.when(layer < layers - 1)
    def _():
        remote(
            source, held.at[layer], send_sems.at[0, 0], recv_sems.at[0, 0],
            {"sp": (layer + 1) * PLANE + spot},
        ).start()

    @pl.when(layer > 0)
    def _():
        remote(
            source, held.at[layer], send_sems.at[1, 0], recv_sems.at[1, 0],
            {"sp": (layer - 1) * PLANE + spot},
        ).start()


def line_pass(layers, layer, spot, hop, held, send_sems, recv_sems, landed=None):
    @pl.when(layer - hop >= 0)
    def _():
        block = held.at[layer - hop]
        remote(block, block, send_sems.at[0, 0], recv_sems.at[0, hop - 1], {"sp": 0}).wait_recv()

        @pl.when(layer < layers - 1)
        def _():
            if hop < layers - 1:
                remote(
                    block, block, send_sems.at[0, hop], recv_sems.at[0, hop],
                    {"sp": (layer + 1) * PLANE + spot},
                ).start()

        if landed is not None:
            landed(0, hop, block)

    @pl.when(layer + hop <= layers - 1)
    def _():
        block = held.at[layer + hop]
        remote(block, block, send_sems.at[1, 0], recv_sems.at[1, hop - 1], {"sp": 0}).wait_recv()

        @pl.when(layer > 0)
        def _():
            if hop < layers - 1:
                remote(
                    block, block, send_sems.at[1, hop], recv_sems.at[1, hop],
                    {"sp": (layer - 1) * PLANE + spot},
                ).start()

        if landed is not None:
            landed(1, hop, block)


def line_drain(layers, layer, source, held, send_sems, recv_sems):
    for hop in range(layers - 1):

        @pl.when((layer - hop >= 0) & (layer < layers - 1))
        def _():
            remote(
                source, held.at[layer], send_sems.at[0, hop], recv_sems.at[0, 0], {"sp": 0}
            ).wait_send()

        @pl.when((layer + hop <= layers - 1) & (layer > 0))
        def _():
            remote(
                source, held.at[layer], send_sems.at[1, hop], recv_sems.at[1, 0], {"sp": 0}
            ).wait_send()


def plane_halves(halves, slots, layer, spot, send_sems, recv_sems, half):
    beside, above = plane_neighbours(spot)
    return [
        remote(
            halves.at[half], slots.at[spot, half], send_sems.at[0, half],
            recv_sems.at[0, half], {"sp": layer * PLANE + beside},
        ),
        remote(
            halves.at[1 - half], slots.at[spot, 1 - half], send_sems.at[1, 1 - half],
            recv_sems.at[1, 1 - half], {"sp": layer * PLANE + above},
        ),
    ]


def plane_first(halves, slots, layer, spot, send_sems, recv_sems):
    for half in (0, 1):
        for copy in plane_halves(halves, slots, layer, spot, send_sems, recv_sems, half):
            copy.start()


def plane_pass(slots, layer, spot, send_sems, recv_sems):
    beside, above = plane_neighbours(spot)
    block = slots.at[beside, 0]
    remote(block, block, send_sems.at[0, 0], recv_sems.at[0, 0], {"sp": 0}).wait_recv()
    remote(
        block, block, send_sems.at[1, 2], recv_sems.at[1, 2], {"sp": layer * PLANE + above}
    ).start()
    block = slots.at[above, 1]
    remote(block, block, send_sems.at[0, 0], recv_sems.at[1, 1], {"sp": 0}).wait_recv()
    remote(
        block, block, send_sems.at[0, 2], recv_sems.at[0, 2], {"sp": layer * PLANE + beside}
    ).start()


def plane_landed(slots, spot, send_sems, recv_sems):
    for way, half in ((0, 1), (1, 0), (0, 2), (1, 2)):
        block = slots.at[spot, 0]
        remote(block, block, send_sems.at[0, 0], recv_sems.at[way, half], {"sp": 0}).wait_recv()
    for way in (0, 1):
        for half in (0, 1, 2):
            block = slots.at[spot, 0]
            remote(block, block, send_sems.at[way, half], recv_sems.at[0, 0], {"sp": 0}).wait_send()


def lanes_of(rows):
    return jnp.concatenate([rows[at : at + 1] for at in range(rows.shape[0])], axis=1)


def split_pair(value):
    high = value.astype(jnp.bfloat16)
    return (high, (value - high.astype(jnp.float32)).astype(jnp.bfloat16))


def make_tables(
    layer, rows, decay_ref, rotation_ref, step_ref, in_re_ref, in_im_ref, out_re_ref, out_im_ref,
    drive, read, powers,
):
    groups, group_width, states = in_re_ref.shape
    kinds, _, width2 = drive.shape
    per = groups // kinds
    width = per * states
    channels = per * group_width
    base = layer * groups
    decay = lanes_of(decay_ref[pl.ds(base, groups), :])
    rotation = lanes_of(rotation_ref[pl.ds(base, groups), :])
    step = jnp.exp(
        jnp.concatenate(
            [jnp.full((1, states), step_ref[base + at], jnp.float32) for at in range(groups)],
            axis=1,
        )
    )
    row = lax.broadcasted_iota(jnp.int32, (SUB, groups * states), 0)
    steps = rows // SUB
    shares = (row * steps, jnp.where(row == 0, 1, jnp.where(row == 1, steps, rows)))
    for at, share in enumerate(shares):
        share = share.astype(jnp.float32)
        modulus = jnp.exp(-decay * step * share)
        angle = rotation * step * share
        powers[2 * at] = modulus * jnp.cos(angle)
        powers[2 * at + 1] = modulus * jnp.sin(angle)
    pole_re, pole_im = (powers[2, 0:1, :], powers[3, 0:1, :])
    minus_one = pole_re - 1.0
    denominator = decay * decay + rotation * rotation
    factor_re = (pole_im * rotation - minus_one * decay) / denominator
    factor_im = (-pole_im * decay - minus_one * rotation) / denominator
    same = (
        lax.broadcasted_iota(jnp.int32, (channels, width), 0) // group_width
        == lax.broadcasted_iota(jnp.int32, (channels, width), 1) // states
    )

    def spread(pieces):
        beside = jnp.concatenate(pieces, axis=1)
        return jnp.concatenate([beside] * per, axis=0)

    for kind in range(kinds):
        lanes = slice(kind * width, (kind + 1) * width)
        f_re, f_im = (factor_re[:, lanes], factor_im[:, lanes])
        own = range(kind * per, (kind + 1) * per)
        m_re = spread([in_re_ref[at] for at in own])
        m_im = spread([in_im_ref[at] for at in own])
        for part, value in ((0, f_re * m_re - f_im * m_im), (1, f_re * m_im + f_im * m_re)):
            high, low = split_pair(jnp.where(same, value, 0.0))
            columns = slice(part * width, (part + 1) * width)
            drive[kind, :channels, columns] = high
            drive[kind, channels:, columns] = low
        r_re = spread([out_re_ref[at] for at in own])
        r_im = spread([-out_im_ref[at] for at in own])
        for part, value in ((0, r_re), (1, r_im)):
            high, low = split_pair(jnp.where(same, value, 0.0))
            columns = slice(part * width, (part + 1) * width)
            read[kind, :channels, columns] = high
            read[kind, channels:, columns] = low


def normalise(block, held, gain_ref, normed):
    _, parts, chunks, part_rows, model = held.shape
    tall = 16
    per = part_rows // tall

    @pl.loop(0, parts * chunks * per)
    def _(at):
        value = held[
            block, at // (chunks * per), (at // per) % chunks,
            pl.ds(pl.multiple_of((at % per) * tall, tall), tall), :,
        ].astype(jnp.float32)
        scale = lax.rsqrt(jnp.sum(value * value, axis=-1, keepdims=True) / model + epsilon)
        normed[block, pl.ds(pl.multiple_of(at * tall, tall), tall), :] = (
            value * scale * gain_ref[...]
        ).astype(jnp.bfloat16)


def project_block(block, spot, normed, weights, tables, queries, pairs, inputs):
    rows = normed.shape[1]
    layers = weights.shape[0]
    depth = weights.shape[2] * weights.shape[3]
    query_width, pair_width = (queries.shape[-1], pairs.shape[-1])
    half_width = HEAD // 2
    row_cos_ref, row_sin_ref, block_cos_ref, block_sin_ref = tables
    lane = lax.broadcasted_iota(jnp.int32, (rows, LANES), 1)
    low = lax.rem(lane, HEAD) < half_width

    def turn(value, cosine, sine):
        swapped = jnp.where(
            low, -pltpu.roll(value, LANES - half_width, 1), pltpu.roll(value, half_width, 1)
        )
        return value * cosine + swapped * sine

    total = None
    for at in range(layers * PLANE):
        piece = jnp.dot(
            normed[block, :, at * depth : (at + 1) * depth],
            weights[at // PLANE, at % PLANE].reshape(depth, weights.shape[-1]),
            preferred_element_type=jnp.float32,
        )
        total = piece if total is None else total + piece
    here = pl.ds(block * PLANE + spot, 1)
    block_cos, block_sin = (block_cos_ref[here, :], block_sin_ref[here, :])
    cosine = row_cos_ref[...] * block_cos - row_sin_ref[...] * block_sin
    sine = row_sin_ref[...] * block_cos + row_cos_ref[...] * block_sin
    turned = [turn(total[:, at : at + LANES], cosine, sine) for at in range(0, query_width, LANES)]
    queries[block] = jnp.concatenate(turned, axis=1).astype(jnp.bfloat16)
    value = total[:, query_width : query_width + pair_width]
    pairs[block] = jnp.where(lane < HEAD, turn(value, cosine, sine), value).astype(jnp.bfloat16)
    inputs[block] = jnp.dot(
        token_shuffle(rows, False), total[:, query_width + pair_width :].astype(jnp.bfloat16),
        preferred_element_type=jnp.float32,
    ).astype(jnp.bfloat16)


def scan_block(block, spot, inputs, drive, powers, states, carries, ends):
    kinds, _, width2 = drive.shape
    width = width2 // 2
    channels = inputs.shape[-1] // kinds
    rows = inputs.shape[1]
    for kind in range(kinds):
        lanes = slice(kind * width, (kind + 1) * width)
        own = inputs[block, :, kind * channels : (kind + 1) * channels]
        states[block, kind] = jnp.dot(
            jnp.concatenate([own, own], axis=1), drive[kind], preferred_element_type=jnp.float32
        )
        pole_re = jnp.broadcast_to(powers[2, 0:1, lanes], (SUB, width))
        pole_im = jnp.broadcast_to(powers[3, 0:1, lanes], (SUB, width))
        now_re = jnp.zeros((SUB, width), jnp.float32)
        now_im = jnp.zeros((SUB, width), jnp.float32)
        for step in range(rows // SUB):
            at = slice(step * SUB, (step + 1) * SUB)
            new_re = pole_re * now_re - pole_im * now_im + states[block, kind, at, :width]
            new_im = pole_re * now_im + pole_im * now_re + states[block, kind, at, width:]
            states[block, kind, at, :width] = new_re
            states[block, kind, at, width:] = new_im
            now_re, now_im = new_re, new_im
        jump_re, jump_im = (powers[2, 1:2, lanes], powers[3, 1:2, lanes])
        held_re = jnp.zeros((1, width), jnp.float32)
        held_im = jnp.zeros((1, width), jnp.float32)
        re, im = ([], [])
        for chunk in range(SUB):
            re.append(held_re)
            im.append(held_im)
            next_re = jump_re * held_re - jump_im * held_im + now_re[chunk : chunk + 1]
            next_im = jump_re * held_im + jump_im * held_re + now_im[chunk : chunk + 1]
            held_re, held_im = next_re, next_im
        carries[block, kind, :, :width] = jnp.concatenate(re, axis=0)
        carries[block, kind, :, width:] = jnp.concatenate(im, axis=0)
        ends[spot, block, kind, :, :width] = held_re
        ends[spot, block, kind, :, width:] = held_im


def attend_block(block, layer, spot, queries, pairs, before, sink_ref, out):
    rows, query_width = queries.shape[1:]
    group = query_width // HEAD
    pair, prior = (pairs[block], before[block])
    keys = jnp.concatenate([prior[:, :HEAD], pair[:, :HEAD]], axis=0)
    values = jnp.concatenate([prior[:, HEAD:], pair[:, HEAD:]], axis=0)
    query_at = lax.broadcasted_iota(jnp.int32, (rows, rows + WINDOW), 0)
    key_at = lax.broadcasted_iota(jnp.int32, (rows, rows + WINDOW), 1) - WINDOW
    gap = query_at - key_at
    first = (block * PLANE + spot) * rows
    visible = (gap >= 0) & (gap < WINDOW) & (key_at + first >= 0)
    pieces = []
    for head in range(group):
        query = queries[block, :, head * HEAD : (head + 1) * HEAD]
        scores = lax.dot_general(
            query, keys, (((1,), (1,)), ((), ())), preferred_element_type=jnp.float32
        ) / math.sqrt(HEAD)
        scores = jnp.where(visible, scores, -jnp.inf)
        sink = jnp.full((1, 1), sink_ref[layer * group + head], jnp.float32)
        top = jnp.maximum(jnp.max(scores, axis=-1, keepdims=True), sink)
        exponent = jnp.exp(scores - top)
        total = jnp.sum(exponent, axis=-1, keepdims=True) + jnp.exp(sink - top)
        weights = (exponent / total).astype(jnp.bfloat16)
        pieces.append(jnp.dot(weights, values, preferred_element_type=jnp.float32))
    out[...] = jnp.concatenate(pieces, axis=1).astype(jnp.bfloat16)


def find_priors(ends, powers, priors):
    plane, layers, kinds = ends.shape[:3]
    width = ends.shape[-1] // 2
    for kind in range(kinds):
        lanes = slice(kind * width, (kind + 1) * width)
        power_re, power_im = (powers[2, 2:3, lanes], powers[3, 2:3, lanes])
        held_re = jnp.zeros((1, width), jnp.float32)
        held_im = jnp.zeros((1, width), jnp.float32)
        for at in range(layers * plane):
            priors[at, kind, :, :width] = held_re
            priors[at, kind, :, width:] = held_im
            end_re = ends[at % plane, at // plane, kind, :, :width]
            end_im = ends[at % plane, at // plane, kind, :, width:]
            held_re, held_im = (
                power_re * held_re - power_im * held_im + end_re,
                power_re * held_im + power_im * held_re + end_im,
            )


def read_block(block, layer, spot, inputs, states, carries, priors, powers, read, skip_ref, out):
    kinds, channels2, width2 = read.shape
    width, channels = (width2 // 2, channels2 // 2)
    rows = inputs.shape[1]
    contract = (((1,), (1,)), ((), ()))
    pieces = []
    for kind in range(kinds):
        lanes = slice(kind * width, (kind + 1) * width)
        prior_re = priors[block * PLANE + spot, kind, :, :width]
        prior_im = priors[block * PLANE + spot, kind, :, width:]
        chunk_re, chunk_im = (powers[0, :, lanes], powers[1, :, lanes])
        add_re = carries[block, kind, :, :width] + chunk_re * prior_re - chunk_im * prior_im
        add_im = carries[block, kind, :, width:] + chunk_re * prior_im + chunk_im * prior_re
        pole_re = jnp.broadcast_to(powers[2, 0:1, lanes], (SUB, width))
        pole_im = jnp.broadcast_to(powers[3, 0:1, lanes], (SUB, width))
        for step in range(rows // SUB):
            at = slice(step * SUB, (step + 1) * SUB)
            turned_re = pole_re * add_re - pole_im * add_im
            turned_im = pole_re * add_im + pole_im * add_re
            states[block, kind, at, :width] += turned_re
            states[block, kind, at, width:] += turned_im
            add_re, add_im = turned_re, turned_im
        high, low = split_pair(states[block, kind])
        both = lax.dot_general(high, read[kind], contract, preferred_element_type=jnp.float32)
        rest = lax.dot_general(
            low, read[kind, :channels], contract, preferred_element_type=jnp.float32
        )
        summed = both[:, :channels] + both[:, channels:] + rest
        at = pl.multiple_of(layer * (kinds * channels) + kind * channels, channels)
        skip = skip_ref[:, pl.ds(at, channels)]
        own = inputs[block, :, kind * channels : (kind + 1) * channels].astype(jnp.float32)
        pieces.append(jax.nn.gelu(summed + skip * own).astype(jnp.bfloat16))
    out[...] = jnp.dot(
        token_shuffle(rows, True), jnp.concatenate(pieces, axis=1),
        preferred_element_type=jnp.float32,
    ).astype(jnp.bfloat16)


def whole_kernel(
    tokens_ref, query_ref, key_ref, value_ref, state_ref,
    in_re_ref, in_im_ref, out_re_ref, out_im_ref, attn_out_ref, state_out_ref,
    norm_gain_ref, out_gain_ref, decay_ref, rotation_ref, skip_ref,
    row_cos_ref, row_sin_ref, block_cos_ref, block_sin_ref, step_ref, sink_ref,
    out_ref,
    key_value, packed, weights, held, normed, in_re, in_im, out_re, out_im, drive, read, powers,
    queries, pairs, before, inputs, states, carries, ends, priors,
    mixers, matrices, total, partial, arrived, summed, pieces,
    load_sem, pack_sem, far_send, far_recv, line_send, line_recv, part_send, part_recv,
    side_send, side_recv, halo_send, halo_recv, end_send, end_recv,
    mixer_send, mixer_recv, matrix_send, matrix_recv, half_send, half_recv,
    piece_send, piece_recv,
):
    layers = held.shape[0]
    rows = pairs.shape[1]
    layer, spot, core = place()
    query_width, pair_width = (queries.shape[-1], pairs.shape[-1])
    state_width = inputs.shape[-1]
    groups = in_re.shape[0]
    mine = pl.ds(layer * groups, groups)
    loads = [
        pltpu.make_async_copy(key_ref, key_value.at[0], load_sem.at[0]),
        pltpu.make_async_copy(value_ref, key_value.at[1], load_sem.at[1]),
    ]
    spans = (
        (query_ref, query_width, 0),
        (state_ref, state_width, query_width + pair_width),
    )
    def loaded(block, target, at):
        return [
            pltpu.make_async_copy(
                source.at[:, :, pl.ds(pl.multiple_of(block * wide, wide), wide)],
                target.at[:, :, pl.ds(to, wide)], pack_sem.at[at, part],
            )
            for part, (source, wide, to) in enumerate(spans)
        ]

    own_weights = loaded(layer, weights.at[layer, spot], layers)
    far_loads = [copy for at in range(layers) for copy in loaded(at, packed.at[at], at)]
    own_tokens = pltpu.make_async_copy(tokens_ref, held.at[layer], load_sem.at[3])
    table_loads = [
        pltpu.make_async_copy(source.at[mine], target, load_sem.at[5 + at])
        for at, (source, target) in enumerate(
            ((in_re_ref, in_re), (in_im_ref, in_im), (out_re_ref, out_re), (out_im_ref, out_im))
        )
    ]
    matrix_loads = [
        pltpu.make_async_copy(source, matrices.at[kind, spot], load_sem.at[9 + kind])
        for kind, source in enumerate((attn_out_ref, state_out_ref))
    ]
    for copy in loads + own_weights + far_loads + [own_tokens] + table_loads + matrix_loads:
        copy.start()
    for copy in loads:
        copy.wait()
    middle = slice(query_width, query_width + pair_width)
    for at in range(layers):
        head = slice(at * HEAD, (at + 1) * HEAD)
        packed[at, :, :, middle] = jnp.concatenate(
            [key_value[0, :, :, head], key_value[1, :, :, head]], axis=-1
        )
    weights[layer, spot, :, :, middle] = packed[layer, :, :, middle]
    for copy in far_loads:
        copy.wait()
    greet(layers, layer, spot, core)

    below, above = (layer, layers - 1 - layer)
    least = jnp.minimum(below, above)
    short = jnp.where(below < above, 0, 1)

    def arrival(at):
        paired = at <= 2 * least
        hop = jnp.where(paired, lax.div(at + 1, 2), at - least)
        way = jnp.where(paired & (lax.rem(at, 2) == 1), short, 1 - short)
        return (jnp.where(way == 0, layer - hop, layer + hop), hop, way)

    def far_copy(way, hop):
        other = layer + hop if way == 0 else layer - hop
        return remote(
            packed.at[other], weights.at[layer, spot], far_send.at[way, hop],
            far_recv.at[way, hop], {"sp": other * PLANE + spot},
        )

    def each_far(hop, action):
        for way, there in ((0, layer + hop <= layers - 1), (1, layer - hop >= 0)):

            @pl.when(there)
            def _():
                action(far_copy(way, hop))

    def start(copy):
        copy.start()

    each_far(1, start)

    @pl.when(least > 0)
    def _():
        for hop in range(2, layers):
            each_far(hop, start)

    chunks = held.shape[2]

    def chunk_lines(action):
        for chunk in range(chunks):
            action(chunk, held.at[:, core, chunk], line_send.at[chunk], line_recv.at[chunk])

    for copy in own_weights:
        copy.wait()

    def part(way, hop, chunk, half):
        block = held.at[layer + hop - 2 * hop * (1 - way), half, chunk]
        return remote(
            block, block, part_send.at[chunk, way, hop - 1], part_recv.at[chunk, way, hop - 1],
            {"tp": 1 - core},
        )

    def send_tokens(side):
        onward = 1 - side
        for chunk in range(chunks):
            remote(
                tokens_ref.at[core, chunk], held.at[layer, core, chunk],
                line_send.at[chunk, onward, 0], line_recv.at[chunk, onward, 0],
                {"sp": (layer + 1 - 2 * onward) * PLANE + spot},
            ).start()

    def pass_tokens(way, hop):
        block = layer + hop - 2 * hop * (1 - way)

        def step(chunk, slots, send, recv):
            half = slots.at[block]
            remote(half, half, send.at[way, 0], recv.at[way, hop - 1], {"sp": 0}).wait_recv()
            onward = jnp.where(way == 0, layer < layers - 1, layer > 0)

            @pl.when(onward & (hop < layers - 1))
            def _():
                remote(
                    half, half, send.at[way, hop], recv.at[way, hop],
                    {"sp": (layer + 1 - 2 * way) * PLANE + spot},
                ).start()

            part(way, hop, chunk, core).start()

        chunk_lines(step)

    plane_first(
        weights.at[layer, spot], weights.at[layer], layer, spot, side_send.at[0], side_recv.at[0]
    )

    @pl.when(least == 0)
    def _():
        send_tokens(1 - short)

    for copy in table_loads:
        copy.wait()
    make_tables(
        layer, rows, decay_ref, rotation_ref, step_ref, in_re, in_im, out_re, out_im,
        drive, read, powers,
    )
    before[0] = jnp.zeros(before.shape[1:], before.dtype)
    own_tokens.wait()
    normalise(layer, held, norm_gain_ref, normed)
    plane_pass(weights.at[layer], layer, spot, side_send.at[0], side_recv.at[0])

    for at in range(1, layers):
        origin, hop, way = arrival(jnp.int32(at))
        block = weights.at[origin, spot]
        remote(block, block, far_send.at[0, 0], far_recv.at[way, hop], {"sp": 0}).wait_recv()

        if at == 1:

            @pl.when(least > 0)
            def _():
                send_tokens(short)

        if at == layers - 1:

            @pl.when(least > 0)
            def _():
                send_tokens(1 - short)

        plane_first(
            weights.at[origin, spot], weights.at[origin], layer, spot,
            side_send.at[at], side_recv.at[at],
        )
        plane_pass(weights.at[origin], layer, spot, side_send.at[at], side_recv.at[at])
        if at == 1:

            @pl.when(least == 0)
            def _():
                for hop in range(2, layers):
                    each_far(hop, start)

    for copy in matrix_loads:
        copy.wait()
    plane_first(
        matrices.at[0, spot], matrices.at[0], layer, spot, matrix_send.at[0], matrix_recv.at[0]
    )

    @pl.when(least > 0)
    def _():
        pass_tokens(short, 1)

    pass_tokens(1 - short, 1)

    def landed(at):
        block, hop, way = arrival(at)
        for chunk in range(chunks):
            part(way, hop, chunk, 1 - core).wait_recv()
        normalise(block, held, norm_gain_ref, normed)

    for at in range(1, layers):
        hop = arrival(jnp.int32(at))[1]

        @pl.when(hop == 1)
        def _():
            landed(jnp.int32(at))

    for at in range(layers):
        origin = layer if at == 0 else arrival(jnp.int32(at))[0]
        plane_landed(weights.at[origin], spot, side_send.at[at], side_recv.at[at])
    for hop in range(1, layers):
        each_far(hop, lambda copy: copy.wait_send())

    behind = layer * PLANE + lax.rem(spot + 1, PLANE)
    late = lax.div(spot, PLANE - 1)

    def hand_on(block):
        return remote(
            pairs.at[block], before.at[block + late], halo_send.at[block],
            halo_recv.at[block + late], {"sp": behind},
        )

    def arrive(block):
        remote(
            pairs.at[0], before.at[block], halo_send.at[0], halo_recv.at[block], {"sp": behind}
        ).wait_recv()

    def tell(block, at):
        other = lax.rem(spot + 1 + at, PLANE)
        return remote(
            ends.at[spot, block], ends.at[spot, block], end_send.at[at, block],
            end_recv.at[at, block], {"sp": layer * PLANE + other},
        )

    def pass_on(at):
        _, hop, way = arrival(at)

        @pl.when(hop > 1)
        def _():
            pass_tokens(way, hop)

    def attend(block):
        attend_block(
            block, layer, spot, queries, pairs, before, sink_ref, mixers.at[layer, 0, block]
        )

    @pl.loop(0, layers + 1)
    def _(at):
        @pl.when(at > 0)
        def _():
            block, hop, way = arrival(at - 1)

            @pl.when((spot > 0) | (block == 0) | ((at > 1) & (way == 1)))
            def _():
                @pl.when((spot > 0) | (block > 0))
                def _():
                    arrive(block)

                attend(block)

            @pl.when((spot == 0) & (at > 1) & (way == 0))
            def _():
                arrive(block + 1)
                attend(block + 1)

        @pl.when(at < layers)
        def _():
            block, hop, way = arrival(at)

            @pl.when((least == 0) & (at > 0))
            def _():
                pass_on(at)

            @pl.when(hop > 1)
            def _():
                landed(at)

            project_block(
                block, spot, normed, weights,
                (row_cos_ref, row_sin_ref, block_cos_ref, block_sin_ref), queries, pairs, inputs,
            )
            hand_on(block).start()
            scan_block(block, spot, inputs, drive, powers, states, carries, ends)
            for peer in range(PLANE - 1):
                tell(block, peer).start()

            @pl.when((least > 0) & (at < layers - 2))
            def _():
                pass_on(at + 2)

            @pl.when((least == 0) & (at == 2))
            def _():
                plane_pass(matrices.at[0], layer, spot, matrix_send.at[0], matrix_recv.at[0])

    @pl.when(spot == 0)
    def _():
        arrive(layers)

    def mixers_first(kind):
        line_first(
            layers, layer, spot, mixers.at[layer, kind], mixers.at[:, kind],
            mixer_send.at[kind], mixer_recv.at[kind],
        )

    mixers_first(0)

    @pl.when(least > 0)
    def _():
        plane_pass(matrices.at[0], layer, spot, matrix_send.at[0], matrix_recv.at[0])

    plane_first(
        matrices.at[1, spot], matrices.at[1], layer, spot, matrix_send.at[1], matrix_recv.at[1]
    )
    for block in range(layers):
        for peer in range(PLANE - 1):
            tell(block, peer).wait()
    find_priors(ends, powers, priors)

    @pl.loop(0, layers)
    def _(block):
        read_block(
            block, layer, spot, inputs, states, carries, priors, powers, read, skip_ref,
            mixers.at[layer, 1, block],
        )

    mixers_first(1)
    depth = mixers.shape[-1]
    tokens = layers * rows
    half_depth, width = matrices.shape[3:]
    half_rows = rows // CORES
    per = half_depth // depth

    def take(at):
        block, hop, way = arrival(at)

        for kind in (0, 1):
            columns = mixers.at[block, kind]
            remote(
                columns, columns, mixer_send.at[kind, 0, 0],
                mixer_recv.at[kind, way, hop - 1], {"sp": 0},
            ).wait_recv()
            onward = jnp.where(way == 0, layer < layers - 1, layer > 0)

            @pl.when(onward & (hop < layers - 1))
            def _():
                remote(
                    columns, columns, mixer_send.at[kind, way, hop],
                    mixer_recv.at[kind, way, hop],
                    {"sp": (layer + 1 - 2 * way) * PLANE + spot},
                ).start()

    def product(block, column):
        low = pl.ds(pl.multiple_of(lax.rem(block, per) * depth, depth), depth)
        return sum(
            jnp.dot(
                mixers[block, kind].reshape(tokens, depth),
                matrices[kind, column, lax.div(block, per), low, :],
                preferred_element_type=jnp.float32,
            )
            for kind in (0, 1)
        )

    for at in range(1, layers - 1):
        take(jnp.where(at <= 2 * least, at - 1 + 2 * (at % 2), at))
        if at == 1:
            plane_pass(matrices.at[1], layer, spot, matrix_send.at[1], matrix_recv.at[1])
    @pl.when(least > 0)
    def _():
        take(jnp.int32(layers - 1))

    for kind in (0, 1):
        plane_landed(matrices.at[kind], spot, matrix_send.at[kind], matrix_recv.at[kind])

    @pl.loop(0, PLANE)
    def _(column):
        total[column] = sum(
            product(arrival(jnp.int32(at))[0], column) for at in range(layers - 1)
        )

    @pl.when(least == 0)
    def _():
        take(jnp.int32(layers - 1))

    last = arrival(jnp.int32(layers - 1))[0]

    def swap(column):
        return remote(
            partial.at[column, 1 - core], arrived.at[column], half_send.at[column],
            half_recv.at[column], {"tp": 1 - core},
        )

    def each_piece(column, action):
        for hop in range(layers - 1, 0, -1):
            for way, there in ((0, layer + hop <= layers - 1), (1, layer - hop >= 0)):

                @pl.when(there)
                def _():
                    other = layer + hop if way == 0 else layer - hop
                    action(
                        remote(
                            summed.at[column, other], pieces.at[column, layer],
                            piece_send.at[column, way, hop], piece_recv.at[column, way, hop],
                            {"sp": other * PLANE + spot},
                        )
                    )

    def each_landing(column):
        for hop in range(1, layers):
            for way, there in ((0, layer - hop >= 0), (1, layer + hop <= layers - 1)):

                @pl.when(there)
                def _():
                    other = layer - hop if way == 0 else layer + hop
                    piece = pieces.at[column, other]
                    remote(
                        piece, piece, piece_send.at[0, 0, 0], piece_recv.at[column, way, hop],
                        {"sp": 0},
                    ).wait_recv()

    def send_column(column):
        swap(column).wait_recv()
        for at in range(layers):
            summed[column, at] = (
                partial[column, core, at].astype(jnp.float32)
                + arrived[column, at].astype(jnp.float32)
            ).astype(jnp.bfloat16)
        each_piece(column, lambda copy: copy.start())
        pieces[column, layer] = summed[column, layer]

    for column in range(PLANE):
        value = total[column] + product(last, column)
        value = value.astype(jnp.bfloat16).reshape(layers, CORES, half_rows, width)
        for half in range(CORES):
            partial[column, half] = value[:, half]
        swap(column).start()
        if column == 0:
            for kind in (0, 1):
                line_drain(
                    layers, layer, mixers.at[layer, kind], mixers.at[:, kind],
                    mixer_send.at[kind], mixer_recv.at[kind],
                )
        if column > 0:
            send_column(column - 1)
    send_column(PLANE - 1)
    chunk_lines(
        lambda chunk, slots, send, recv: line_drain(
            layers, layer, slots.at[layer], slots, send, recv
        )
    )
    for hop in range(1, layers):
        for way, there in ((0, layer - hop >= 0), (1, layer + hop <= layers - 1)):

            @pl.when(there)
            def _():
                for chunk in range(chunks):
                    part(way, hop, chunk, core).wait_send()

    for block in range(layers):
        hand_on(block).wait_send()
    squares = jnp.zeros((half_rows, width), jnp.float32)
    for column in range(PLANE):
        each_landing(column)
        for at in range(layers):
            value = pieces[column, at].astype(jnp.float32)
            squares = squares + value * value
    for column in range(PLANE):
        swap(column).wait_send()
        each_piece(column, lambda copy: copy.wait_send())
    mean = jnp.sum(squares, axis=-1, keepdims=True) / (layers * PLANE * width)
    scale = lax.rsqrt(mean + epsilon)
    for at in range(layers):
        for column in range(PLANE):
            low = (at * PLANE + column) * width
            columns = slice(low, low + width)
            out_ref[:, columns] = (
                pieces[column, at].astype(jnp.float32) * scale * out_gain_ref[:, columns]
            ).astype(jnp.bfloat16)


def body(
    tokens,
    norm_gain,
    w_query,
    w_key,
    w_value,
    w_state_in,
    sink_logit,
    decay_rate,
    rotation,
    log_step,
    in_re,
    in_im,
    out_re,
    out_im,
    skip_gain,
    w_attn_out,
    w_state_out,
    out_gain,
):
    rows, model = tokens.shape
    layers = lax.axis_size("sp") // PLANE
    half_rows = rows // CORES
    depth = w_query.shape[0]
    query_width = w_query.shape[1] // layers
    pair_width = 2 * (w_key.shape[1] // layers)
    state_width = w_state_in.shape[1] // layers
    width = query_width + pair_width + state_width
    groups, states, group_width = (in_re.shape[0] // layers, in_re.shape[1], in_re.shape[2])
    kinds = state_width // LANES
    lanes = groups // kinds * states
    height, out_width = w_attn_out.shape
    half = HEAD // 2
    frequency = rotary_base ** (-(np.arange(half) * 2.0 / HEAD))
    frequency = np.tile(frequency, LANES // half)[None, :]
    within = np.arange(rows)[:, None] * frequency
    across = (np.arange(layers * PLANE) * rows)[:, None] * frequency
    tables = [np.cos(within), np.sin(within), np.cos(across), np.sin(across)]
    tables = [jnp.asarray(t, jnp.float32) for t in tables]
    anywhere = pl.BlockSpec(memory_space=pl.ANY)
    vmem = pl.BlockSpec(memory_space=pltpu.VMEM)
    smem = pl.BlockSpec(memory_space=pltpu.SMEM)
    dma = pltpu.SemaphoreType.DMA
    low, full = (jnp.bfloat16, jnp.float32)
    piece = pltpu.VMEM((PLANE, layers, half_rows, out_width), low)

    def halved(matrix):
        return matrix.reshape(2, matrix.shape[0] // 2, matrix.shape[1])

    return pl.pallas_call(
        whole_kernel,
        out_shape=jax.ShapeDtypeStruct((half_rows, model), low),
        in_specs=[anywhere] * 11 + [vmem] * 9 + [smem] * 2,
        out_specs=vmem,
        scratch_shapes=[
            pltpu.VMEM((2, 2, depth // 2, w_key.shape[1]), low),
            pltpu.VMEM((layers, 2, depth // 2, width), low),
            pltpu.VMEM((layers, PLANE, 2, depth // 2, width), low),
            pltpu.VMEM((layers, CORES, CHUNKS, half_rows // CHUNKS, model), low),
            pltpu.VMEM((layers, rows, model), low),
            pltpu.VMEM((groups, group_width, states), full),
            pltpu.VMEM((groups, group_width, states), full),
            pltpu.VMEM((groups, group_width, states), full),
            pltpu.VMEM((groups, group_width, states), full),
            pltpu.VMEM((kinds, 2 * LANES, 2 * lanes), low),
            pltpu.VMEM((kinds, 2 * LANES, 2 * lanes), low),
            pltpu.VMEM((4, SUB, groups * states), full),
            pltpu.VMEM((layers, rows, query_width), low),
            pltpu.VMEM((layers, rows, pair_width), low),
            pltpu.VMEM((layers + 1, rows, pair_width), low),
            pltpu.VMEM((layers, rows, state_width), low),
            pltpu.VMEM((layers, kinds, rows, 2 * lanes), full),
            pltpu.VMEM((layers, kinds, SUB, 2 * lanes), full),
            pltpu.VMEM((PLANE, layers, kinds, 1, 2 * lanes), full),
            pltpu.VMEM((layers * PLANE, kinds, 1, 2 * lanes), full),
            pltpu.VMEM((layers, 2, layers, rows, query_width), low),
            pltpu.VMEM((2, PLANE, 2, height // 2, out_width), low),
            pltpu.VMEM((PLANE, layers * rows, out_width), full),
            pltpu.VMEM((PLANE, CORES, layers, half_rows, out_width), low),
            piece, piece, piece,
            dma((11,)), dma((layers + 1, 2)), dma((2, layers)), dma((2, layers)),
            dma((CHUNKS, 2, layers)), dma((CHUNKS, 2, layers)),
            dma((CHUNKS, 2, layers)), dma((CHUNKS, 2, layers)),
            dma((layers, 2, 3)), dma((layers, 2, 3)), dma((layers,)), dma((layers + 1,)),
            dma((PLANE - 1, layers)), dma((PLANE - 1, layers)),
            dma((2, 2, layers)), dma((2, 2, layers)), dma((2, 2, 3)), dma((2, 2, 3)),
            dma((PLANE,)), dma((PLANE,)), dma((PLANE, 2, layers)), dma((PLANE, 2, layers)),
        ],
        compiler_params=pltpu.CompilerParams(
            collective_id=0, has_side_effects=True, vmem_limit_bytes=60 * 2**20
        ),
    )(
        tokens.reshape(CORES, CHUNKS, half_rows // CHUNKS, model), halved(w_query), halved(w_key), halved(w_value),
        halved(w_state_in), jnp.swapaxes(in_re, 1, 2), jnp.swapaxes(in_im, 1, 2), out_re, out_im, halved(w_attn_out),
        halved(w_state_out), norm_gain.reshape(1, -1), out_gain.reshape(1, -1), decay_rate,
        rotation, skip_gain.reshape(1, -1), *tables, log_step, sink_logit,
    )


def suits(mesh, shapes):
    size, cores = (mesh.shape["sp"], mesh.shape["tp"])
    layers = size // PLANE
    query_width, key_width, state_width = (shapes[at][1] // cores for at in (2, 3, 5))
    return (
        size % PLANE == 0
        and layers % 4 == 0
        and cores == CORES
        and shapes[0][0] // size == WINDOW
        and key_width == layers * HEAD
        and state_width == query_width
        and query_width % (layers * LANES) == 0
    )


def solution(mesh):
    def run(*arrays):
        chosen = body if suits(mesh, [array.shape for array in arrays]) else whole_weights_body
        return sharded(mesh, chosen)(*arrays)

    return run


def sharded(mesh, chosen):
    return jax.shard_map(
        chosen,
        mesh=mesh,
        in_specs=(
            P("sp", None),
            P(),
            P("sp", "tp"),
            P("sp", "tp"),
            P("sp", "tp"),
            P("sp", "tp"),
            P("tp"),
            P("tp", None),
            P("tp", None),
            P("tp"),
            P("tp", None, None),
            P("tp", None, None),
            P("tp", None, None),
            P("tp", None, None),
            P("tp"),
            P("tp", "sp"),
            P("tp", "sp"),
            P(),
        ),
        out_specs=P(("sp", "tp"), None),
        check_vma=False,
    )
```

```python
import math

import jax
import jax.numpy as jnp
import numpy as np
from jax import lax
from jax.experimental import pallas as pl
from jax.experimental.pallas import tpu as pltpu
from jax.sharding import PartitionSpec as P

HEAD = 64
WINDOW = 128
SUB = 8


epsilon = 1e-06
rotary_base = 500000.0


def passed_along(value, axis, by):
    size = lax.axis_size(axis)
    pairs = [(i, i + by) for i in range(size) if 0 <= i + by < size]
    return lax.ppermute(value, axis, pairs)


def rotate(heads_block, positions):
    head_width = heads_block.shape[-1]
    half_width = head_width // 2
    frequency = rotary_base ** (-(jnp.arange(half_width, dtype=jnp.float32) * 2.0 / head_width))
    angles = positions.astype(jnp.float32)[:, None] * frequency[None, :]
    cosine = jnp.cos(angles)[:, None, :]
    sine_part = jnp.sin(angles)[:, None, :]
    lower_half = heads_block[..., :half_width]
    upper_half = heads_block[..., half_width:]
    return jnp.concatenate(
        [
            lower_half * cosine - upper_half * sine_part,
            upper_half * cosine + lower_half * sine_part,
        ],
        axis=-1,
    )


def shape_heads(query_sum, key_sum, value_sum, positions, head_width):
    row_count = query_sum.shape[0]
    kv_heads = key_sum.shape[1] // head_width
    group_size = query_sum.shape[1] // key_sum.shape[1]
    queries = rotate(
        query_sum.reshape(row_count, kv_heads * group_size, head_width), positions
    ).astype(jnp.bfloat16)
    queries = queries.reshape(row_count, kv_heads, group_size, head_width)
    key_rows = rotate(key_sum.reshape(row_count, kv_heads, head_width), positions).astype(
        jnp.bfloat16
    )
    key_rows = key_rows.reshape(row_count, kv_heads * head_width)
    value_rows = value_sum.astype(jnp.bfloat16)
    return (queries, key_rows, value_rows)


def band_attention(queries, key_rows, value_rows, sink_logit, first_row, window):
    row_count, kv_heads, group_size, head_width = queries.shape
    blocks = row_count // window
    query_blocks = queries.reshape(blocks, window, kv_heads, group_size, head_width)
    key_blocks = jnp.concatenate(
        [
            key_rows[:row_count].reshape(blocks, window, kv_heads, head_width),
            key_rows[window:].reshape(blocks, window, kv_heads, head_width),
        ],
        axis=1,
    )
    value_blocks = jnp.concatenate(
        [
            value_rows[:row_count].reshape(blocks, window, kv_heads, head_width),
            value_rows[window:].reshape(blocks, window, kv_heads, head_width),
        ],
        axis=1,
    )
    scores = jnp.einsum(
        "bqkgd,bskd->bkgqs", query_blocks, key_blocks, preferred_element_type=jnp.float32
    ) / math.sqrt(head_width)
    block_start = jnp.arange(blocks, dtype=jnp.int32)[:, None, None] * window
    query_at = first_row + block_start + jnp.arange(window, dtype=jnp.int32)[None, :, None]
    key_at = (
        first_row - window + block_start + jnp.arange(2 * window, dtype=jnp.int32)[None, None, :]
    )
    offset_gap = query_at - key_at
    visible = (offset_gap >= 0) & (offset_gap < window) & (key_at >= 0)
    scores = jnp.where(visible[:, None, None, :, :], scores, -jnp.inf)
    sink_value = sink_logit.reshape(1, kv_heads, group_size, 1, 1)
    top_score = jnp.maximum(jnp.max(scores, axis=-1, keepdims=True), sink_value)
    exponent = jnp.exp(scores - top_score)
    totals = jnp.sum(exponent, axis=-1, keepdims=True) + jnp.exp(sink_value - top_score)
    weights = (exponent / totals).astype(jnp.bfloat16)
    attended = jnp.einsum(
        "bkgqs,bskd->bqkgd", weights, value_blocks, preferred_element_type=jnp.float32
    )
    return attended.reshape(row_count, kv_heads * group_size * head_width).astype(jnp.bfloat16)


def discretize(decay_rate, rotation, log_step, in_re, in_im):
    time_step = jnp.exp(log_step)[:, None]
    lambda_re = -decay_rate
    modulus = jnp.exp(lambda_re * time_step)
    pole_re = modulus * jnp.cos(rotation * time_step)
    pole_im = modulus * jnp.sin(rotation * time_step)
    minus_one = pole_re - 1.0
    denominator = lambda_re * lambda_re + rotation * rotation
    factor_re = ((minus_one * lambda_re + pole_im * rotation) / denominator)[..., None]
    factor_im = ((pole_im * lambda_re - minus_one * rotation) / denominator)[..., None]
    drive_re = factor_re * in_re - factor_im * in_im
    drive_im = factor_re * in_im + factor_im * in_re
    return (pole_re, pole_im, drive_re, drive_im)


def complex_power(decay_rate, rotation, log_step, exponent):
    time_step = jnp.exp(log_step)[:, None]
    modulus = jnp.exp(-decay_rate * time_step * exponent)
    angle = rotation * time_step * exponent
    return (modulus * jnp.cos(angle), modulus * jnp.sin(angle))


def token_shuffle(rows, inverse):
    steps = rows // SUB
    out_row = lax.broadcasted_iota(jnp.int32, (rows, rows), 1 if inverse else 0)
    in_row = lax.broadcasted_iota(jnp.int32, (rows, rows), 0 if inverse else 1)
    token = (out_row % SUB) * steps + out_row // SUB
    return (token == in_row).astype(jnp.bfloat16)


def scan_kernel(
    u_ref, drive_ref, pole_re_ref, pole_im_ref, jump_re_ref, jump_im_ref,
    state_ref, carry_re_ref, carry_im_ref, end_re_ref, end_im_ref,
):
    rows = u_ref.shape[0]
    width = pole_re_ref.shape[-1]
    shuffle = token_shuffle(rows, False)
    shuffled = jnp.dot(shuffle, u_ref[...], preferred_element_type=jnp.float32)
    state_ref[...] = jnp.dot(
        shuffled, drive_ref[0], precision=lax.Precision.HIGHEST,
        preferred_element_type=jnp.float32,
    )
    pole_re = jnp.broadcast_to(pole_re_ref[0], (SUB, width))
    pole_im = jnp.broadcast_to(pole_im_ref[0], (SUB, width))
    now_re = jnp.zeros((SUB, width), jnp.float32)
    now_im = jnp.zeros((SUB, width), jnp.float32)
    for step in range(rows // SUB):
        at = slice(step * SUB, (step + 1) * SUB)
        new_re = pole_re * now_re - pole_im * now_im + state_ref[at, :width]
        new_im = pole_re * now_im + pole_im * now_re + state_ref[at, width:]
        state_ref[at, :width] = new_re
        state_ref[at, width:] = new_im
        now_re, now_im = new_re, new_im
    jump_re, jump_im = (jump_re_ref[0], jump_im_ref[0])
    held_re = jnp.zeros((1, width), jnp.float32)
    held_im = jnp.zeros((1, width), jnp.float32)
    for chunk in range(SUB):
        carry_re_ref[chunk : chunk + 1, :] = held_re
        carry_im_ref[chunk : chunk + 1, :] = held_im
        next_re = jump_re * held_re - jump_im * held_im + now_re[chunk : chunk + 1]
        next_im = jump_re * held_im + jump_im * held_re + now_im[chunk : chunk + 1]
        held_re, held_im = next_re, next_im
    end_re_ref[0] = held_re
    end_im_ref[0] = held_im


def readout_kernel(
    u_ref, state_ref, carry_re_ref, carry_im_ref, prior_re_ref, prior_im_ref,
    chunk_re_ref, chunk_im_ref, pole_re_ref, pole_im_ref, read_ref, skip_ref, out_ref, full_ref,
):
    rows = u_ref.shape[0]
    width = pole_re_ref.shape[-1]
    prior_re, prior_im = (prior_re_ref[0], prior_im_ref[0])
    chunk_re, chunk_im = (chunk_re_ref[...], chunk_im_ref[...])
    add_re = carry_re_ref[...] + chunk_re * prior_re - chunk_im * prior_im
    add_im = carry_im_ref[...] + chunk_re * prior_im + chunk_im * prior_re
    pole_re = jnp.broadcast_to(pole_re_ref[0], (SUB, width))
    pole_im = jnp.broadcast_to(pole_im_ref[0], (SUB, width))
    for step in range(rows // SUB):
        at = slice(step * SUB, (step + 1) * SUB)
        turned_re = pole_re * add_re - pole_im * add_im
        turned_im = pole_re * add_im + pole_im * add_re
        full_ref[at, :width] = state_ref[at, :width] + turned_re
        full_ref[at, width:] = state_ref[at, width:] + turned_im
        add_re, add_im = turned_re, turned_im
    summed = jnp.dot(
        full_ref[...], read_ref[0], precision=lax.Precision.HIGHEST,
        preferred_element_type=jnp.float32,
    )
    shuffled = jnp.dot(
        token_shuffle(rows, False), u_ref[...], preferred_element_type=jnp.float32
    )
    mixed = jax.nn.gelu(summed + skip_ref[...] * shuffled).astype(jnp.bfloat16)
    out_ref[...] = jnp.dot(
        token_shuffle(rows, True), mixed, preferred_element_type=jnp.float32
    ).astype(jnp.bfloat16)


def block_diagonal(parts):
    blocks, per, rows, columns = parts[0].shape
    same = jnp.eye(per, dtype=bool)[None, :, None, :, None]
    spread = [
        jnp.where(same, part[:, :, :, None, :], 0.0).reshape(blocks, per * rows, per * columns)
        for part in parts
    ]
    return jnp.concatenate(spread, axis=2)


def state_tables(rows, decay_rate, rotation, log_step, in_re, in_im, out_re, out_im):
    groups, states = decay_rate.shape
    group_width = in_re.shape[-1]
    per = min(groups, max(1, 128 // group_width))
    blocks, width = (groups // per, per * states)
    pole_re, pole_im, drive_re, drive_im = discretize(decay_rate, rotation, log_step, in_re, in_im)
    steps = rows // SUB

    def by_block(value):
        return value.reshape(blocks, per, *value.shape[1:])

    def flat(value):
        return value.reshape(blocks, 1, width)

    drive = block_diagonal(
        [by_block(jnp.swapaxes(drive_re, 1, 2)), by_block(jnp.swapaxes(drive_im, 1, 2))]
    )
    read = jnp.swapaxes(block_diagonal([by_block(out_re), by_block(-out_im)]), 1, 2)
    jump = complex_power(decay_rate, rotation, log_step, float(steps))
    chunk_powers = [
        complex_power(decay_rate, rotation, log_step, float(steps * c)) for c in range(SUB)
    ]
    chunk_re = jnp.stack([p[0].reshape(groups * states) for p in chunk_powers])
    chunk_im = jnp.stack([p[1].reshape(groups * states) for p in chunk_powers])
    return dict(
        drive=drive, read=read, pole_re=flat(pole_re), pole_im=flat(pole_im),
        jump_re=flat(jump[0]), jump_im=flat(jump[1]), chunk_re=chunk_re, chunk_im=chunk_im,
        blocks=blocks, width=width, channels=per * group_width,
    )


def local_scan(inputs, tables):
    rows = inputs.shape[0]
    blocks, width, channels = (tables["blocks"], tables["width"], tables["channels"])
    row_spec = pl.BlockSpec((1, 1, width), lambda b: (b, 0, 0))
    carry_spec = pl.BlockSpec((SUB, width), lambda b: (0, b))
    return pl.pallas_call(
        scan_kernel,
        grid=(blocks,),
        in_specs=[
            pl.BlockSpec((rows, channels), lambda b: (0, b)),
            pl.BlockSpec((1, channels, 2 * width), lambda b: (b, 0, 0)),
            row_spec, row_spec, row_spec, row_spec,
        ],
        out_specs=[
            pl.BlockSpec((rows, 2 * width), lambda b: (0, b)),
            carry_spec, carry_spec, row_spec, row_spec,
        ],
        out_shape=[
            jax.ShapeDtypeStruct((rows, 2 * width * blocks), jnp.float32),
            jax.ShapeDtypeStruct((SUB, width * blocks), jnp.float32),
            jax.ShapeDtypeStruct((SUB, width * blocks), jnp.float32),
            jax.ShapeDtypeStruct((blocks, 1, width), jnp.float32),
            jax.ShapeDtypeStruct((blocks, 1, width), jnp.float32),
        ],
        cost_estimate=pl.CostEstimate(
            flops=12 * rows * channels * width * blocks, bytes_accessed=10**7, transcendentals=0
        ),
    )(
        inputs, tables["drive"], tables["pole_re"], tables["pole_im"],
        tables["jump_re"], tables["jump_im"],
    )


def read_states(inputs, scanned, prior_re, prior_im, tables, skip_gain):
    rows = inputs.shape[0]
    state, carry_re, carry_im = scanned[:3]
    blocks, width, channels = (tables["blocks"], tables["width"], tables["channels"])
    row_spec = pl.BlockSpec((1, 1, width), lambda b: (b, 0, 0))
    carry_spec = pl.BlockSpec((SUB, width), lambda b: (0, b))
    return pl.pallas_call(
        readout_kernel,
        grid=(blocks,),
        in_specs=[
            pl.BlockSpec((rows, channels), lambda b: (0, b)),
            pl.BlockSpec((rows, 2 * width), lambda b: (0, b)),
            carry_spec, carry_spec, row_spec, row_spec, carry_spec, carry_spec,
            row_spec, row_spec,
            pl.BlockSpec((1, 2 * width, channels), lambda b: (b, 0, 0)),
            pl.BlockSpec((1, channels), lambda b: (0, b)),
        ],
        out_specs=pl.BlockSpec((rows, channels), lambda b: (0, b)),
        out_shape=jax.ShapeDtypeStruct((rows, channels * blocks), jnp.bfloat16),
        scratch_shapes=[pltpu.VMEM((rows, 2 * width), jnp.float32)],
        cost_estimate=pl.CostEstimate(
            flops=12 * rows * channels * width * blocks, bytes_accessed=10**7, transcendentals=0
        ),
    )(
        inputs, state, carry_re, carry_im, prior_re, prior_im,
        tables["chunk_re"], tables["chunk_im"], tables["pole_re"], tables["pole_im"],
        tables["read"], skip_gain.reshape(1, -1),
    )


def carried_state(end_re, end_im, decay_rate, rotation, log_step, rows):
    ends = jnp.stack([end_re, end_im])
    shape = end_re.shape
    size = lax.axis_size("sp")
    reach = 1
    while reach < size:
        power_re, power_im = complex_power(decay_rate, rotation, log_step, float(rows * reach))
        power_re, power_im = (power_re.reshape(shape), power_im.reshape(shape))
        prior = passed_along(ends, "sp", reach)
        ends = ends + jnp.stack(
            [
                power_re * prior[0] - power_im * prior[1],
                power_re * prior[1] + power_im * prior[0],
            ]
        )
        reach *= 2
    before = passed_along(ends, "sp", 1)
    return (before[0], before[1])


def state_branch(inputs, decay_rate, rotation, log_step, in_re, in_im, out_re, out_im, skip_gain):
    rows = inputs.shape[0]
    tables = state_tables(rows, decay_rate, rotation, log_step, in_re, in_im, out_re, out_im)
    scanned = local_scan(inputs, tables)
    prior_re, prior_im = carried_state(
        scanned[3], scanned[4], decay_rate, rotation, log_step, rows
    )
    return read_states(inputs, scanned, prior_re, prior_im, tables, skip_gain)


def earlier_window(key_rows, value_rows):
    joined = jnp.concatenate([key_rows, value_rows], axis=1)
    prior = passed_along(joined, "sp", 1)
    return jnp.concatenate([prior, joined], axis=0)


def make_adder(normed_cols):

    def add_pieces(carried, weight_pieces, row_start):
        updated = []
        for running_total, weight_piece in zip(carried, weight_pieces):
            product = lax.dot_general(
                normed_cols,
                weight_piece,
                (((0,), (0,)), ((), ())),
                preferred_element_type=jnp.float32,
            )
            updated.append(product)
        return tuple(updated)

    return add_pieces


def whole_weights_body(
    tokens,
    norm_gain,
    w_query,
    w_key,
    w_value,
    w_state_in,
    sink_logit,
    decay_rate,
    rotation,
    log_step,
    in_re,
    in_im,
    out_re,
    out_im,
    skip_gain,
    w_attn_out,
    w_state_out,
    out_gain,
):
    row_count = tokens.shape[0]
    window = WINDOW
    head_width = HEAD
    wide_tokens = tokens.astype(jnp.float32)
    normed = (
        wide_tokens
        * lax.rsqrt(jnp.mean(wide_tokens * wide_tokens, axis=-1, keepdims=True) + epsilon)
        * norm_gain
    ).astype(jnp.bfloat16)
    first_row = lax.axis_index("sp") * row_count
    positions = first_row + jnp.arange(row_count, dtype=jnp.int32)
    add_pieces = make_adder(jnp.transpose(normed))

    def empty_like(weight_shard):
        return jnp.zeros((row_count, weight_shard.shape[1]), jnp.float32)

    query_sum, key_sum, value_sum, input_sum = add_pieces(
        (empty_like(w_query), empty_like(w_key), empty_like(w_value), empty_like(w_state_in)),
        (
            lax.all_gather(w_query, "sp", axis=0, tiled=True),
            lax.all_gather(w_key, "sp", axis=0, tiled=True),
            lax.all_gather(w_value, "sp", axis=0, tiled=True),
            lax.all_gather(w_state_in, "sp", axis=0, tiled=True),
        ),
        jnp.int32(0),
    )
    queries, key_rows, value_rows = shape_heads(
        query_sum, key_sum, value_sum, positions, head_width
    )
    joined_rows = earlier_window(key_rows, value_rows)
    inputs = input_sum.astype(jnp.bfloat16)
    mixed_state = state_branch(
        inputs, decay_rate, rotation, log_step, in_re, in_im, out_re, out_im, skip_gain
    )
    kv_width = key_rows.shape[1]
    kv_heads = kv_width // head_width
    all_keys = joined_rows[:, :kv_width].reshape(window + row_count, kv_heads, head_width)
    all_values = joined_rows[:, kv_width:].reshape(window + row_count, kv_heads, head_width)
    attended = band_attention(queries, all_keys, all_values, sink_logit, first_row, window)
    attn_rows, state_rows = (
        lax.all_gather(w_attn_out, "sp", axis=1, tiled=True),
        lax.all_gather(w_state_out, "sp", axis=1, tiled=True),
    )
    projected = lax.psum_scatter(
        (
            jnp.dot(attended, attn_rows, preferred_element_type=jnp.float32)
            + jnp.dot(mixed_state, state_rows, preferred_element_type=jnp.float32)
        ).astype(jnp.bfloat16),
        "tp",
        scatter_dimension=0,
        tiled=True,
    ).astype(jnp.float32)
    row_scale = lax.rsqrt(jnp.mean(projected * projected, axis=-1, keepdims=True) + epsilon)
    return (projected * row_scale * out_gain).astype(jnp.bfloat16)


SIDE = 2
PLANE = SIDE * SIDE
CORES = 2
CHUNKS = 2
LANES = 128
MESH = pl.DeviceIdType.MESH


def place():
    me = lax.axis_index("sp")
    return (lax.div(me, PLANE), lax.rem(me, PLANE), lax.axis_index("tp"))


def plane_neighbours(spot):
    beside = spot + 1 - 2 * lax.rem(spot, SIDE)
    above = spot + SIDE - 2 * SIDE * lax.div(spot, SIDE)
    return (beside, above)


def greet(layers, layer, spot, core):
    barrier = pltpu.get_barrier_semaphore()
    beside, above = plane_neighbours(spot)
    for ahead in range(1, layers):
        other = lax.rem(layer + ahead, layers)
        pl.semaphore_signal(
            barrier, inc=1, device_id={"sp": other * PLANE + spot}, device_id_type=MESH
        )
    for other in (beside, above, PLANE - 1 - spot):
        pl.semaphore_signal(
            barrier, inc=1, device_id={"sp": layer * PLANE + other}, device_id_type=MESH
        )
    pl.semaphore_signal(barrier, inc=1, device_id={"tp": 1 - core}, device_id_type=MESH)


def greeted(layers):
    pl.semaphore_wait(pltpu.get_barrier_semaphore(), layers + 3)


def remote(source, target, send_sem, recv_sem, device):
    return pltpu.make_async_remote_copy(
        src_ref=source, dst_ref=target, send_sem=send_sem, recv_sem=recv_sem,
        device_id=device, device_id_type=MESH,
    )


def line_first(layers, layer, spot, source, held, send_sems, recv_sems):
    @pl.when(layer < layers - 1)
    def _():
        remote(
            source, held.at[layer], send_sems.at[0, 0], recv_sems.at[0, 0],
            {"sp": (layer + 1) * PLANE + spot},
        ).start()

    @pl.when(layer > 0)
    def _():
        remote(
            source, held.at[layer], send_sems.at[1, 0], recv_sems.at[1, 0],
            {"sp": (layer - 1) * PLANE + spot},
        ).start()


def line_pass(layers, layer, spot, hop, held, send_sems, recv_sems, landed=None):
    @pl.when(layer - hop >= 0)
    def _():
        block = held.at[layer - hop]
        remote(block, block, send_sems.at[0, 0], recv_sems.at[0, hop - 1], {"sp": 0}).wait_recv()

        @pl.when(layer < layers - 1)
        def _():
            if hop < layers - 1:
                remote(
                    block, block, send_sems.at[0, hop], recv_sems.at[0, hop],
                    {"sp": (layer + 1) * PLANE + spot},
                ).start()

        if landed is not None:
            landed(0, hop, block)

    @pl.when(layer + hop <= layers - 1)
    def _():
        block = held.at[layer + hop]
        remote(block, block, send_sems.at[1, 0], recv_sems.at[1, hop - 1], {"sp": 0}).wait_recv()

        @pl.when(layer > 0)
        def _():
            if hop < layers - 1:
                remote(
                    block, block, send_sems.at[1, hop], recv_sems.at[1, hop],
                    {"sp": (layer - 1) * PLANE + spot},
                ).start()

        if landed is not None:
            landed(1, hop, block)


def line_drain(layers, layer, source, held, send_sems, recv_sems):
    for hop in range(layers - 1):

        @pl.when((layer - hop >= 0) & (layer < layers - 1))
        def _():
            remote(
                source, held.at[layer], send_sems.at[0, hop], recv_sems.at[0, 0], {"sp": 0}
            ).wait_send()

        @pl.when((layer + hop <= layers - 1) & (layer > 0))
        def _():
            remote(
                source, held.at[layer], send_sems.at[1, hop], recv_sems.at[1, 0], {"sp": 0}
            ).wait_send()


def plane_halves(halves, slots, layer, spot, send_sems, recv_sems, half):
    beside, above = plane_neighbours(spot)
    return [
        remote(
            halves.at[half], slots.at[spot, half], send_sems.at[0, half],
            recv_sems.at[0, half], {"sp": layer * PLANE + beside},
        ),
        remote(
            halves.at[1 - half], slots.at[spot, 1 - half], send_sems.at[1, 1 - half],
            recv_sems.at[1, 1 - half], {"sp": layer * PLANE + above},
        ),
    ]


def plane_first(halves, slots, layer, spot, send_sems, recv_sems):
    for half in (0, 1):
        for copy in plane_halves(halves, slots, layer, spot, send_sems, recv_sems, half):
            copy.start()


def plane_pass(slots, layer, spot, send_sems, recv_sems):
    beside, above = plane_neighbours(spot)
    block = slots.at[beside, 0]
    remote(block, block, send_sems.at[0, 0], recv_sems.at[0, 0], {"sp": 0}).wait_recv()
    remote(
        block, block, send_sems.at[1, 2], recv_sems.at[1, 2], {"sp": layer * PLANE + above}
    ).start()
    block = slots.at[above, 1]
    remote(block, block, send_sems.at[0, 0], recv_sems.at[1, 1], {"sp": 0}).wait_recv()
    remote(
        block, block, send_sems.at[0, 2], recv_sems.at[0, 2], {"sp": layer * PLANE + beside}
    ).start()


def plane_landed(slots, spot, send_sems, recv_sems):
    for way, half in ((0, 1), (1, 0), (0, 2), (1, 2)):
        block = slots.at[spot, 0]
        remote(block, block, send_sems.at[0, 0], recv_sems.at[way, half], {"sp": 0}).wait_recv()
    for way in (0, 1):
        for half in (0, 1, 2):
            block = slots.at[spot, 0]
            remote(block, block, send_sems.at[way, half], recv_sems.at[0, 0], {"sp": 0}).wait_send()


def lanes_of(rows):
    return jnp.concatenate([rows[at : at + 1] for at in range(rows.shape[0])], axis=1)


def split_pair(value):
    high = value.astype(jnp.bfloat16)
    return (high, (value - high.astype(jnp.float32)).astype(jnp.bfloat16))


def make_tables(
    layer, rows, decay_ref, rotation_ref, step_ref, in_re_ref, in_im_ref, out_re_ref, out_im_ref,
    drive, read, powers,
):
    groups, group_width, states = in_re_ref.shape
    kinds, _, width2 = drive.shape
    per = groups // kinds
    width = per * states
    channels = per * group_width
    base = layer * groups
    decay = lanes_of(decay_ref[pl.ds(base, groups), :])
    rotation = lanes_of(rotation_ref[pl.ds(base, groups), :])
    step = jnp.exp(
        jnp.concatenate(
            [jnp.full((1, states), step_ref[base + at], jnp.float32) for at in range(groups)],
            axis=1,
        )
    )
    row = lax.broadcasted_iota(jnp.int32, (SUB, groups * states), 0)
    steps = rows // SUB
    shares = (row * steps, jnp.where(row == 0, 1, jnp.where(row == 1, steps, rows)))
    for at, share in enumerate(shares):
        share = share.astype(jnp.float32)
        modulus = jnp.exp(-decay * step * share)
        angle = rotation * step * share
        powers[2 * at] = modulus * jnp.cos(angle)
        powers[2 * at + 1] = modulus * jnp.sin(angle)
    pole_re, pole_im = (powers[2, 0:1, :], powers[3, 0:1, :])
    minus_one = pole_re - 1.0
    denominator = decay * decay + rotation * rotation
    factor_re = (pole_im * rotation - minus_one * decay) / denominator
    factor_im = (-pole_im * decay - minus_one * rotation) / denominator
    same = (
        lax.broadcasted_iota(jnp.int32, (channels, width), 0) // group_width
        == lax.broadcasted_iota(jnp.int32, (channels, width), 1) // states
    )

    def spread(pieces):
        beside = jnp.concatenate(pieces, axis=1)
        return jnp.concatenate([beside] * per, axis=0)

    for kind in range(kinds):
        lanes = slice(kind * width, (kind + 1) * width)
        f_re, f_im = (factor_re[:, lanes], factor_im[:, lanes])
        own = range(kind * per, (kind + 1) * per)
        m_re = spread([in_re_ref[at] for at in own])
        m_im = spread([in_im_ref[at] for at in own])
        for part, value in ((0, f_re * m_re - f_im * m_im), (1, f_re * m_im + f_im * m_re)):
            high, low = split_pair(jnp.where(same, value, 0.0))
            columns = slice(part * width, (part + 1) * width)
            drive[kind, :channels, columns] = high
            drive[kind, channels:, columns] = low
        r_re = spread([out_re_ref[at] for at in own])
        r_im = spread([-out_im_ref[at] for at in own])
        for part, value in ((0, r_re), (1, r_im)):
            high, low = split_pair(jnp.where(same, value, 0.0))
            columns = slice(part * width, (part + 1) * width)
            read[kind, :channels, columns] = high
            read[kind, channels:, columns] = low


def normalise(block, held, gain_ref, normed):
    _, parts, chunks, part_rows, model = held.shape
    tall = 16
    per = part_rows // tall

    @pl.loop(0, parts * chunks * per)
    def _(at):
        value = held[
            block, at // (chunks * per), (at // per) % chunks,
            pl.ds(pl.multiple_of((at % per) * tall, tall), tall), :,
        ].astype(jnp.float32)
        scale = lax.rsqrt(jnp.sum(value * value, axis=-1, keepdims=True) / model + epsilon)
        normed[block, pl.ds(pl.multiple_of(at * tall, tall), tall), :] = (
            value * scale * gain_ref[...]
        ).astype(jnp.bfloat16)


def project_block(block, spot, normed, weights, tables, queries, pairs, inputs):
    rows = normed.shape[1]
    layers = weights.shape[0]
    depth = weights.shape[2] * weights.shape[3]
    query_width, pair_width = (queries.shape[-1], pairs.shape[-1])
    half_width = HEAD // 2
    row_cos_ref, row_sin_ref, block_cos_ref, block_sin_ref = tables
    lane = lax.broadcasted_iota(jnp.int32, (rows, LANES), 1)
    low = lax.rem(lane, HEAD) < half_width

    def turn(value, cosine, sine):
        swapped = jnp.where(
            low, -pltpu.roll(value, LANES - half_width, 1), pltpu.roll(value, half_width, 1)
        )
        return value * cosine + swapped * sine

    total = None
    for at in range(layers * PLANE):
        piece = jnp.dot(
            normed[block, :, at * depth : (at + 1) * depth],
            weights[at // PLANE, at % PLANE].reshape(depth, weights.shape[-1]),
            preferred_element_type=jnp.float32,
        )
        total = piece if total is None else total + piece
    here = pl.ds(block * PLANE + spot, 1)
    block_cos, block_sin = (block_cos_ref[here, :], block_sin_ref[here, :])
    cosine = row_cos_ref[...] * block_cos - row_sin_ref[...] * block_sin
    sine = row_sin_ref[...] * block_cos + row_cos_ref[...] * block_sin
    turned = [turn(total[:, at : at + LANES], cosine, sine) for at in range(0, query_width, LANES)]
    queries[block] = jnp.concatenate(turned, axis=1).astype(jnp.bfloat16)
    value = total[:, query_width : query_width + pair_width]
    pairs[block] = jnp.where(lane < HEAD, turn(value, cosine, sine), value).astype(jnp.bfloat16)
    inputs[block] = jnp.dot(
        token_shuffle(rows, False), total[:, query_width + pair_width :].astype(jnp.bfloat16),
        preferred_element_type=jnp.float32,
    ).astype(jnp.bfloat16)


def scan_block(block, spot, inputs, drive, powers, states, carries, ends):
    kinds, _, width2 = drive.shape
    width = width2 // 2
    channels = inputs.shape[-1] // kinds
    rows = inputs.shape[1]
    for kind in range(kinds):
        lanes = slice(kind * width, (kind + 1) * width)
        own = inputs[block, :, kind * channels : (kind + 1) * channels]
        states[block, kind] = jnp.dot(
            jnp.concatenate([own, own], axis=1), drive[kind], preferred_element_type=jnp.float32
        )
        pole_re = jnp.broadcast_to(powers[2, 0:1, lanes], (SUB, width))
        pole_im = jnp.broadcast_to(powers[3, 0:1, lanes], (SUB, width))
        now_re = jnp.zeros((SUB, width), jnp.float32)
        now_im = jnp.zeros((SUB, width), jnp.float32)
        for step in range(rows // SUB):
            at = slice(step * SUB, (step + 1) * SUB)
            new_re = pole_re * now_re - pole_im * now_im + states[block, kind, at, :width]
            new_im = pole_re * now_im + pole_im * now_re + states[block, kind, at, width:]
            states[block, kind, at, :width] = new_re
            states[block, kind, at, width:] = new_im
            now_re, now_im = new_re, new_im
        jump_re, jump_im = (powers[2, 1:2, lanes], powers[3, 1:2, lanes])
        held_re = jnp.zeros((1, width), jnp.float32)
        held_im = jnp.zeros((1, width), jnp.float32)
        re, im = ([], [])
        for chunk in range(SUB):
            re.append(held_re)
            im.append(held_im)
            next_re = jump_re * held_re - jump_im * held_im + now_re[chunk : chunk + 1]
            next_im = jump_re * held_im + jump_im * held_re + now_im[chunk : chunk + 1]
            held_re, held_im = next_re, next_im
        carries[block, kind, :, :width] = jnp.concatenate(re, axis=0)
        carries[block, kind, :, width:] = jnp.concatenate(im, axis=0)
        ends[spot, block, kind, :, :width] = held_re
        ends[spot, block, kind, :, width:] = held_im


def attend_block(block, layer, spot, queries, pairs, before, sink_ref, out):
    rows, query_width = queries.shape[1:]
    group = query_width // HEAD
    pair, prior = (pairs[block], before[block])
    keys = jnp.concatenate([prior[:, :HEAD], pair[:, :HEAD]], axis=0)
    values = jnp.concatenate([prior[:, HEAD:], pair[:, HEAD:]], axis=0)
    query_at = lax.broadcasted_iota(jnp.int32, (rows, rows + WINDOW), 0)
    key_at = lax.broadcasted_iota(jnp.int32, (rows, rows + WINDOW), 1) - WINDOW
    gap = query_at - key_at
    first = (block * PLANE + spot) * rows
    visible = (gap >= 0) & (gap < WINDOW) & (key_at + first >= 0)
    pieces = []
    for head in range(group):
        query = queries[block, :, head * HEAD : (head + 1) * HEAD]
        scores = lax.dot_general(
            query, keys, (((1,), (1,)), ((), ())), preferred_element_type=jnp.float32
        ) / math.sqrt(HEAD)
        scores = jnp.where(visible, scores, -jnp.inf)
        sink = jnp.full((1, 1), sink_ref[layer * group + head], jnp.float32)
        top = jnp.maximum(jnp.max(scores, axis=-1, keepdims=True), sink)
        exponent = jnp.exp(scores - top)
        total = jnp.sum(exponent, axis=-1, keepdims=True) + jnp.exp(sink - top)
        weights = (exponent / total).astype(jnp.bfloat16)
        pieces.append(jnp.dot(weights, values, preferred_element_type=jnp.float32))
    out[...] = jnp.concatenate(pieces, axis=1).astype(jnp.bfloat16)


def find_priors(ends, powers, priors):
    plane, layers, kinds = ends.shape[:3]
    width = ends.shape[-1] // 2
    for kind in range(kinds):
        lanes = slice(kind * width, (kind + 1) * width)
        power_re, power_im = (powers[2, 2:3, lanes], powers[3, 2:3, lanes])
        held_re = jnp.zeros((1, width), jnp.float32)
        held_im = jnp.zeros((1, width), jnp.float32)
        for at in range(layers * plane):
            priors[at, kind, :, :width] = held_re
            priors[at, kind, :, width:] = held_im
            end_re = ends[at % plane, at // plane, kind, :, :width]
            end_im = ends[at % plane, at // plane, kind, :, width:]
            held_re, held_im = (
                power_re * held_re - power_im * held_im + end_re,
                power_re * held_im + power_im * held_re + end_im,
            )


def read_block(block, layer, spot, inputs, states, carries, priors, powers, read, skip_ref, out):
    kinds, channels2, width2 = read.shape
    width, channels = (width2 // 2, channels2 // 2)
    rows = inputs.shape[1]
    contract = (((1,), (1,)), ((), ()))
    pieces = []
    for kind in range(kinds):
        lanes = slice(kind * width, (kind + 1) * width)
        prior_re = priors[block * PLANE + spot, kind, :, :width]
        prior_im = priors[block * PLANE + spot, kind, :, width:]
        chunk_re, chunk_im = (powers[0, :, lanes], powers[1, :, lanes])
        add_re = carries[block, kind, :, :width] + chunk_re * prior_re - chunk_im * prior_im
        add_im = carries[block, kind, :, width:] + chunk_re * prior_im + chunk_im * prior_re
        pole_re = jnp.broadcast_to(powers[2, 0:1, lanes], (SUB, width))
        pole_im = jnp.broadcast_to(powers[3, 0:1, lanes], (SUB, width))
        for step in range(rows // SUB):
            at = slice(step * SUB, (step + 1) * SUB)
            turned_re = pole_re * add_re - pole_im * add_im
            turned_im = pole_re * add_im + pole_im * add_re
            states[block, kind, at, :width] += turned_re
            states[block, kind, at, width:] += turned_im
            add_re, add_im = turned_re, turned_im
        high, low = split_pair(states[block, kind])
        both = lax.dot_general(high, read[kind], contract, preferred_element_type=jnp.float32)
        rest = lax.dot_general(
            low, read[kind, :channels], contract, preferred_element_type=jnp.float32
        )
        summed = both[:, :channels] + both[:, channels:] + rest
        at = pl.multiple_of(layer * (kinds * channels) + kind * channels, channels)
        skip = skip_ref[:, pl.ds(at, channels)]
        own = inputs[block, :, kind * channels : (kind + 1) * channels].astype(jnp.float32)
        pieces.append(jax.nn.gelu(summed + skip * own).astype(jnp.bfloat16))
    out[...] = jnp.dot(
        token_shuffle(rows, True), jnp.concatenate(pieces, axis=1),
        preferred_element_type=jnp.float32,
    ).astype(jnp.bfloat16)


def whole_kernel(
    tokens_ref, query_ref, key_ref, value_ref, state_ref,
    in_re_ref, in_im_ref, out_re_ref, out_im_ref, attn_out_ref, state_out_ref,
    norm_gain_ref, out_gain_ref, decay_ref, rotation_ref, skip_ref,
    row_cos_ref, row_sin_ref, block_cos_ref, block_sin_ref, step_ref, sink_ref,
    out_ref,
    key_value, packed, weights, held, normed, in_re, in_im, out_re, out_im, drive, read, powers,
    queries, pairs, before, inputs, states, carries, ends, priors,
    mixers, matrices, total, partial, arrived, summed, pieces,
    load_sem, pack_sem, far_send, far_recv, line_send, line_recv, part_send, part_recv,
    side_send, side_recv, halo_send, halo_recv, end_send, end_recv,
    mixer_send, mixer_recv, matrix_send, matrix_recv, half_send, half_recv,
    piece_send, piece_recv,
):
    layers = held.shape[0]
    rows = pairs.shape[1]
    layer, spot, core = place()
    greet(layers, layer, spot, core)
    query_width, pair_width = (queries.shape[-1], pairs.shape[-1])
    state_width = inputs.shape[-1]
    groups = in_re.shape[0]
    mine = pl.ds(layer * groups, groups)
    loads = [
        pltpu.make_async_copy(key_ref, key_value.at[0], load_sem.at[0]),
        pltpu.make_async_copy(value_ref, key_value.at[1], load_sem.at[1]),
    ]
    spans = (
        (query_ref, query_width, 0),
        (state_ref, state_width, query_width + pair_width),
    )
    def loaded(block, target, at):
        return [
            pltpu.make_async_copy(
                source.at[:, :, pl.ds(pl.multiple_of(block * wide, wide), wide)],
                target.at[:, :, pl.ds(to, wide)], pack_sem.at[at, part],
            )
            for part, (source, wide, to) in enumerate(spans)
        ]

    own_weights = loaded(layer, weights.at[layer, spot], layers)
    far_loads = [copy for at in range(layers) for copy in loaded(at, packed.at[at], at)]
    own_tokens = pltpu.make_async_copy(tokens_ref, held.at[layer], load_sem.at[3])
    table_loads = [
        pltpu.make_async_copy(source.at[mine], target, load_sem.at[5 + at])
        for at, (source, target) in enumerate(
            ((in_re_ref, in_re), (in_im_ref, in_im), (out_re_ref, out_re), (out_im_ref, out_im))
        )
    ]
    matrix_loads = [
        pltpu.make_async_copy(source, matrices.at[kind, spot], load_sem.at[9 + kind])
        for kind, source in enumerate((attn_out_ref, state_out_ref))
    ]
    for copy in loads + own_weights + far_loads + [own_tokens] + table_loads + matrix_loads:
        copy.start()
    for copy in loads:
        copy.wait()
    middle = slice(query_width, query_width + pair_width)
    for at in range(layers):
        head = slice(at * HEAD, (at + 1) * HEAD)
        packed[at, :, :, middle] = jnp.concatenate(
            [key_value[0, :, :, head], key_value[1, :, :, head]], axis=-1
        )
    weights[layer, spot, :, :, middle] = packed[layer, :, :, middle]
    for copy in far_loads:
        copy.wait()
    greeted(layers)

    below, above = (layer, layers - 1 - layer)
    least = jnp.minimum(below, above)
    short = jnp.where(below < above, 0, 1)

    def arrival(at):
        paired = at <= 2 * least
        hop = jnp.where(paired, lax.div(at + 1, 2), at - least)
        way = jnp.where(paired & (lax.rem(at, 2) == 1), short, 1 - short)
        return (jnp.where(way == 0, layer - hop, layer + hop), hop, way)

    def far_copy(way, hop):
        other = layer + hop if way == 0 else layer - hop
        return remote(
            packed.at[other], weights.at[layer, spot], far_send.at[way, hop],
            far_recv.at[way, hop], {"sp": other * PLANE + spot},
        )

    def each_far(hop, action):
        for way, there in ((0, layer + hop <= layers - 1), (1, layer - hop >= 0)):

            @pl.when(there)
            def _():
                action(far_copy(way, hop))

    def start(copy):
        copy.start()

    each_far(1, start)

    @pl.when(least > 0)
    def _():
        for hop in range(2, layers):
            each_far(hop, start)

    chunks = held.shape[2]

    def chunk_lines(action):
        for chunk in range(chunks):
            action(chunk, held.at[:, core, chunk], line_send.at[chunk], line_recv.at[chunk])

    for copy in own_weights:
        copy.wait()

    def part(way, hop, chunk, half):
        block = held.at[layer + hop - 2 * hop * (1 - way), half, chunk]
        return remote(
            block, block, part_send.at[chunk, way, hop - 1], part_recv.at[chunk, way, hop - 1],
            {"tp": 1 - core},
        )

    def send_tokens(side):
        onward = 1 - side
        for chunk in range(chunks):
            remote(
                tokens_ref.at[core, chunk], held.at[layer, core, chunk],
                line_send.at[chunk, onward, 0], line_recv.at[chunk, onward, 0],
                {"sp": (layer + 1 - 2 * onward) * PLANE + spot},
            ).start()

    def pass_tokens(way, hop):
        block = layer + hop - 2 * hop * (1 - way)

        def step(chunk, slots, send, recv):
            half = slots.at[block]
            remote(half, half, send.at[way, 0], recv.at[way, hop - 1], {"sp": 0}).wait_recv()
            onward = jnp.where(way == 0, layer < layers - 1, layer > 0)

            @pl.when(onward & (hop < layers - 1))
            def _():
                remote(
                    half, half, send.at[way, hop], recv.at[way, hop],
                    {"sp": (layer + 1 - 2 * way) * PLANE + spot},
                ).start()

            part(way, hop, chunk, core).start()

        chunk_lines(step)

    plane_first(
        weights.at[layer, spot], weights.at[layer], layer, spot, side_send.at[0], side_recv.at[0]
    )

    @pl.when(least == 0)
    def _():
        send_tokens(1 - short)

    for copy in table_loads:
        copy.wait()
    make_tables(
        layer, rows, decay_ref, rotation_ref, step_ref, in_re, in_im, out_re, out_im,
        drive, read, powers,
    )
    before[0] = jnp.zeros(before.shape[1:], before.dtype)
    own_tokens.wait()
    normalise(layer, held, norm_gain_ref, normed)
    plane_pass(weights.at[layer], layer, spot, side_send.at[0], side_recv.at[0])

    for at in range(1, layers):
        origin, hop, way = arrival(jnp.int32(at))
        block = weights.at[origin, spot]
        remote(block, block, far_send.at[0, 0], far_recv.at[way, hop], {"sp": 0}).wait_recv()

        if at == 1:

            @pl.when(least > 0)
            def _():
                send_tokens(short)

        if at == layers - 1:

            @pl.when(least > 0)
            def _():
                send_tokens(1 - short)

        plane_first(
            weights.at[origin, spot], weights.at[origin], layer, spot,
            side_send.at[at], side_recv.at[at],
        )
        plane_pass(weights.at[origin], layer, spot, side_send.at[at], side_recv.at[at])
        if at == 1:

            @pl.when(least == 0)
            def _():
                for hop in range(2, layers):
                    each_far(hop, start)

    for copy in matrix_loads:
        copy.wait()
    plane_first(
        matrices.at[0, spot], matrices.at[0], layer, spot, matrix_send.at[0], matrix_recv.at[0]
    )

    @pl.when(least > 0)
    def _():
        pass_tokens(short, 1)

    pass_tokens(1 - short, 1)

    def landed(at):
        block, hop, way = arrival(at)
        for chunk in range(chunks):
            part(way, hop, chunk, 1 - core).wait_recv()
        normalise(block, held, norm_gain_ref, normed)

    for at in range(1, layers):
        hop = arrival(jnp.int32(at))[1]

        @pl.when(hop == 1)
        def _():
            landed(jnp.int32(at))

    for at in range(layers):
        origin = layer if at == 0 else arrival(jnp.int32(at))[0]
        plane_landed(weights.at[origin], spot, side_send.at[at], side_recv.at[at])
    for hop in range(1, layers):
        each_far(hop, lambda copy: copy.wait_send())

    behind = layer * PLANE + lax.rem(spot + 1, PLANE)
    late = lax.div(spot, PLANE - 1)

    def hand_on(block):
        return remote(
            pairs.at[block], before.at[block + late], halo_send.at[block],
            halo_recv.at[block + late], {"sp": behind},
        )

    def arrive(block):
        remote(
            pairs.at[0], before.at[block], halo_send.at[0], halo_recv.at[block], {"sp": behind}
        ).wait_recv()

    def tell(block, at):
        other = lax.rem(spot + 1 + at, PLANE)
        return remote(
            ends.at[spot, block], ends.at[spot, block], end_send.at[at, block],
            end_recv.at[at, block], {"sp": layer * PLANE + other},
        )

    def pass_on(at):
        _, hop, way = arrival(at)

        @pl.when(hop > 1)
        def _():
            pass_tokens(way, hop)

    def send_mixer(kind, block):
        columns = mixers.at[layer, kind, block]
        for way, there in ((0, layer < layers - 1), (1, layer > 0)):

            @pl.when(there)
            def _():
                remote(
                    columns, columns, mixer_send.at[kind, block, way, 0],
                    mixer_recv.at[kind, block, way, 0],
                    {"sp": (layer + 1 - 2 * way) * PLANE + spot},
                ).start()

    def attend(block):
        attend_block(
            block, layer, spot, queries, pairs, before, sink_ref, mixers.at[layer, 0, block]
        )
        send_mixer(0, block)

    def attend_step(at):
        block, hop, way = arrival(at)

        @pl.when((spot > 0) | (block == 0) | ((at > 0) & (way == 1)))
        def _():
            @pl.when((spot > 0) | (block > 0))
            def _():
                arrive(block)

            attend(block)

        @pl.when((spot == 0) & (at > 0) & (way == 0))
        def _():
            arrive(block + 1)
            attend(block + 1)

    def second_matrix(half):
        for copy in plane_halves(
            matrices.at[1, spot], matrices.at[1], layer, spot, matrix_send.at[1],
            matrix_recv.at[1], half,
        ):
            copy.start()

    def attend_all_but_last():
        @pl.loop(0, layers - 1)
        def _(at):
            attend_step(at)

    @pl.loop(0, layers)
    def _(at):
        block, hop, way = arrival(at)
        is_last = at == layers - 1

        @pl.when((least == 0) & is_last)
        def _():
            attend_all_but_last()

        @pl.when((least == 0) & (at > 0))
        def _():
            pass_on(at)

        @pl.when(hop > 1)
        def _():
            landed(at)

        project_block(
            block, spot, normed, weights,
            (row_cos_ref, row_sin_ref, block_cos_ref, block_sin_ref), queries, pairs, inputs,
        )
        hand_on(block).start()
        scan_block(block, spot, inputs, drive, powers, states, carries, ends)
        for peer in range(PLANE - 1):
            tell(block, peer).start()

        @pl.when((least > 0) & (at < layers - 1))
        def _():
            pass_on(at + 1)

        @pl.when((least == 0) & (at == 2))
        def _():
            plane_pass(matrices.at[0], layer, spot, matrix_send.at[0], matrix_recv.at[0])
            second_matrix(0)

        @pl.when((least > 0) & is_last)
        def _():
            attend_all_but_last()

    attend_step(jnp.int32(layers - 1))

    @pl.when(spot == 0)
    def _():
        arrive(layers)

    @pl.when(least > 0)
    def _():
        plane_pass(matrices.at[0], layer, spot, matrix_send.at[0], matrix_recv.at[0])
        second_matrix(0)

    second_matrix(1)
    for block in range(layers):
        for peer in range(PLANE - 1):
            tell(block, peer).wait()
    find_priors(ends, powers, priors)

    @pl.loop(0, layers)
    def _(block):
        read_block(
            block, layer, spot, inputs, states, carries, priors, powers, read, skip_ref,
            mixers.at[layer, 1, block],
        )
        send_mixer(1, block)

    depth = mixers.shape[-1]
    tokens = layers * rows
    half_depth, width = matrices.shape[3:]
    half_rows = rows // CORES
    per = half_depth // depth

    def take(at):
        block, hop, way = arrival(at)

        onward = jnp.where(way == 0, layer < layers - 1, layer > 0)
        for kind in (0, 1):
            for part in range(layers):
                at = jnp.where(2 * block < layers, part, layers - 1 - part) if kind == 0 else part
                columns = mixers.at[block, kind, at]
                remote(
                    columns, columns, mixer_send.at[kind, at, 0, 0],
                    mixer_recv.at[kind, at, way, hop - 1], {"sp": 0},
                ).wait_recv()

                @pl.when(onward & (hop < layers - 1))
                def _():
                    remote(
                        columns, columns, mixer_send.at[kind, at, way, hop],
                        mixer_recv.at[kind, at, way, hop],
                        {"sp": (layer + 1 - 2 * way) * PLANE + spot},
                    ).start()

    def product(block, column):
        low = pl.ds(pl.multiple_of(lax.rem(block, per) * depth, depth), depth)
        return sum(
            jnp.dot(
                mixers[block, kind].reshape(tokens, depth),
                matrices[kind, column, lax.div(block, per), low, :],
                preferred_element_type=jnp.float32,
            )
            for kind in (0, 1)
        )

    for at in range(1, layers - 1):
        take(jnp.where(at <= 2 * least, at - 1 + 2 * (at % 2), at))
        if at == 1:
            plane_pass(matrices.at[1], layer, spot, matrix_send.at[1], matrix_recv.at[1])
    @pl.when(least > 0)
    def _():
        take(jnp.int32(layers - 1))

    for kind in (0, 1):
        plane_landed(matrices.at[kind], spot, matrix_send.at[kind], matrix_recv.at[kind])

    @pl.loop(0, PLANE)
    def _(column):
        total[column] = sum(
            product(arrival(jnp.int32(at))[0], column) for at in range(layers - 1)
        )

    @pl.when(least == 0)
    def _():
        take(jnp.int32(layers - 1))

    last = arrival(jnp.int32(layers - 1))[0]

    def swap(column):
        return remote(
            partial.at[column, 1 - core], arrived.at[column], half_send.at[column],
            half_recv.at[column], {"tp": 1 - core},
        )

    def each_piece(column, action):
        for hop in range(layers - 1, 0, -1):
            for way, there in ((0, layer + hop <= layers - 1), (1, layer - hop >= 0)):

                @pl.when(there)
                def _():
                    other = layer + hop if way == 0 else layer - hop
                    action(
                        remote(
                            summed.at[column, other], pieces.at[column, layer],
                            piece_send.at[column, way, hop], piece_recv.at[column, way, hop],
                            {"sp": other * PLANE + spot},
                        )
                    )

    def each_landing(column):
        for hop in range(1, layers):
            for way, there in ((0, layer - hop >= 0), (1, layer + hop <= layers - 1)):

                @pl.when(there)
                def _():
                    other = layer - hop if way == 0 else layer + hop
                    piece = pieces.at[column, other]
                    remote(
                        piece, piece, piece_send.at[0, 0, 0], piece_recv.at[column, way, hop],
                        {"sp": 0},
                    ).wait_recv()

    def send_column(column):
        swap(column).wait_recv()
        for at in range(layers):
            summed[column, at] = (
                partial[column, core, at].astype(jnp.float32)
                + arrived[column, at].astype(jnp.float32)
            ).astype(jnp.bfloat16)
        each_piece(column, lambda copy: copy.start())
        pieces[column, layer] = summed[column, layer]

    for column in range(PLANE):
        value = total[column] + product(last, column)
        value = value.astype(jnp.bfloat16).reshape(layers, CORES, half_rows, width)
        for half in range(CORES):
            partial[column, half] = value[:, half]
        swap(column).start()
        if column == 0:
            for kind in (0, 1):
                for at in range(layers):
                    line_drain(
                        layers, layer, mixers.at[layer, kind, at], mixers.at[:, kind, at],
                        mixer_send.at[kind, at], mixer_recv.at[kind, at],
                    )
        if column > 0:
            send_column(column - 1)
    send_column(PLANE - 1)
    chunk_lines(
        lambda chunk, slots, send, recv: line_drain(
            layers, layer, slots.at[layer], slots, send, recv
        )
    )
    for hop in range(1, layers):
        for way, there in ((0, layer - hop >= 0), (1, layer + hop <= layers - 1)):

            @pl.when(there)
            def _():
                for chunk in range(chunks):
                    part(way, hop, chunk, core).wait_send()

    for block in range(layers):
        hand_on(block).wait_send()
    squares = jnp.zeros((half_rows, width), jnp.float32)
    for column in range(PLANE):
        each_landing(column)
        for at in range(layers):
            value = pieces[column, at].astype(jnp.float32)
            squares = squares + value * value
    for column in range(PLANE):
        swap(column).wait_send()
        each_piece(column, lambda copy: copy.wait_send())
    mean = jnp.sum(squares, axis=-1, keepdims=True) / (layers * PLANE * width)
    scale = lax.rsqrt(mean + epsilon)
    for at in range(layers):
        for column in range(PLANE):
            low = (at * PLANE + column) * width
            columns = slice(low, low + width)
            out_ref[:, columns] = (
                pieces[column, at].astype(jnp.float32) * scale * out_gain_ref[:, columns]
            ).astype(jnp.bfloat16)


def body(
    tokens,
    norm_gain,
    w_query,
    w_key,
    w_value,
    w_state_in,
    sink_logit,
    decay_rate,
    rotation,
    log_step,
    in_re,
    in_im,
    out_re,
    out_im,
    skip_gain,
    w_attn_out,
    w_state_out,
    out_gain,
):
    rows, model = tokens.shape
    layers = lax.axis_size("sp") // PLANE
    half_rows = rows // CORES
    depth = w_query.shape[0]
    query_width = w_query.shape[1] // layers
    pair_width = 2 * (w_key.shape[1] // layers)
    state_width = w_state_in.shape[1] // layers
    width = query_width + pair_width + state_width
    groups, states, group_width = (in_re.shape[0] // layers, in_re.shape[1], in_re.shape[2])
    kinds = state_width // LANES
    lanes = groups // kinds * states
    height, out_width = w_attn_out.shape
    half = HEAD // 2
    frequency = rotary_base ** (-(np.arange(half) * 2.0 / HEAD))
    frequency = np.tile(frequency, LANES // half)[None, :]
    within = np.arange(rows)[:, None] * frequency
    across = (np.arange(layers * PLANE) * rows)[:, None] * frequency
    tables = [np.cos(within), np.sin(within), np.cos(across), np.sin(across)]
    tables = [jnp.asarray(t, jnp.float32) for t in tables]
    anywhere = pl.BlockSpec(memory_space=pl.ANY)
    vmem = pl.BlockSpec(memory_space=pltpu.VMEM)
    smem = pl.BlockSpec(memory_space=pltpu.SMEM)
    dma = pltpu.SemaphoreType.DMA
    low, full = (jnp.bfloat16, jnp.float32)
    piece = pltpu.VMEM((PLANE, layers, half_rows, out_width), low)

    def halved(matrix):
        return matrix.reshape(2, matrix.shape[0] // 2, matrix.shape[1])

    return pl.pallas_call(
        whole_kernel,
        out_shape=jax.ShapeDtypeStruct((half_rows, model), low),
        in_specs=[anywhere] * 11 + [vmem] * 9 + [smem] * 2,
        out_specs=vmem,
        scratch_shapes=[
            pltpu.VMEM((2, 2, depth // 2, w_key.shape[1]), low),
            pltpu.VMEM((layers, 2, depth // 2, width), low),
            pltpu.VMEM((layers, PLANE, 2, depth // 2, width), low),
            pltpu.VMEM((layers, CORES, CHUNKS, half_rows // CHUNKS, model), low),
            pltpu.VMEM((layers, rows, model), low),
            pltpu.VMEM((groups, group_width, states), full),
            pltpu.VMEM((groups, group_width, states), full),
            pltpu.VMEM((groups, group_width, states), full),
            pltpu.VMEM((groups, group_width, states), full),
            pltpu.VMEM((kinds, 2 * LANES, 2 * lanes), low),
            pltpu.VMEM((kinds, 2 * LANES, 2 * lanes), low),
            pltpu.VMEM((4, SUB, groups * states), full),
            pltpu.VMEM((layers, rows, query_width), low),
            pltpu.VMEM((layers, rows, pair_width), low),
            pltpu.VMEM((layers + 1, rows, pair_width), low),
            pltpu.VMEM((layers, rows, state_width), low),
            pltpu.VMEM((layers, kinds, rows, 2 * lanes), full),
            pltpu.VMEM((layers, kinds, SUB, 2 * lanes), full),
            pltpu.VMEM((PLANE, layers, kinds, 1, 2 * lanes), full),
            pltpu.VMEM((layers * PLANE, kinds, 1, 2 * lanes), full),
            pltpu.VMEM((layers, 2, layers, rows, query_width), low),
            pltpu.VMEM((2, PLANE, 2, height // 2, out_width), low),
            pltpu.VMEM((PLANE, layers * rows, out_width), full),
            pltpu.VMEM((PLANE, CORES, layers, half_rows, out_width), low),
            piece, piece, piece,
            dma((11,)), dma((layers + 1, 2)), dma((2, layers)), dma((2, layers)),
            dma((CHUNKS, 2, layers)), dma((CHUNKS, 2, layers)),
            dma((CHUNKS, 2, layers)), dma((CHUNKS, 2, layers)),
            dma((layers, 2, 3)), dma((layers, 2, 3)), dma((layers,)), dma((layers + 1,)),
            dma((PLANE - 1, layers)), dma((PLANE - 1, layers)),
            dma((2, layers, 2, layers)), dma((2, layers, 2, layers)),
            dma((2, 2, 3)), dma((2, 2, 3)),
            dma((PLANE,)), dma((PLANE,)), dma((PLANE, 2, layers)), dma((PLANE, 2, layers)),
        ],
        compiler_params=pltpu.CompilerParams(
            collective_id=0, has_side_effects=True, vmem_limit_bytes=60 * 2**20
        ),
    )(
        tokens.reshape(CORES, CHUNKS, half_rows // CHUNKS, model), halved(w_query), halved(w_key), halved(w_value),
        halved(w_state_in), jnp.swapaxes(in_re, 1, 2), jnp.swapaxes(in_im, 1, 2), out_re, out_im, halved(w_attn_out),
        halved(w_state_out), norm_gain.reshape(1, -1), out_gain.reshape(1, -1), decay_rate,
        rotation, skip_gain.reshape(1, -1), *tables, log_step, sink_logit,
    )


def suits(mesh, shapes):
    size, cores = (mesh.shape["sp"], mesh.shape["tp"])
    layers = size // PLANE
    query_width, key_width, state_width = (shapes[at][1] // cores for at in (2, 3, 5))
    return (
        size % PLANE == 0
        and layers % 4 == 0
        and cores == CORES
        and shapes[0][0] // size == WINDOW
        and key_width == layers * HEAD
        and state_width == query_width
        and query_width % (layers * LANES) == 0
    )


def solution(mesh):
    def run(*arrays):
        chosen = body if suits(mesh, [array.shape for array in arrays]) else whole_weights_body
        return sharded(mesh, chosen)(*arrays)

    return run


def sharded(mesh, chosen):
    return jax.shard_map(
        chosen,
        mesh=mesh,
        in_specs=(
            P("sp", None),
            P(),
            P("sp", "tp"),
            P("sp", "tp"),
            P("sp", "tp"),
            P("sp", "tp"),
            P("tp"),
            P("tp", None),
            P("tp", None),
            P("tp"),
            P("tp", None, None),
            P("tp", None, None),
            P("tp", None, None),
            P("tp", None, None),
            P("tp"),
            P("tp", "sp"),
            P("tp", "sp"),
            P(),
        ),
        out_specs=P(("sp", "tp"), None),
        check_vma=False,
    )
```

```python
import math

import jax
import jax.numpy as jnp
import numpy as np
from jax import lax
from jax.experimental import pallas as pl
from jax.experimental.pallas import tpu as pltpu
from jax.sharding import PartitionSpec as P

HEAD = 64
WINDOW = 128
SUB = 8


epsilon = 1e-06
rotary_base = 500000.0


def passed_along(value, axis, by):
    size = lax.axis_size(axis)
    pairs = [(i, i + by) for i in range(size) if 0 <= i + by < size]
    return lax.ppermute(value, axis, pairs)


def rotate(heads_block, positions):
    head_width = heads_block.shape[-1]
    half_width = head_width // 2
    frequency = rotary_base ** (-(jnp.arange(half_width, dtype=jnp.float32) * 2.0 / head_width))
    angles = positions.astype(jnp.float32)[:, None] * frequency[None, :]
    cosine = jnp.cos(angles)[:, None, :]
    sine_part = jnp.sin(angles)[:, None, :]
    lower_half = heads_block[..., :half_width]
    upper_half = heads_block[..., half_width:]
    return jnp.concatenate(
        [
            lower_half * cosine - upper_half * sine_part,
            upper_half * cosine + lower_half * sine_part,
        ],
        axis=-1,
    )


def shape_heads(query_sum, key_sum, value_sum, positions, head_width):
    row_count = query_sum.shape[0]
    kv_heads = key_sum.shape[1] // head_width
    group_size = query_sum.shape[1] // key_sum.shape[1]
    queries = rotate(
        query_sum.reshape(row_count, kv_heads * group_size, head_width), positions
    ).astype(jnp.bfloat16)
    queries = queries.reshape(row_count, kv_heads, group_size, head_width)
    key_rows = rotate(key_sum.reshape(row_count, kv_heads, head_width), positions).astype(
        jnp.bfloat16
    )
    key_rows = key_rows.reshape(row_count, kv_heads * head_width)
    value_rows = value_sum.astype(jnp.bfloat16)
    return (queries, key_rows, value_rows)


def band_attention(queries, key_rows, value_rows, sink_logit, first_row, window):
    row_count, kv_heads, group_size, head_width = queries.shape
    blocks = row_count // window
    query_blocks = queries.reshape(blocks, window, kv_heads, group_size, head_width)
    key_blocks = jnp.concatenate(
        [
            key_rows[:row_count].reshape(blocks, window, kv_heads, head_width),
            key_rows[window:].reshape(blocks, window, kv_heads, head_width),
        ],
        axis=1,
    )
    value_blocks = jnp.concatenate(
        [
            value_rows[:row_count].reshape(blocks, window, kv_heads, head_width),
            value_rows[window:].reshape(blocks, window, kv_heads, head_width),
        ],
        axis=1,
    )
    scores = jnp.einsum(
        "bqkgd,bskd->bkgqs", query_blocks, key_blocks, preferred_element_type=jnp.float32
    ) / math.sqrt(head_width)
    block_start = jnp.arange(blocks, dtype=jnp.int32)[:, None, None] * window
    query_at = first_row + block_start + jnp.arange(window, dtype=jnp.int32)[None, :, None]
    key_at = (
        first_row - window + block_start + jnp.arange(2 * window, dtype=jnp.int32)[None, None, :]
    )
    offset_gap = query_at - key_at
    visible = (offset_gap >= 0) & (offset_gap < window) & (key_at >= 0)
    scores = jnp.where(visible[:, None, None, :, :], scores, -jnp.inf)
    sink_value = sink_logit.reshape(1, kv_heads, group_size, 1, 1)
    top_score = jnp.maximum(jnp.max(scores, axis=-1, keepdims=True), sink_value)
    exponent = jnp.exp(scores - top_score)
    totals = jnp.sum(exponent, axis=-1, keepdims=True) + jnp.exp(sink_value - top_score)
    weights = (exponent / totals).astype(jnp.bfloat16)
    attended = jnp.einsum(
        "bkgqs,bskd->bqkgd", weights, value_blocks, preferred_element_type=jnp.float32
    )
    return attended.reshape(row_count, kv_heads * group_size * head_width).astype(jnp.bfloat16)


def discretize(decay_rate, rotation, log_step, in_re, in_im):
    time_step = jnp.exp(log_step)[:, None]
    lambda_re = -decay_rate
    modulus = jnp.exp(lambda_re * time_step)
    pole_re = modulus * jnp.cos(rotation * time_step)
    pole_im = modulus * jnp.sin(rotation * time_step)
    minus_one = pole_re - 1.0
    denominator = lambda_re * lambda_re + rotation * rotation
    factor_re = ((minus_one * lambda_re + pole_im * rotation) / denominator)[..., None]
    factor_im = ((pole_im * lambda_re - minus_one * rotation) / denominator)[..., None]
    drive_re = factor_re * in_re - factor_im * in_im
    drive_im = factor_re * in_im + factor_im * in_re
    return (pole_re, pole_im, drive_re, drive_im)


def complex_power(decay_rate, rotation, log_step, exponent):
    time_step = jnp.exp(log_step)[:, None]
    modulus = jnp.exp(-decay_rate * time_step * exponent)
    angle = rotation * time_step * exponent
    return (modulus * jnp.cos(angle), modulus * jnp.sin(angle))


def token_shuffle(rows, inverse):
    steps = rows // SUB
    out_row = lax.broadcasted_iota(jnp.int32, (rows, rows), 1 if inverse else 0)
    in_row = lax.broadcasted_iota(jnp.int32, (rows, rows), 0 if inverse else 1)
    token = (out_row % SUB) * steps + out_row // SUB
    return (token == in_row).astype(jnp.bfloat16)


def scan_kernel(
    u_ref, drive_ref, pole_re_ref, pole_im_ref, jump_re_ref, jump_im_ref,
    state_ref, carry_re_ref, carry_im_ref, end_re_ref, end_im_ref,
):
    rows = u_ref.shape[0]
    width = pole_re_ref.shape[-1]
    shuffle = token_shuffle(rows, False)
    shuffled = jnp.dot(shuffle, u_ref[...], preferred_element_type=jnp.float32)
    state_ref[...] = jnp.dot(
        shuffled, drive_ref[0], precision=lax.Precision.HIGHEST,
        preferred_element_type=jnp.float32,
    )
    pole_re = jnp.broadcast_to(pole_re_ref[0], (SUB, width))
    pole_im = jnp.broadcast_to(pole_im_ref[0], (SUB, width))
    now_re = jnp.zeros((SUB, width), jnp.float32)
    now_im = jnp.zeros((SUB, width), jnp.float32)
    for step in range(rows // SUB):
        at = slice(step * SUB, (step + 1) * SUB)
        new_re = pole_re * now_re - pole_im * now_im + state_ref[at, :width]
        new_im = pole_re * now_im + pole_im * now_re + state_ref[at, width:]
        state_ref[at, :width] = new_re
        state_ref[at, width:] = new_im
        now_re, now_im = new_re, new_im
    jump_re, jump_im = (jump_re_ref[0], jump_im_ref[0])
    held_re = jnp.zeros((1, width), jnp.float32)
    held_im = jnp.zeros((1, width), jnp.float32)
    for chunk in range(SUB):
        carry_re_ref[chunk : chunk + 1, :] = held_re
        carry_im_ref[chunk : chunk + 1, :] = held_im
        next_re = jump_re * held_re - jump_im * held_im + now_re[chunk : chunk + 1]
        next_im = jump_re * held_im + jump_im * held_re + now_im[chunk : chunk + 1]
        held_re, held_im = next_re, next_im
    end_re_ref[0] = held_re
    end_im_ref[0] = held_im


def readout_kernel(
    u_ref, state_ref, carry_re_ref, carry_im_ref, prior_re_ref, prior_im_ref,
    chunk_re_ref, chunk_im_ref, pole_re_ref, pole_im_ref, read_ref, skip_ref, out_ref, full_ref,
):
    rows = u_ref.shape[0]
    width = pole_re_ref.shape[-1]
    prior_re, prior_im = (prior_re_ref[0], prior_im_ref[0])
    chunk_re, chunk_im = (chunk_re_ref[...], chunk_im_ref[...])
    add_re = carry_re_ref[...] + chunk_re * prior_re - chunk_im * prior_im
    add_im = carry_im_ref[...] + chunk_re * prior_im + chunk_im * prior_re
    pole_re = jnp.broadcast_to(pole_re_ref[0], (SUB, width))
    pole_im = jnp.broadcast_to(pole_im_ref[0], (SUB, width))
    for step in range(rows // SUB):
        at = slice(step * SUB, (step + 1) * SUB)
        turned_re = pole_re * add_re - pole_im * add_im
        turned_im = pole_re * add_im + pole_im * add_re
        full_ref[at, :width] = state_ref[at, :width] + turned_re
        full_ref[at, width:] = state_ref[at, width:] + turned_im
        add_re, add_im = turned_re, turned_im
    summed = jnp.dot(
        full_ref[...], read_ref[0], precision=lax.Precision.HIGHEST,
        preferred_element_type=jnp.float32,
    )
    shuffled = jnp.dot(
        token_shuffle(rows, False), u_ref[...], preferred_element_type=jnp.float32
    )
    mixed = jax.nn.gelu(summed + skip_ref[...] * shuffled).astype(jnp.bfloat16)
    out_ref[...] = jnp.dot(
        token_shuffle(rows, True), mixed, preferred_element_type=jnp.float32
    ).astype(jnp.bfloat16)


def block_diagonal(parts):
    blocks, per, rows, columns = parts[0].shape
    same = jnp.eye(per, dtype=bool)[None, :, None, :, None]
    spread = [
        jnp.where(same, part[:, :, :, None, :], 0.0).reshape(blocks, per * rows, per * columns)
        for part in parts
    ]
    return jnp.concatenate(spread, axis=2)


def state_tables(rows, decay_rate, rotation, log_step, in_re, in_im, out_re, out_im):
    groups, states = decay_rate.shape
    group_width = in_re.shape[-1]
    per = min(groups, max(1, 128 // group_width))
    blocks, width = (groups // per, per * states)
    pole_re, pole_im, drive_re, drive_im = discretize(decay_rate, rotation, log_step, in_re, in_im)
    steps = rows // SUB

    def by_block(value):
        return value.reshape(blocks, per, *value.shape[1:])

    def flat(value):
        return value.reshape(blocks, 1, width)

    drive = block_diagonal(
        [by_block(jnp.swapaxes(drive_re, 1, 2)), by_block(jnp.swapaxes(drive_im, 1, 2))]
    )
    read = jnp.swapaxes(block_diagonal([by_block(out_re), by_block(-out_im)]), 1, 2)
    jump = complex_power(decay_rate, rotation, log_step, float(steps))
    chunk_powers = [
        complex_power(decay_rate, rotation, log_step, float(steps * c)) for c in range(SUB)
    ]
    chunk_re = jnp.stack([p[0].reshape(groups * states) for p in chunk_powers])
    chunk_im = jnp.stack([p[1].reshape(groups * states) for p in chunk_powers])
    return dict(
        drive=drive, read=read, pole_re=flat(pole_re), pole_im=flat(pole_im),
        jump_re=flat(jump[0]), jump_im=flat(jump[1]), chunk_re=chunk_re, chunk_im=chunk_im,
        blocks=blocks, width=width, channels=per * group_width,
    )


def local_scan(inputs, tables):
    rows = inputs.shape[0]
    blocks, width, channels = (tables["blocks"], tables["width"], tables["channels"])
    row_spec = pl.BlockSpec((1, 1, width), lambda b: (b, 0, 0))
    carry_spec = pl.BlockSpec((SUB, width), lambda b: (0, b))
    return pl.pallas_call(
        scan_kernel,
        grid=(blocks,),
        in_specs=[
            pl.BlockSpec((rows, channels), lambda b: (0, b)),
            pl.BlockSpec((1, channels, 2 * width), lambda b: (b, 0, 0)),
            row_spec, row_spec, row_spec, row_spec,
        ],
        out_specs=[
            pl.BlockSpec((rows, 2 * width), lambda b: (0, b)),
            carry_spec, carry_spec, row_spec, row_spec,
        ],
        out_shape=[
            jax.ShapeDtypeStruct((rows, 2 * width * blocks), jnp.float32),
            jax.ShapeDtypeStruct((SUB, width * blocks), jnp.float32),
            jax.ShapeDtypeStruct((SUB, width * blocks), jnp.float32),
            jax.ShapeDtypeStruct((blocks, 1, width), jnp.float32),
            jax.ShapeDtypeStruct((blocks, 1, width), jnp.float32),
        ],
        cost_estimate=pl.CostEstimate(
            flops=12 * rows * channels * width * blocks, bytes_accessed=10**7, transcendentals=0
        ),
    )(
        inputs, tables["drive"], tables["pole_re"], tables["pole_im"],
        tables["jump_re"], tables["jump_im"],
    )


def read_states(inputs, scanned, prior_re, prior_im, tables, skip_gain):
    rows = inputs.shape[0]
    state, carry_re, carry_im = scanned[:3]
    blocks, width, channels = (tables["blocks"], tables["width"], tables["channels"])
    row_spec = pl.BlockSpec((1, 1, width), lambda b: (b, 0, 0))
    carry_spec = pl.BlockSpec((SUB, width), lambda b: (0, b))
    return pl.pallas_call(
        readout_kernel,
        grid=(blocks,),
        in_specs=[
            pl.BlockSpec((rows, channels), lambda b: (0, b)),
            pl.BlockSpec((rows, 2 * width), lambda b: (0, b)),
            carry_spec, carry_spec, row_spec, row_spec, carry_spec, carry_spec,
            row_spec, row_spec,
            pl.BlockSpec((1, 2 * width, channels), lambda b: (b, 0, 0)),
            pl.BlockSpec((1, channels), lambda b: (0, b)),
        ],
        out_specs=pl.BlockSpec((rows, channels), lambda b: (0, b)),
        out_shape=jax.ShapeDtypeStruct((rows, channels * blocks), jnp.bfloat16),
        scratch_shapes=[pltpu.VMEM((rows, 2 * width), jnp.float32)],
        cost_estimate=pl.CostEstimate(
            flops=12 * rows * channels * width * blocks, bytes_accessed=10**7, transcendentals=0
        ),
    )(
        inputs, state, carry_re, carry_im, prior_re, prior_im,
        tables["chunk_re"], tables["chunk_im"], tables["pole_re"], tables["pole_im"],
        tables["read"], skip_gain.reshape(1, -1),
    )


def carried_state(end_re, end_im, decay_rate, rotation, log_step, rows):
    ends = jnp.stack([end_re, end_im])
    shape = end_re.shape
    size = lax.axis_size("sp")
    reach = 1
    while reach < size:
        power_re, power_im = complex_power(decay_rate, rotation, log_step, float(rows * reach))
        power_re, power_im = (power_re.reshape(shape), power_im.reshape(shape))
        prior = passed_along(ends, "sp", reach)
        ends = ends + jnp.stack(
            [
                power_re * prior[0] - power_im * prior[1],
                power_re * prior[1] + power_im * prior[0],
            ]
        )
        reach *= 2
    before = passed_along(ends, "sp", 1)
    return (before[0], before[1])


def state_branch(inputs, decay_rate, rotation, log_step, in_re, in_im, out_re, out_im, skip_gain):
    rows = inputs.shape[0]
    tables = state_tables(rows, decay_rate, rotation, log_step, in_re, in_im, out_re, out_im)
    scanned = local_scan(inputs, tables)
    prior_re, prior_im = carried_state(
        scanned[3], scanned[4], decay_rate, rotation, log_step, rows
    )
    return read_states(inputs, scanned, prior_re, prior_im, tables, skip_gain)


def earlier_window(key_rows, value_rows):
    joined = jnp.concatenate([key_rows, value_rows], axis=1)
    prior = passed_along(joined, "sp", 1)
    return jnp.concatenate([prior, joined], axis=0)


def make_adder(normed_cols):

    def add_pieces(carried, weight_pieces, row_start):
        updated = []
        for running_total, weight_piece in zip(carried, weight_pieces):
            product = lax.dot_general(
                normed_cols,
                weight_piece,
                (((0,), (0,)), ((), ())),
                preferred_element_type=jnp.float32,
            )
            updated.append(product)
        return tuple(updated)

    return add_pieces


def whole_weights_body(
    tokens,
    norm_gain,
    w_query,
    w_key,
    w_value,
    w_state_in,
    sink_logit,
    decay_rate,
    rotation,
    log_step,
    in_re,
    in_im,
    out_re,
    out_im,
    skip_gain,
    w_attn_out,
    w_state_out,
    out_gain,
):
    row_count = tokens.shape[0]
    window = WINDOW
    head_width = HEAD
    wide_tokens = tokens.astype(jnp.float32)
    normed = (
        wide_tokens
        * lax.rsqrt(jnp.mean(wide_tokens * wide_tokens, axis=-1, keepdims=True) + epsilon)
        * norm_gain
    ).astype(jnp.bfloat16)
    first_row = lax.axis_index("sp") * row_count
    positions = first_row + jnp.arange(row_count, dtype=jnp.int32)
    add_pieces = make_adder(jnp.transpose(normed))

    def empty_like(weight_shard):
        return jnp.zeros((row_count, weight_shard.shape[1]), jnp.float32)

    query_sum, key_sum, value_sum, input_sum = add_pieces(
        (empty_like(w_query), empty_like(w_key), empty_like(w_value), empty_like(w_state_in)),
        (
            lax.all_gather(w_query, "sp", axis=0, tiled=True),
            lax.all_gather(w_key, "sp", axis=0, tiled=True),
            lax.all_gather(w_value, "sp", axis=0, tiled=True),
            lax.all_gather(w_state_in, "sp", axis=0, tiled=True),
        ),
        jnp.int32(0),
    )
    queries, key_rows, value_rows = shape_heads(
        query_sum, key_sum, value_sum, positions, head_width
    )
    joined_rows = earlier_window(key_rows, value_rows)
    inputs = input_sum.astype(jnp.bfloat16)
    mixed_state = state_branch(
        inputs, decay_rate, rotation, log_step, in_re, in_im, out_re, out_im, skip_gain
    )
    kv_width = key_rows.shape[1]
    kv_heads = kv_width // head_width
    all_keys = joined_rows[:, :kv_width].reshape(window + row_count, kv_heads, head_width)
    all_values = joined_rows[:, kv_width:].reshape(window + row_count, kv_heads, head_width)
    attended = band_attention(queries, all_keys, all_values, sink_logit, first_row, window)
    attn_rows, state_rows = (
        lax.all_gather(w_attn_out, "sp", axis=1, tiled=True),
        lax.all_gather(w_state_out, "sp", axis=1, tiled=True),
    )
    projected = lax.psum_scatter(
        (
            jnp.dot(attended, attn_rows, preferred_element_type=jnp.float32)
            + jnp.dot(mixed_state, state_rows, preferred_element_type=jnp.float32)
        ).astype(jnp.bfloat16),
        "tp",
        scatter_dimension=0,
        tiled=True,
    ).astype(jnp.float32)
    row_scale = lax.rsqrt(jnp.mean(projected * projected, axis=-1, keepdims=True) + epsilon)
    return (projected * row_scale * out_gain).astype(jnp.bfloat16)


SIDE = 2
PLANE = SIDE * SIDE
CORES = 2
CHUNKS = 2
LANES = 128
MESH = pl.DeviceIdType.MESH


def place():
    me = lax.axis_index("sp")
    return (lax.div(me, PLANE), lax.rem(me, PLANE), lax.axis_index("tp"))


def plane_neighbours(spot):
    beside = spot + 1 - 2 * lax.rem(spot, SIDE)
    above = spot + SIDE - 2 * SIDE * lax.div(spot, SIDE)
    return (beside, above)


def greet(layers, layer, spot, core):
    barrier = pltpu.get_barrier_semaphore()
    beside, above = plane_neighbours(spot)
    for ahead in range(1, layers):
        other = lax.rem(layer + ahead, layers)
        pl.semaphore_signal(
            barrier, inc=1, device_id={"sp": other * PLANE + spot}, device_id_type=MESH
        )
    for other in (beside, above, PLANE - 1 - spot):
        pl.semaphore_signal(
            barrier, inc=1, device_id={"sp": layer * PLANE + other}, device_id_type=MESH
        )
    pl.semaphore_signal(barrier, inc=1, device_id={"tp": 1 - core}, device_id_type=MESH)


def greeted(layers):
    pl.semaphore_wait(pltpu.get_barrier_semaphore(), layers + 3)


def remote(source, target, send_sem, recv_sem, device):
    return pltpu.make_async_remote_copy(
        src_ref=source, dst_ref=target, send_sem=send_sem, recv_sem=recv_sem,
        device_id=device, device_id_type=MESH,
    )


def line_first(layers, layer, spot, source, held, send_sems, recv_sems):
    @pl.when(layer < layers - 1)
    def _():
        remote(
            source, held.at[layer], send_sems.at[0, 0], recv_sems.at[0, 0],
            {"sp": (layer + 1) * PLANE + spot},
        ).start()

    @pl.when(layer > 0)
    def _():
        remote(
            source, held.at[layer], send_sems.at[1, 0], recv_sems.at[1, 0],
            {"sp": (layer - 1) * PLANE + spot},
        ).start()


def line_pass(layers, layer, spot, hop, held, send_sems, recv_sems, landed=None):
    @pl.when(layer - hop >= 0)
    def _():
        block = held.at[layer - hop]
        remote(block, block, send_sems.at[0, 0], recv_sems.at[0, hop - 1], {"sp": 0}).wait_recv()

        @pl.when(layer < layers - 1)
        def _():
            if hop < layers - 1:
                remote(
                    block, block, send_sems.at[0, hop], recv_sems.at[0, hop],
                    {"sp": (layer + 1) * PLANE + spot},
                ).start()

        if landed is not None:
            landed(0, hop, block)

    @pl.when(layer + hop <= layers - 1)
    def _():
        block = held.at[layer + hop]
        remote(block, block, send_sems.at[1, 0], recv_sems.at[1, hop - 1], {"sp": 0}).wait_recv()

        @pl.when(layer > 0)
        def _():
            if hop < layers - 1:
                remote(
                    block, block, send_sems.at[1, hop], recv_sems.at[1, hop],
                    {"sp": (layer - 1) * PLANE + spot},
                ).start()

        if landed is not None:
            landed(1, hop, block)


def line_drain(layers, layer, source, held, send_sems, recv_sems):
    for hop in range(layers - 1):

        @pl.when((layer - hop >= 0) & (layer < layers - 1))
        def _():
            remote(
                source, held.at[layer], send_sems.at[0, hop], recv_sems.at[0, 0], {"sp": 0}
            ).wait_send()

        @pl.when((layer + hop <= layers - 1) & (layer > 0))
        def _():
            remote(
                source, held.at[layer], send_sems.at[1, hop], recv_sems.at[1, 0], {"sp": 0}
            ).wait_send()


def plane_halves(halves, slots, layer, spot, send_sems, recv_sems, half):
    beside, above = plane_neighbours(spot)
    return [
        remote(
            halves.at[half], slots.at[spot, half], send_sems.at[0, half],
            recv_sems.at[0, half], {"sp": layer * PLANE + beside},
        ),
        remote(
            halves.at[1 - half], slots.at[spot, 1 - half], send_sems.at[1, 1 - half],
            recv_sems.at[1, 1 - half], {"sp": layer * PLANE + above},
        ),
    ]


def plane_first(halves, slots, layer, spot, send_sems, recv_sems):
    for half in (0, 1):
        for copy in plane_halves(halves, slots, layer, spot, send_sems, recv_sems, half):
            copy.start()


def plane_pass(slots, layer, spot, send_sems, recv_sems):
    beside, above = plane_neighbours(spot)
    block = slots.at[beside, 0]
    remote(block, block, send_sems.at[0, 0], recv_sems.at[0, 0], {"sp": 0}).wait_recv()
    remote(
        block, block, send_sems.at[1, 2], recv_sems.at[1, 2], {"sp": layer * PLANE + above}
    ).start()
    block = slots.at[above, 1]
    remote(block, block, send_sems.at[0, 0], recv_sems.at[1, 1], {"sp": 0}).wait_recv()
    remote(
        block, block, send_sems.at[0, 2], recv_sems.at[0, 2], {"sp": layer * PLANE + beside}
    ).start()


def plane_landed(slots, spot, send_sems, recv_sems):
    for way, half in ((0, 1), (1, 0), (0, 2), (1, 2)):
        block = slots.at[spot, 0]
        remote(block, block, send_sems.at[0, 0], recv_sems.at[way, half], {"sp": 0}).wait_recv()
    for way in (0, 1):
        for half in (0, 1, 2):
            block = slots.at[spot, 0]
            remote(block, block, send_sems.at[way, half], recv_sems.at[0, 0], {"sp": 0}).wait_send()


def lanes_of(rows):
    return jnp.concatenate([rows[at : at + 1] for at in range(rows.shape[0])], axis=1)


def split_pair(value):
    high = value.astype(jnp.bfloat16)
    return (high, (value - high.astype(jnp.float32)).astype(jnp.bfloat16))


def make_tables(
    layer, rows, decay_ref, rotation_ref, step_ref, in_re_ref, in_im_ref, out_re_ref, out_im_ref,
    drive, read, powers,
):
    groups, group_width, states = in_re_ref.shape
    kinds, _, width2 = drive.shape
    per = groups // kinds
    width = per * states
    channels = per * group_width
    base = layer * groups
    decay = lanes_of(decay_ref[pl.ds(base, groups), :])
    rotation = lanes_of(rotation_ref[pl.ds(base, groups), :])
    step = jnp.exp(
        jnp.concatenate(
            [jnp.full((1, states), step_ref[base + at], jnp.float32) for at in range(groups)],
            axis=1,
        )
    )
    row = lax.broadcasted_iota(jnp.int32, (SUB, groups * states), 0)
    steps = rows // SUB
    shares = (row * steps, jnp.where(row == 0, 1, jnp.where(row == 1, steps, rows)))
    for at, share in enumerate(shares):
        share = share.astype(jnp.float32)
        modulus = jnp.exp(-decay * step * share)
        angle = rotation * step * share
        powers[2 * at] = modulus * jnp.cos(angle)
        powers[2 * at + 1] = modulus * jnp.sin(angle)
    pole_re, pole_im = (powers[2, 0:1, :], powers[3, 0:1, :])
    minus_one = pole_re - 1.0
    denominator = decay * decay + rotation * rotation
    factor_re = (pole_im * rotation - minus_one * decay) / denominator
    factor_im = (-pole_im * decay - minus_one * rotation) / denominator
    same = (
        lax.broadcasted_iota(jnp.int32, (channels, width), 0) // group_width
        == lax.broadcasted_iota(jnp.int32, (channels, width), 1) // states
    )

    def spread(pieces):
        beside = jnp.concatenate(pieces, axis=1)
        return jnp.concatenate([beside] * per, axis=0)

    for kind in range(kinds):
        lanes = slice(kind * width, (kind + 1) * width)
        f_re, f_im = (factor_re[:, lanes], factor_im[:, lanes])
        own = range(kind * per, (kind + 1) * per)
        m_re = spread([in_re_ref[at] for at in own])
        m_im = spread([in_im_ref[at] for at in own])
        for part, value in ((0, f_re * m_re - f_im * m_im), (1, f_re * m_im + f_im * m_re)):
            high, low = split_pair(jnp.where(same, value, 0.0))
            columns = slice(part * width, (part + 1) * width)
            drive[kind, :channels, columns] = high
            drive[kind, channels:, columns] = low
        r_re = spread([out_re_ref[at] for at in own])
        r_im = spread([-out_im_ref[at] for at in own])
        for part, value in ((0, r_re), (1, r_im)):
            high, low = split_pair(jnp.where(same, value, 0.0))
            columns = slice(part * width, (part + 1) * width)
            read[kind, :channels, columns] = high
            read[kind, channels:, columns] = low


def normalise(block, held, gain_ref, normed):
    _, parts, chunks, part_rows, model = held.shape
    tall = 16
    per = part_rows // tall

    @pl.loop(0, parts * chunks * per)
    def _(at):
        value = held[
            block, at // (chunks * per), (at // per) % chunks,
            pl.ds(pl.multiple_of((at % per) * tall, tall), tall), :,
        ].astype(jnp.float32)
        scale = lax.rsqrt(jnp.sum(value * value, axis=-1, keepdims=True) / model + epsilon)
        normed[block, pl.ds(pl.multiple_of(at * tall, tall), tall), :] = (
            value * scale * gain_ref[...]
        ).astype(jnp.bfloat16)


def project_block(block, spot, normed, weights, tables, queries, pairs, inputs):
    rows = normed.shape[1]
    layers = weights.shape[0]
    depth = weights.shape[2] * weights.shape[3]
    query_width, pair_width = (queries.shape[-1], pairs.shape[-1])
    half_width = HEAD // 2
    row_cos_ref, row_sin_ref, block_cos_ref, block_sin_ref = tables
    lane = lax.broadcasted_iota(jnp.int32, (rows, LANES), 1)
    low = lax.rem(lane, HEAD) < half_width

    def turn(value, cosine, sine):
        swapped = jnp.where(
            low, -pltpu.roll(value, LANES - half_width, 1), pltpu.roll(value, half_width, 1)
        )
        return value * cosine + swapped * sine

    total = None
    for at in range(layers * PLANE):
        piece = jnp.dot(
            normed[block, :, at * depth : (at + 1) * depth],
            weights[at // PLANE, at % PLANE].reshape(depth, weights.shape[-1]),
            preferred_element_type=jnp.float32,
        )
        total = piece if total is None else total + piece
    here = pl.ds(block * PLANE + spot, 1)
    block_cos, block_sin = (block_cos_ref[here, :], block_sin_ref[here, :])
    cosine = row_cos_ref[...] * block_cos - row_sin_ref[...] * block_sin
    sine = row_sin_ref[...] * block_cos + row_cos_ref[...] * block_sin
    turned = [turn(total[:, at : at + LANES], cosine, sine) for at in range(0, query_width, LANES)]
    queries[block] = jnp.concatenate(turned, axis=1).astype(jnp.bfloat16)
    value = total[:, query_width : query_width + pair_width]
    pairs[block] = jnp.where(lane < HEAD, turn(value, cosine, sine), value).astype(jnp.bfloat16)
    inputs[block] = jnp.dot(
        token_shuffle(rows, False), total[:, query_width + pair_width :].astype(jnp.bfloat16),
        preferred_element_type=jnp.float32,
    ).astype(jnp.bfloat16)


def scan_block(block, spot, inputs, drive, powers, states, carries, ends):
    kinds, _, width2 = drive.shape
    width = width2 // 2
    channels = inputs.shape[-1] // kinds
    rows = inputs.shape[1]
    for kind in range(kinds):
        lanes = slice(kind * width, (kind + 1) * width)
        own = inputs[block, :, kind * channels : (kind + 1) * channels]
        states[block, kind] = jnp.dot(
            jnp.concatenate([own, own], axis=1), drive[kind], preferred_element_type=jnp.float32
        )
        pole_re = jnp.broadcast_to(powers[2, 0:1, lanes], (SUB, width))
        pole_im = jnp.broadcast_to(powers[3, 0:1, lanes], (SUB, width))
        now_re = jnp.zeros((SUB, width), jnp.float32)
        now_im = jnp.zeros((SUB, width), jnp.float32)
        for step in range(rows // SUB):
            at = slice(step * SUB, (step + 1) * SUB)
            new_re = pole_re * now_re - pole_im * now_im + states[block, kind, at, :width]
            new_im = pole_re * now_im + pole_im * now_re + states[block, kind, at, width:]
            states[block, kind, at, :width] = new_re
            states[block, kind, at, width:] = new_im
            now_re, now_im = new_re, new_im
        jump_re, jump_im = (powers[2, 1:2, lanes], powers[3, 1:2, lanes])
        held_re = jnp.zeros((1, width), jnp.float32)
        held_im = jnp.zeros((1, width), jnp.float32)
        re, im = ([], [])
        for chunk in range(SUB):
            re.append(held_re)
            im.append(held_im)
            next_re = jump_re * held_re - jump_im * held_im + now_re[chunk : chunk + 1]
            next_im = jump_re * held_im + jump_im * held_re + now_im[chunk : chunk + 1]
            held_re, held_im = next_re, next_im
        carries[block, kind, :, :width] = jnp.concatenate(re, axis=0)
        carries[block, kind, :, width:] = jnp.concatenate(im, axis=0)
        ends[spot, block, kind, :, :width] = held_re
        ends[spot, block, kind, :, width:] = held_im


def attend_block(block, layer, spot, queries, pairs, before, sink_ref, out):
    rows, query_width = queries.shape[1:]
    group = query_width // HEAD
    pair, prior = (pairs[block], before[block])
    keys = jnp.concatenate([prior[:, :HEAD], pair[:, :HEAD]], axis=0)
    values = jnp.concatenate([prior[:, HEAD:], pair[:, HEAD:]], axis=0)
    query_at = lax.broadcasted_iota(jnp.int32, (rows, rows + WINDOW), 0)
    key_at = lax.broadcasted_iota(jnp.int32, (rows, rows + WINDOW), 1) - WINDOW
    gap = query_at - key_at
    first = (block * PLANE + spot) * rows
    visible = (gap >= 0) & (gap < WINDOW) & (key_at + first >= 0)
    pieces = []
    for head in range(group):
        query = queries[block, :, head * HEAD : (head + 1) * HEAD]
        scores = lax.dot_general(
            query, keys, (((1,), (1,)), ((), ())), preferred_element_type=jnp.float32
        ) / math.sqrt(HEAD)
        scores = jnp.where(visible, scores, -jnp.inf)
        sink = jnp.full((1, 1), sink_ref[layer * group + head], jnp.float32)
        top = jnp.maximum(jnp.max(scores, axis=-1, keepdims=True), sink)
        exponent = jnp.exp(scores - top)
        total = jnp.sum(exponent, axis=-1, keepdims=True) + jnp.exp(sink - top)
        weights = (exponent / total).astype(jnp.bfloat16)
        pieces.append(jnp.dot(weights, values, preferred_element_type=jnp.float32))
    out[...] = jnp.concatenate(pieces, axis=1).astype(jnp.bfloat16)


def find_priors(ends, powers, priors):
    plane, layers, kinds = ends.shape[:3]
    width = ends.shape[-1] // 2
    for kind in range(kinds):
        lanes = slice(kind * width, (kind + 1) * width)
        power_re, power_im = (powers[2, 2:3, lanes], powers[3, 2:3, lanes])
        held_re = jnp.zeros((1, width), jnp.float32)
        held_im = jnp.zeros((1, width), jnp.float32)
        for at in range(layers * plane):
            priors[at, kind, :, :width] = held_re
            priors[at, kind, :, width:] = held_im
            end_re = ends[at % plane, at // plane, kind, :, :width]
            end_im = ends[at % plane, at // plane, kind, :, width:]
            held_re, held_im = (
                power_re * held_re - power_im * held_im + end_re,
                power_re * held_im + power_im * held_re + end_im,
            )


def read_block(block, layer, spot, inputs, states, carries, priors, powers, read, skip_ref, out):
    kinds, channels2, width2 = read.shape
    width, channels = (width2 // 2, channels2 // 2)
    rows = inputs.shape[1]
    contract = (((1,), (1,)), ((), ()))
    pieces = []
    for kind in range(kinds):
        lanes = slice(kind * width, (kind + 1) * width)
        prior_re = priors[block * PLANE + spot, kind, :, :width]
        prior_im = priors[block * PLANE + spot, kind, :, width:]
        chunk_re, chunk_im = (powers[0, :, lanes], powers[1, :, lanes])
        add_re = carries[block, kind, :, :width] + chunk_re * prior_re - chunk_im * prior_im
        add_im = carries[block, kind, :, width:] + chunk_re * prior_im + chunk_im * prior_re
        pole_re = jnp.broadcast_to(powers[2, 0:1, lanes], (SUB, width))
        pole_im = jnp.broadcast_to(powers[3, 0:1, lanes], (SUB, width))
        for step in range(rows // SUB):
            at = slice(step * SUB, (step + 1) * SUB)
            turned_re = pole_re * add_re - pole_im * add_im
            turned_im = pole_re * add_im + pole_im * add_re
            states[block, kind, at, :width] += turned_re
            states[block, kind, at, width:] += turned_im
            add_re, add_im = turned_re, turned_im
        high, low = split_pair(states[block, kind])
        both = lax.dot_general(high, read[kind], contract, preferred_element_type=jnp.float32)
        rest = lax.dot_general(
            low, read[kind, :channels], contract, preferred_element_type=jnp.float32
        )
        summed = both[:, :channels] + both[:, channels:] + rest
        at = pl.multiple_of(layer * (kinds * channels) + kind * channels, channels)
        skip = skip_ref[:, pl.ds(at, channels)]
        own = inputs[block, :, kind * channels : (kind + 1) * channels].astype(jnp.float32)
        pieces.append(jax.nn.gelu(summed + skip * own).astype(jnp.bfloat16))
    out[...] = jnp.dot(
        token_shuffle(rows, True), jnp.concatenate(pieces, axis=1),
        preferred_element_type=jnp.float32,
    ).astype(jnp.bfloat16)


def whole_kernel(
    tokens_ref, query_ref, key_ref, value_ref, state_ref,
    in_re_ref, in_im_ref, out_re_ref, out_im_ref, attn_out_ref, state_out_ref,
    norm_gain_ref, out_gain_ref, decay_ref, rotation_ref, skip_ref,
    row_cos_ref, row_sin_ref, block_cos_ref, block_sin_ref, step_ref, sink_ref,
    out_ref,
    key_value, packed, weights, held, normed, in_re, in_im, out_re, out_im, drive, read, powers,
    queries, pairs, before, inputs, states, carries, ends, priors,
    mixers, matrices, total, partial, arrived, summed, pieces,
    load_sem, pack_sem, far_send, far_recv, line_send, line_recv, part_send, part_recv,
    side_send, side_recv, halo_send, halo_recv, end_send, end_recv,
    mixer_send, mixer_recv, matrix_send, matrix_recv, half_send, half_recv,
    piece_send, piece_recv,
):
    layers = held.shape[0]
    rows = pairs.shape[1]
    layer, spot, core = place()
    greet(layers, layer, spot, core)
    query_width, pair_width = (queries.shape[-1], pairs.shape[-1])
    state_width = inputs.shape[-1]
    groups = in_re.shape[0]
    mine = pl.ds(layer * groups, groups)
    loads = [
        pltpu.make_async_copy(key_ref, key_value.at[0], load_sem.at[0]),
        pltpu.make_async_copy(value_ref, key_value.at[1], load_sem.at[1]),
    ]
    spans = (
        (query_ref, query_width, 0),
        (state_ref, state_width, query_width + pair_width),
    )
    def loaded(block, target, at):
        return [
            pltpu.make_async_copy(
                source.at[:, :, pl.ds(pl.multiple_of(block * wide, wide), wide)],
                target.at[:, :, pl.ds(to, wide)], pack_sem.at[at, part],
            )
            for part, (source, wide, to) in enumerate(spans)
        ]

    own_weights = loaded(layer, weights.at[layer, spot], layers)
    far_loads = [copy for at in range(layers) for copy in loaded(at, packed.at[at], at)]
    own_tokens = pltpu.make_async_copy(tokens_ref, held.at[layer], load_sem.at[3])
    table_loads = [
        pltpu.make_async_copy(source.at[mine], target, load_sem.at[5 + at])
        for at, (source, target) in enumerate(
            ((in_re_ref, in_re), (in_im_ref, in_im), (out_re_ref, out_re), (out_im_ref, out_im))
        )
    ]
    matrix_loads = [
        pltpu.make_async_copy(source, matrices.at[kind, spot], load_sem.at[9 + kind])
        for kind, source in enumerate((attn_out_ref, state_out_ref))
    ]
    for copy in loads + own_weights + far_loads + [own_tokens] + table_loads + matrix_loads:
        copy.start()
    for copy in loads:
        copy.wait()
    middle = slice(query_width, query_width + pair_width)
    for at in range(layers):
        head = slice(at * HEAD, (at + 1) * HEAD)
        packed[at, :, :, middle] = jnp.concatenate(
            [key_value[0, :, :, head], key_value[1, :, :, head]], axis=-1
        )
    weights[layer, spot, :, :, middle] = packed[layer, :, :, middle]
    for copy in far_loads:
        copy.wait()
    greeted(layers)

    below, above = (layer, layers - 1 - layer)
    least = jnp.minimum(below, above)
    short = jnp.where(below < above, 0, 1)

    def arrival(at):
        paired = at <= 2 * least
        hop = jnp.where(paired, lax.div(at + 1, 2), at - least)
        way = jnp.where(paired & (lax.rem(at, 2) == 1), short, 1 - short)
        return (jnp.where(way == 0, layer - hop, layer + hop), hop, way)

    def far_copy(way, hop):
        other = layer + hop if way == 0 else layer - hop
        return remote(
            packed.at[other], weights.at[layer, spot], far_send.at[way, hop],
            far_recv.at[way, hop], {"sp": other * PLANE + spot},
        )

    def each_far(hop, action):
        for way, there in ((0, layer + hop <= layers - 1), (1, layer - hop >= 0)):

            @pl.when(there)
            def _():
                action(far_copy(way, hop))

    def start(copy):
        copy.start()

    each_far(1, start)

    @pl.when(least > 0)
    def _():
        for hop in range(2, layers):
            each_far(hop, start)

    chunks = held.shape[2]

    def chunk_lines(action):
        for chunk in range(chunks):
            action(chunk, held.at[:, core, chunk], line_send.at[chunk], line_recv.at[chunk])

    for copy in own_weights:
        copy.wait()

    def part(way, hop, chunk, half):
        block = held.at[layer + hop - 2 * hop * (1 - way), half, chunk]
        return remote(
            block, block, part_send.at[chunk, way, hop - 1], part_recv.at[chunk, way, hop - 1],
            {"tp": 1 - core},
        )

    def send_tokens(side):
        onward = 1 - side
        for chunk in range(chunks):
            remote(
                tokens_ref.at[core, chunk], held.at[layer, core, chunk],
                line_send.at[chunk, onward, 0], line_recv.at[chunk, onward, 0],
                {"sp": (layer + 1 - 2 * onward) * PLANE + spot},
            ).start()

    def pass_tokens(way, hop):
        block = layer + hop - 2 * hop * (1 - way)

        def step(chunk, slots, send, recv):
            half = slots.at[block]
            remote(half, half, send.at[way, 0], recv.at[way, hop - 1], {"sp": 0}).wait_recv()
            onward = jnp.where(way == 0, layer < layers - 1, layer > 0)

            @pl.when(onward & (hop < layers - 1))
            def _():
                remote(
                    half, half, send.at[way, hop], recv.at[way, hop],
                    {"sp": (layer + 1 - 2 * way) * PLANE + spot},
                ).start()

            part(way, hop, chunk, core).start()

        chunk_lines(step)

    plane_first(
        weights.at[layer, spot], weights.at[layer], layer, spot, side_send.at[0], side_recv.at[0]
    )

    @pl.when(least == 0)
    def _():
        send_tokens(1 - short)

    for copy in table_loads:
        copy.wait()
    make_tables(
        layer, rows, decay_ref, rotation_ref, step_ref, in_re, in_im, out_re, out_im,
        drive, read, powers,
    )
    before[0] = jnp.zeros(before.shape[1:], before.dtype)
    own_tokens.wait()
    normalise(layer, held, norm_gain_ref, normed)
    plane_pass(weights.at[layer], layer, spot, side_send.at[0], side_recv.at[0])

    for at in range(1, layers):
        origin, hop, way = arrival(jnp.int32(at))
        block = weights.at[origin, spot]
        remote(block, block, far_send.at[0, 0], far_recv.at[way, hop], {"sp": 0}).wait_recv()

        if at == 1:

            @pl.when(least > 0)
            def _():
                send_tokens(short)

        if at == 1:

            @pl.when(least > 0)
            def _():
                send_tokens(1 - short)

        plane_first(
            weights.at[origin, spot], weights.at[origin], layer, spot,
            side_send.at[at], side_recv.at[at],
        )
        plane_pass(weights.at[origin], layer, spot, side_send.at[at], side_recv.at[at])
        if at == 1:

            @pl.when(least == 0)
            def _():
                for hop in range(2, layers):
                    each_far(hop, start)

    for copy in matrix_loads:
        copy.wait()
    plane_first(
        matrices.at[0, spot], matrices.at[0], layer, spot, matrix_send.at[0], matrix_recv.at[0]
    )

    @pl.when(least > 0)
    def _():
        pass_tokens(short, 1)

    pass_tokens(1 - short, 1)

    def landed(at):
        block, hop, way = arrival(at)
        for chunk in range(chunks):
            part(way, hop, chunk, 1 - core).wait_recv()
        normalise(block, held, norm_gain_ref, normed)

    for at in range(1, layers):
        hop = arrival(jnp.int32(at))[1]

        @pl.when(hop == 1)
        def _():
            landed(jnp.int32(at))

    for at in range(layers):
        origin = layer if at == 0 else arrival(jnp.int32(at))[0]
        plane_landed(weights.at[origin], spot, side_send.at[at], side_recv.at[at])
    for hop in range(1, layers):
        each_far(hop, lambda copy: copy.wait_send())

    behind = layer * PLANE + lax.rem(spot + 1, PLANE)
    late = lax.div(spot, PLANE - 1)

    def hand_on(block):
        return remote(
            pairs.at[block], before.at[block + late], halo_send.at[block],
            halo_recv.at[block + late], {"sp": behind},
        )

    def arrive(block):
        remote(
            pairs.at[0], before.at[block], halo_send.at[0], halo_recv.at[block], {"sp": behind}
        ).wait_recv()

    def tell(block, at):
        other = lax.rem(spot + 1 + at, PLANE)
        return remote(
            ends.at[spot, block], ends.at[spot, block], end_send.at[at, block],
            end_recv.at[at, block], {"sp": layer * PLANE + other},
        )

    def pass_on(at):
        _, hop, way = arrival(at)

        @pl.when(hop > 1)
        def _():
            pass_tokens(way, hop)

    def send_mixer(kind, block):
        columns = mixers.at[layer, kind, block]
        for way, there in ((0, layer < layers - 1), (1, layer > 0)):

            @pl.when(there)
            def _():
                remote(
                    columns, columns, mixer_send.at[kind, block, way, 0],
                    mixer_recv.at[kind, block, way, 0],
                    {"sp": (layer + 1 - 2 * way) * PLANE + spot},
                ).start()

    def attend(block):
        attend_block(
            block, layer, spot, queries, pairs, before, sink_ref, mixers.at[layer, 0, block]
        )
        send_mixer(0, block)

    def attend_step(at):
        block, hop, way = arrival(at)

        @pl.when((spot > 0) | (block == 0) | ((at > 0) & (way == 1)))
        def _():
            @pl.when((spot > 0) | (block > 0))
            def _():
                arrive(block)

            attend(block)

        @pl.when((spot == 0) & (at > 0) & (way == 0))
        def _():
            arrive(block + 1)
            attend(block + 1)

    def second_matrix(half):
        for copy in plane_halves(
            matrices.at[1, spot], matrices.at[1], layer, spot, matrix_send.at[1],
            matrix_recv.at[1], half,
        ):
            copy.start()

    def attend_all_but_last():
        @pl.loop(0, layers - 1)
        def _(at):
            attend_step(at)

    @pl.loop(0, layers)
    def _(at):
        block, hop, way = arrival(at)
        is_last = at == layers - 1

        @pl.when((least == 0) & is_last)
        def _():
            attend_all_but_last()

        @pl.when((least == 0) & (at > 0))
        def _():
            pass_on(at)

        @pl.when(hop > 1)
        def _():
            landed(at)

        project_block(
            block, spot, normed, weights,
            (row_cos_ref, row_sin_ref, block_cos_ref, block_sin_ref), queries, pairs, inputs,
        )
        hand_on(block).start()
        scan_block(block, spot, inputs, drive, powers, states, carries, ends)
        for peer in range(PLANE - 1):
            tell(block, peer).start()

        @pl.when((least > 0) & (at < layers - 1))
        def _():
            pass_on(at + 1)

        @pl.when((least == 0) & (at == 2))
        def _():
            plane_pass(matrices.at[0], layer, spot, matrix_send.at[0], matrix_recv.at[0])
            second_matrix(0)

        @pl.when((least > 0) & is_last)
        def _():
            attend_all_but_last()

    attend_step(jnp.int32(layers - 1))

    @pl.when(spot == 0)
    def _():
        arrive(layers)

    @pl.when(least > 0)
    def _():
        plane_pass(matrices.at[0], layer, spot, matrix_send.at[0], matrix_recv.at[0])
        second_matrix(0)

    second_matrix(1)
    for block in range(layers):
        for peer in range(PLANE - 1):
            tell(block, peer).wait()
    find_priors(ends, powers, priors)

    @pl.loop(0, layers)
    def _(block):
        read_block(
            block, layer, spot, inputs, states, carries, priors, powers, read, skip_ref,
            mixers.at[layer, 1, block],
        )
        send_mixer(1, block)

    depth = mixers.shape[-1]
    tokens = layers * rows
    half_depth, width = matrices.shape[3:]
    half_rows = rows // CORES
    per = half_depth // depth

    def take(at):
        block, hop, way = arrival(at)

        onward = jnp.where(way == 0, layer < layers - 1, layer > 0)
        for kind in (0, 1):
            for part in range(layers):
                at = jnp.where(2 * block < layers, part, layers - 1 - part) if kind == 0 else part
                columns = mixers.at[block, kind, at]
                remote(
                    columns, columns, mixer_send.at[kind, at, 0, 0],
                    mixer_recv.at[kind, at, way, hop - 1], {"sp": 0},
                ).wait_recv()

                @pl.when(onward & (hop < layers - 1))
                def _():
                    remote(
                        columns, columns, mixer_send.at[kind, at, way, hop],
                        mixer_recv.at[kind, at, way, hop],
                        {"sp": (layer + 1 - 2 * way) * PLANE + spot},
                    ).start()

    def product(block, column):
        low = pl.ds(pl.multiple_of(lax.rem(block, per) * depth, depth), depth)
        return sum(
            jnp.dot(
                mixers[block, kind].reshape(tokens, depth),
                matrices[kind, column, lax.div(block, per), low, :],
                preferred_element_type=jnp.float32,
            )
            for kind in (0, 1)
        )

    for at in range(1, layers - 1):
        take(jnp.where(at <= 2 * least, at - 1 + 2 * (at % 2), at))
        if at == 1:
            plane_pass(matrices.at[1], layer, spot, matrix_send.at[1], matrix_recv.at[1])
    @pl.when(least > 0)
    def _():
        take(jnp.int32(layers - 1))

    for kind in (0, 1):
        plane_landed(matrices.at[kind], spot, matrix_send.at[kind], matrix_recv.at[kind])

    @pl.loop(0, PLANE)
    def _(column):
        total[column] = sum(
            product(arrival(jnp.int32(at))[0], column) for at in range(layers - 1)
        )

    @pl.when(least == 0)
    def _():
        take(jnp.int32(layers - 1))

    last = arrival(jnp.int32(layers - 1))[0]

    def swap(column):
        return remote(
            partial.at[column, 1 - core], arrived.at[column], half_send.at[column],
            half_recv.at[column], {"tp": 1 - core},
        )

    def each_piece(column, action):
        for hop in range(layers - 1, 0, -1):
            for way, there in ((0, layer + hop <= layers - 1), (1, layer - hop >= 0)):

                @pl.when(there)
                def _():
                    other = layer + hop if way == 0 else layer - hop
                    action(
                        remote(
                            summed.at[column, other], pieces.at[column, layer],
                            piece_send.at[column, way, hop], piece_recv.at[column, way, hop],
                            {"sp": other * PLANE + spot},
                        )
                    )

    def each_landing(column):
        for hop in range(1, layers):
            for way, there in ((0, layer - hop >= 0), (1, layer + hop <= layers - 1)):

                @pl.when(there)
                def _():
                    other = layer - hop if way == 0 else layer + hop
                    piece = pieces.at[column, other]
                    remote(
                        piece, piece, piece_send.at[0, 0, 0], piece_recv.at[column, way, hop],
                        {"sp": 0},
                    ).wait_recv()

    def send_column(column):
        swap(column).wait_recv()
        for at in range(layers):
            summed[column, at] = (
                partial[column, core, at].astype(jnp.float32)
                + arrived[column, at].astype(jnp.float32)
            ).astype(jnp.bfloat16)
        each_piece(column, lambda copy: copy.start())
        pieces[column, layer] = summed[column, layer]

    for column in range(PLANE):
        value = total[column] + product(last, column)
        value = value.astype(jnp.bfloat16).reshape(layers, CORES, half_rows, width)
        for half in range(CORES):
            partial[column, half] = value[:, half]
        swap(column).start()
        if column == 0:
            for kind in (0, 1):
                for at in range(layers):
                    line_drain(
                        layers, layer, mixers.at[layer, kind, at], mixers.at[:, kind, at],
                        mixer_send.at[kind, at], mixer_recv.at[kind, at],
                    )
        if column > 0:
            send_column(column - 1)
    send_column(PLANE - 1)
    chunk_lines(
        lambda chunk, slots, send, recv: line_drain(
            layers, layer, slots.at[layer], slots, send, recv
        )
    )
    for hop in range(1, layers):
        for way, there in ((0, layer - hop >= 0), (1, layer + hop <= layers - 1)):

            @pl.when(there)
            def _():
                for chunk in range(chunks):
                    part(way, hop, chunk, core).wait_send()

    for block in range(layers):
        hand_on(block).wait_send()
    squares = jnp.zeros((half_rows, width), jnp.float32)
    for column in range(PLANE):
        each_landing(column)
        for at in range(layers):
            value = pieces[column, at].astype(jnp.float32)
            squares = squares + value * value
    for column in range(PLANE):
        swap(column).wait_send()
        each_piece(column, lambda copy: copy.wait_send())
    mean = jnp.sum(squares, axis=-1, keepdims=True) / (layers * PLANE * width)
    scale = lax.rsqrt(mean + epsilon)
    for at in range(layers):
        for column in range(PLANE):
            low = (at * PLANE + column) * width
            columns = slice(low, low + width)
            out_ref[:, columns] = (
                pieces[column, at].astype(jnp.float32) * scale * out_gain_ref[:, columns]
            ).astype(jnp.bfloat16)


def body(
    tokens,
    norm_gain,
    w_query,
    w_key,
    w_value,
    w_state_in,
    sink_logit,
    decay_rate,
    rotation,
    log_step,
    in_re,
    in_im,
    out_re,
    out_im,
    skip_gain,
    w_attn_out,
    w_state_out,
    out_gain,
):
    rows, model = tokens.shape
    layers = lax.axis_size("sp") // PLANE
    half_rows = rows // CORES
    depth = w_query.shape[0]
    query_width = w_query.shape[1] // layers
    pair_width = 2 * (w_key.shape[1] // layers)
    state_width = w_state_in.shape[1] // layers
    width = query_width + pair_width + state_width
    groups, states, group_width = (in_re.shape[0] // layers, in_re.shape[1], in_re.shape[2])
    kinds = state_width // LANES
    lanes = groups // kinds * states
    height, out_width = w_attn_out.shape
    half = HEAD // 2
    frequency = rotary_base ** (-(np.arange(half) * 2.0 / HEAD))
    frequency = np.tile(frequency, LANES // half)[None, :]
    within = np.arange(rows)[:, None] * frequency
    across = (np.arange(layers * PLANE) * rows)[:, None] * frequency
    tables = [np.cos(within), np.sin(within), np.cos(across), np.sin(across)]
    tables = [jnp.asarray(t, jnp.float32) for t in tables]
    anywhere = pl.BlockSpec(memory_space=pl.ANY)
    vmem = pl.BlockSpec(memory_space=pltpu.VMEM)
    smem = pl.BlockSpec(memory_space=pltpu.SMEM)
    dma = pltpu.SemaphoreType.DMA
    low, full = (jnp.bfloat16, jnp.float32)
    piece = pltpu.VMEM((PLANE, layers, half_rows, out_width), low)

    def halved(matrix):
        return matrix.reshape(2, matrix.shape[0] // 2, matrix.shape[1])

    return pl.pallas_call(
        whole_kernel,
        out_shape=jax.ShapeDtypeStruct((half_rows, model), low),
        in_specs=[anywhere] * 11 + [vmem] * 9 + [smem] * 2,
        out_specs=vmem,
        scratch_shapes=[
            pltpu.VMEM((2, 2, depth // 2, w_key.shape[1]), low),
            pltpu.VMEM((layers, 2, depth // 2, width), low),
            pltpu.VMEM((layers, PLANE, 2, depth // 2, width), low),
            pltpu.VMEM((layers, CORES, CHUNKS, half_rows // CHUNKS, model), low),
            pltpu.VMEM((layers, rows, model), low),
            pltpu.VMEM((groups, group_width, states), full),
            pltpu.VMEM((groups, group_width, states), full),
            pltpu.VMEM((groups, group_width, states), full),
            pltpu.VMEM((groups, group_width, states), full),
            pltpu.VMEM((kinds, 2 * LANES, 2 * lanes), low),
            pltpu.VMEM((kinds, 2 * LANES, 2 * lanes), low),
            pltpu.VMEM((4, SUB, groups * states), full),
            pltpu.VMEM((layers, rows, query_width), low),
            pltpu.VMEM((layers, rows, pair_width), low),
            pltpu.VMEM((layers + 1, rows, pair_width), low),
            pltpu.VMEM((layers, rows, state_width), low),
            pltpu.VMEM((layers, kinds, rows, 2 * lanes), full),
            pltpu.VMEM((layers, kinds, SUB, 2 * lanes), full),
            pltpu.VMEM((PLANE, layers, kinds, 1, 2 * lanes), full),
            pltpu.VMEM((layers * PLANE, kinds, 1, 2 * lanes), full),
            pltpu.VMEM((layers, 2, layers, rows, query_width), low),
            pltpu.VMEM((2, PLANE, 2, height // 2, out_width), low),
            pltpu.VMEM((PLANE, layers * rows, out_width), full),
            pltpu.VMEM((PLANE, CORES, layers, half_rows, out_width), low),
            piece, piece, piece,
            dma((11,)), dma((layers + 1, 2)), dma((2, layers)), dma((2, layers)),
            dma((CHUNKS, 2, layers)), dma((CHUNKS, 2, layers)),
            dma((CHUNKS, 2, layers)), dma((CHUNKS, 2, layers)),
            dma((layers, 2, 3)), dma((layers, 2, 3)), dma((layers,)), dma((layers + 1,)),
            dma((PLANE - 1, layers)), dma((PLANE - 1, layers)),
            dma((2, layers, 2, layers)), dma((2, layers, 2, layers)),
            dma((2, 2, 3)), dma((2, 2, 3)),
            dma((PLANE,)), dma((PLANE,)), dma((PLANE, 2, layers)), dma((PLANE, 2, layers)),
        ],
        compiler_params=pltpu.CompilerParams(
            collective_id=0, has_side_effects=True, vmem_limit_bytes=60 * 2**20
        ),
    )(
        tokens.reshape(CORES, CHUNKS, half_rows // CHUNKS, model), halved(w_query), halved(w_key), halved(w_value),
        halved(w_state_in), jnp.swapaxes(in_re, 1, 2), jnp.swapaxes(in_im, 1, 2), out_re, out_im, halved(w_attn_out),
        halved(w_state_out), norm_gain.reshape(1, -1), out_gain.reshape(1, -1), decay_rate,
        rotation, skip_gain.reshape(1, -1), *tables, log_step, sink_logit,
    )


def suits(mesh, shapes):
    size, cores = (mesh.shape["sp"], mesh.shape["tp"])
    layers = size // PLANE
    query_width, key_width, state_width = (shapes[at][1] // cores for at in (2, 3, 5))
    return (
        size % PLANE == 0
        and layers % 4 == 0
        and cores == CORES
        and shapes[0][0] // size == WINDOW
        and key_width == layers * HEAD
        and state_width == query_width
        and query_width % (layers * LANES) == 0
    )


def solution(mesh):
    def run(*arrays):
        chosen = body if suits(mesh, [array.shape for array in arrays]) else whole_weights_body
        return sharded(mesh, chosen)(*arrays)

    return run


def sharded(mesh, chosen):
    return jax.shard_map(
        chosen,
        mesh=mesh,
        in_specs=(
            P("sp", None),
            P(),
            P("sp", "tp"),
            P("sp", "tp"),
            P("sp", "tp"),
            P("sp", "tp"),
            P("tp"),
            P("tp", None),
            P("tp", None),
            P("tp"),
            P("tp", None, None),
            P("tp", None, None),
            P("tp", None, None),
            P("tp", None, None),
            P("tp"),
            P("tp", "sp"),
            P("tp", "sp"),
            P(),
        ),
        out_specs=P(("sp", "tp"), None),
        check_vma=False,
    )
```
